32 devices in a mesh: grp: 2 (over y), kv: 4 (over z), tp: 4 (over x, core).
Axes of the slice: x: 2, y: 2, z: 4, core: 2. Of those that a mesh axis runs over, the one named last changes fastest.
Arguments:
- tokens: bfloat16 [256, 4, 2048], P(('grp', 'kv'), None, 'tp'), parts along dimension 0, may hold values from -6 to 6
- in_gain: float32 [2048], replicated, may hold values from 0.1 to 1.9
- w_query: bfloat16 [2048, 1024], P('kv', 'tp'), may hold values from -0.125 to 0.125
- w_key: bfloat16 [2048, 1024], P('kv', 'tp'), may hold values from -0.125 to 0.125
- w_value: bfloat16 [2048, 1024], P('kv', 'tp'), may hold values from -0.125 to 0.125
- w_gate: bfloat16 [2048, 1024], P('kv', 'tp'), may hold values from -0.125 to 0.125
- w_beta: bfloat16 [2048, 16], replicated, may hold values from -0.125 to 0.125
- w_decay: bfloat16 [2048, 16], replicated, may hold values from -0.125 to 0.125
- decay_base: float32 [16], P('tp'), may hold values from 0.05 to 1
- out_gain: float32 [64], replicated, may hold values from 0.1 to 1.9
- w_out: bfloat16 [1024, 2048], P('tp', 'kv'), may hold values from -0.1875 to 0.1875
- state: float32 [256, 64, 1024], P(('grp', 'kv'), None, 'tp'), parts along dimension 0, may hold values from -0.8 to 0.8
- prev_keys: bfloat16 [256, 4, 1024], P(('grp', 'kv'), None, 'tp'), parts along dimension 0, may hold values from -6 to 6
- prev_values: bfloat16 [256, 4, 1024], P(('grp', 'kv'), None, 'tp'), parts along dimension 0, may hold values from -6 to 6
- prev_beta: float32 [256, 4, 16], P(('grp', 'kv'), None, 'tp'), parts along dimension 0, may hold values from -6 to 6
- prev_decay: float32 [256, 4, 16], P(('grp', 'kv'), None, 'tp'), parts along dimension 0, may hold values from -1 to -0.02
- accepted: int32 [256], P(('grp', 'kv')), parts along dimension 0, may hold values from 0 to 4
Outputs:
- mixed: bfloat16 [256, 4, 2048], P(('grp', 'kv'), None, 'tp'), parts along dimension 0
- new_state: float32 [256, 64, 1024], P(('grp', 'kv'), None, 'tp'), parts along dimension 0
The draws below stay inside these ranges and needn't reach their ends.
There are 2 independent parts, one for each index of `grp`. The reference program is written for one: setup_inputs(seed, part) draws one part's arguments, and reference() takes and returns one part's arrays. A program takes and returns all parts, laid end to end along the dimension named above; an argument that names none is the same for every part. Nothing has to cross between parts.
All inputs are finite; a program needn't handle non-finite values.
Results may differ from the reference program's by a relative error of at most 0.012.
Values may be sent and summed in bfloat16 or wider, within the bound.
A program may use at most 128 MiB of HBM per device.

```python
import math
import jax
import jax.numpy as jnp
from jax import lax

D = 2048
HEADS = 16
HD = 64
P_SIZE = 4
SEQ_DEV = 32
SEQS = 128
N_KV = 4


def plant(entries, rng, least, top_value):
    spot = [jax.random.randint(jax.random.fold_in(rng, axis), (), 0, length) for axis, length in enumerate(entries.shape)]
    widest = entries.shape.index(max(entries.shape))
    neighbour = spot[:widest] + [(spot[widest] + 1) % entries.shape[widest]] + spot[widest + 1:]
    return entries.at[tuple(spot)].set(least).at[tuple(neighbour)].set(top_value)


def shard_levels(stream_key, shape, cuts, smallest, high):
    gain = 1.0
    for axis_at, shards_of in cuts:
        draws = jax.random.uniform(jax.random.fold_in(jax.random.fold_in(stream_key, 6), axis_at), (shards_of,), jnp.float32, smallest / len(cuts), high / len(cuts))
        gain = gain * jnp.repeat(jnp.exp(draws), shape[axis_at] // shards_of).reshape((-1,) + (1,) * (len(shape) - 1 - axis_at))
    return gain


def centred(own_key, dims, scale, limit, split=(), kind=jnp.bfloat16):
    entries = scale * jax.random.normal(own_key, dims, jnp.float32)
    if split:
        entries = entries * shard_levels(own_key, dims, split, -0.22, 0.18)
    return jnp.clip(entries, -limit, limit).astype(kind)


def setup_inputs(seed: int = 0, part: int = 0) -> dict:
    splits = jax.random.split(jax.random.key(seed), 18)
    part_keys = jax.random.split(jax.random.fold_in(splits[17], part), 18)
    return {
        "tokens": centred(part_keys[0], (SEQS, P_SIZE, D), 1.0, 6.0, ((0, 4), (2, 4))),
        "in_gain": jnp.clip(1.0 + 0.18 * jax.random.normal(splits[1], (D,), jnp.float32), 0.1, 1.9),
        "w_query": centred(splits[2], (D, HEADS * HD), D ** -0.5, 0.125, ((0, 4), (1, 4))),
        "w_key": centred(splits[3], (D, HEADS * HD), D ** -0.5, 0.125, ((0, 4), (1, 4))),
        "w_value": centred(splits[4], (D, HEADS * HD), D ** -0.5, 0.125, ((0, 4), (1, 4))),
        "w_gate": centred(splits[5], (D, HEADS * HD), D ** -0.5, 0.125, ((0, 4), (1, 4))),
        "w_beta": centred(splits[6], (D, HEADS), D ** -0.5, 0.125),
        "w_decay": centred(splits[7], (D, HEADS), D ** -0.5, 0.125),
        "decay_base": jnp.clip(jnp.exp(math.log(1.0) - 2.9957323 * jax.random.uniform(splits[8], (HEADS,), jnp.float32) ** shard_levels(splits[8], (HEADS,), ((0, 4),), -0.2, 0.2)), 0.05, 1.0),
        "out_gain": jnp.clip(1.0 + 0.18 * jax.random.normal(splits[9], (HD,), jnp.float32), 0.1, 1.9),
        "w_out": centred(splits[10], (HEADS * HD, D), (HEADS * HD) ** -0.5, 0.1875, ((0, 4), (1, 4))),
        "state": centred(part_keys[11], (SEQS, HD, HEADS * HD), 0.1, 0.8, ((0, 4), (2, 4)), jnp.float32),
        "prev_keys": centred(part_keys[12], (SEQS, P_SIZE, HEADS * HD), 1.0, 6.0, ((0, 4), (2, 4))),
        "prev_values": centred(part_keys[13], (SEQS, P_SIZE, HEADS * HD), 1.0, 6.0, ((0, 4), (2, 4))),
        "prev_beta": centred(part_keys[14], (SEQS, P_SIZE, HEADS), 1.5, 6.0, ((0, 4), (2, 4)), jnp.float32),
        "prev_decay": jnp.clip(-1.0 + 0.98 * jax.random.uniform(part_keys[15], (SEQS, P_SIZE, HEADS), jnp.float32) ** shard_levels(part_keys[15], (SEQS, P_SIZE, HEADS), ((0, 4), (2, 4)), -0.2, 0.2), -1.0, -0.02),
        "accepted": plant(jax.random.randint(part_keys[16], (SEQS,), 0, P_SIZE + 1), jax.random.fold_in(part_keys[16], 1), 0, P_SIZE).astype(jnp.int32),
    }


EPS = 1e-06

def normalize_rows(vector):
    return vector * lax.rsqrt(lax.optimization_barrier(jnp.sum(vector * vector, -1, keepdims=True)) + EPS)

def delta_block(saved, queries, keys_in, values_in, strength, log_decay):
    highest = lax.Precision.HIGHEST
    steps_len = queries.shape[1]
    cumul = jnp.transpose(jnp.cumsum(log_decay, axis=1), (0, 2, 1))
    q_heads = jnp.transpose(queries, (0, 2, 1, 3))
    k_heads = jnp.transpose(keys_in, (0, 2, 1, 3))
    v_heads = jnp.transpose(values_in, (0, 2, 1, 3))
    weight_t = jnp.transpose(strength, (0, 2, 1))
    spread = cumul[..., :, None] - cumul[..., None, :]
    order = jnp.arange(steps_len)
    inside = order[:, None] >= order[None, :]
    below = order[:, None] > order[None, :]
    dec_incl = jnp.where(inside, jnp.exp(jnp.where(inside, spread, 0.0)), 0.0)
    dec_strict = jnp.where(below, dec_incl, 0.0)
    lower_mat = weight_t[..., :, None] * jnp.einsum('bhik,bhjk->bhij', k_heads, k_heads, precision=highest) * dec_strict
    growth = jnp.exp(cumul)
    rhs_all = jnp.concatenate([weight_t[..., None] * v_heads, (weight_t * growth)[..., None] * k_heads], axis=-1)
    solved = []
    for row_index in range(steps_len):
        current = rhs_all[:, :, row_index]
        for col_index in range(row_index):
            current = current - lower_mat[:, :, row_index, col_index, None] * solved[col_index]
        solved.append(current)
    solution = jnp.stack(solved, axis=2)
    value_size = v_heads.shape[-1]
    update = solution[..., :value_size] - jnp.einsum('bhpk,bhkv->bhpv', solution[..., value_size:], saved, precision=highest)
    scores = jnp.einsum('bhik,bhjk->bhij', q_heads, k_heads, precision=highest) * dec_incl
    output = jnp.einsum('bhpk,bhkv->bhpv', growth[..., None] * q_heads, saved, precision=highest) + jnp.einsum('bhij,bhjv->bhiv', scores, update, precision=highest)
    tail = jnp.exp(cumul[..., -1:] - cumul)[..., None] * k_heads
    renewed = jnp.exp(cumul[..., -1])[..., None, None] * saved + jnp.einsum('bhpk,bhpv->bhkv', tail, update, precision=highest)
    return (jnp.transpose(output, (0, 2, 1, 3)), renewed)

def reference(tokens, in_gain, w_query, w_key, w_value, w_gate, w_beta, w_decay, decay_base, out_gain, w_out, state, prev_keys, prev_values, prev_beta, prev_decay, accepted):
    rows = SEQS * P_SIZE
    wide = tokens.astype(jnp.float32)
    normed = (wide * lax.rsqrt(lax.optimization_barrier(jnp.mean(wide * wide, -1, keepdims=True)) + EPS) * in_gain).astype(jnp.bfloat16)
    flat = normed.reshape(rows, D)
    shape4 = (SEQS, P_SIZE, HEADS, HD)
    query = normalize_rows(jnp.dot(flat, w_query, preferred_element_type=jnp.float32).reshape(shape4)) * HD ** (-0.5)
    key_vec = normalize_rows(jnp.dot(flat, w_key, preferred_element_type=jnp.float32).reshape(shape4))
    value_vec = jnp.dot(flat, w_value, preferred_element_type=jnp.float32).reshape(shape4)
    gate = jnp.dot(flat, w_gate, preferred_element_type=jnp.float32).reshape(shape4)
    strength = jax.nn.sigmoid(jnp.dot(flat, w_beta, preferred_element_type=jnp.float32)).reshape(SEQS, P_SIZE, HEADS)
    log_decay = (-decay_base * jax.nn.softplus(jnp.dot(flat, w_decay, preferred_element_type=jnp.float32))).reshape(SEQS, P_SIZE, HEADS)
    live = (jnp.arange(P_SIZE, dtype=jnp.int32)[None, :] < accepted[:, None]).astype(jnp.float32)
    prev_strength = jax.nn.sigmoid(prev_beta) * live[..., None]
    prev_log = prev_decay * live[..., None]
    prev_k = normalize_rows(prev_keys.astype(jnp.float32).reshape(shape4))
    prev_v = prev_values.astype(jnp.float32).reshape(shape4)
    saved = jnp.transpose(state.reshape(SEQS, HD, HEADS, HD), (0, 2, 1, 3))

    def per_block(inputs):
        held, pk_in, pv_in, pb_in, pg_in, qu_in, ke_in, va_in, st_in, lg_in = inputs
        committed = delta_block(held, pk_in, pk_in, pv_in, pb_in, pg_in)[1]
        output = delta_block(committed, qu_in, ke_in, va_in, st_in, lg_in)[0]
        return (output, committed)
    pieces = (saved, prev_k, prev_v, prev_strength, prev_log, query, key_vec, value_vec, strength, log_decay)
    blocked = tuple((array.reshape((N_KV, SEQ_DEV) + array.shape[1:]) for array in pieces))
    output, committed = lax.map(per_block, blocked)
    output = output.reshape(shape4)
    committed = committed.reshape(SEQS, HEADS, HD, HD)
    gated = (output * lax.rsqrt(lax.optimization_barrier(jnp.mean(output * output, -1, keepdims=True)) + EPS) * out_gain * jax.nn.silu(gate)).astype(jnp.bfloat16).reshape(rows, HEADS * HD)
    mixed = jnp.dot(gated, w_out, preferred_element_type=jnp.float32).astype(jnp.bfloat16).reshape(SEQS, P_SIZE, D)
    new_state = jnp.transpose(committed, (0, 2, 1, 3)).reshape(SEQS, HD, HEADS * HD)
    return (mixed, new_state)
```

```python
import functools

import jax
import jax.numpy as jnp
from jax import lax
from jax.experimental import pallas as pl
from jax.experimental.pallas import tpu as pltpu
from jax.sharding import PartitionSpec as P

EPS = 1e-06
F32 = jnp.float32
BF16 = jnp.bfloat16
MESH = pl.DeviceIdType.MESH


def kernel(
    cfg,
    tok_hbm, gain_hbm, wq_hbm, wk_hbm, wv_hbm, wg_hbm, wb_hbm, wd_hbm, base_hbm, og_hbm, wo_hbm,
    state_hbm, pk_hbm, pv_hbm, pb_hbm, pd_hbm, acc_hbm,
    mixed_ref, new_hbm,
    gain_ref, wb_ref, wd_ref, base_ref, og_ref, pk_ref, pv_ref, pb_ref, pd_ref, acc_ref, tok, wp, wo, st, normed, kq, res, tk, up, al, rows_a, rows_b, proj, send_buf, recv_buf, gate_buf, own_share,
    in_sem, own_sem, zr_send, zl_send, z_recv, y_send, y_recv, t_send, t_recv, r_send, r_recv,
    out_sem, small_sem,
):
    n_grp, n_kv, n_tp, seqs, props, heads, hd, gather_out = cfg
    width = heads * hd
    g = lax.axis_index("grp")
    k = lax.axis_index("kv")
    t_me = lax.axis_index("tp")
    rows = seqs * props
    own_rows = wk_hbm.shape[0]
    piece = own_rows // n_grp
    out_piece = wo.shape[1] // n_grp
    sources = [wk_hbm, wq_hbm, wv_hbm, wg_hbm]
    n_mat = len(sources) + (1 if gather_out else 0)

    tok_in = pltpu.make_async_copy(tok_hbm, tok.at[t_me], in_sem.at[0])
    tok_in.start()
    own_copies = []
    for m in range(n_mat):
        if m < len(sources):
            dst = wp.at[m, pl.ds(k * own_rows, own_rows), :]
            copy = pltpu.make_async_copy(sources[m], dst, own_sem.at[m])
        else:
            copy = pltpu.make_async_copy(wo_hbm, wo.at[k], own_sem.at[m])
        copy.start()
        own_copies.append(copy)
    early, late = [], []
    pairs = [
        (pk_hbm, pk_ref, early), (pv_hbm, pv_ref, early), (pb_hbm, pb_ref, early),
        (pd_hbm, pd_ref, early), (acc_hbm, acc_ref, early), (gain_hbm, gain_ref, late),
        (wb_hbm, wb_ref, late), (wd_hbm, wd_ref, late), (base_hbm, base_ref, late),
        (og_hbm, og_ref, late),
    ]
    for i, (src, dst, group) in enumerate(pairs):
        copy = pltpu.make_async_copy(src, dst, small_sem.at[i])
        copy.start()
        group.append(copy)
    state_in = pltpu.make_async_copy(state_hbm, st, in_sem.at[1])
    state_in.start()
    out_in = None
    if not gather_out:
        out_in = pltpu.make_async_copy(wo_hbm, wo, own_sem.at[n_mat])
        out_in.start()

    barrier = pltpu.get_barrier_semaphore()

    def greet(dev):
        pl.semaphore_signal(barrier, inc=1, device_id=dev, device_id_type=MESH)

    @pl.when(k > 0)
    def _():
        greet({"kv": k - 1})

    @pl.when(k < n_kv - 1)
    def _():
        greet({"kv": k + 1})

    for d in range(1, n_grp):
        greet({"grp": lax.rem(g + d, n_grp)})
    for d in range(1, n_tp):
        greet({"tp": lax.rem(t_me + d, n_tp)})

    beside = jnp.minimum(k, 1) + jnp.minimum(n_kv - 1 - k, 1)
    pl.semaphore_wait(barrier, n_grp + n_tp - 2 + beside)

    def slot(m, origin, part):
        if m < len(sources):
            return wp.at[m, pl.ds(origin * own_rows + part * piece, piece), :]
        return wo.at[origin, pl.ds(part * out_piece, out_piece), :]

    def z_right(m, origin):
        ref = slot(m, origin, g)
        return pltpu.make_async_remote_copy(
            ref, ref, zr_send.at[m, origin], z_recv.at[m, origin],
            device_id={"kv": k + 1}, device_id_type=MESH)

    def z_left(m, origin):
        ref = slot(m, origin, g)
        return pltpu.make_async_remote_copy(
            ref, ref, zl_send.at[m, origin], z_recv.at[m, origin],
            device_id={"kv": k - 1}, device_id_type=MESH)

    def y_copy(m, origin, d):
        ref = slot(m, origin, g)
        return pltpu.make_async_remote_copy(
            ref, ref, y_send.at[d - 1, m, origin], y_recv.at[d - 1, m, origin],
            device_id={"grp": lax.rem(g + d, n_grp)}, device_id_type=MESH)

    def y_wait(m, origin, d):
        ref = slot(m, origin, lax.rem(g + n_grp - d, n_grp))
        pltpu.make_async_remote_copy(
            ref, ref, y_send.at[d - 1, m, origin], y_recv.at[d - 1, m, origin],
            device_id={"grp": lax.rem(g + d, n_grp)}, device_id_type=MESH).wait_recv()

    def send_own(m):
        own_copies[m].wait()

        @pl.when(k < n_kv - 1)
        def _():
            z_right(m, k).start()

        @pl.when(k > 0)
        def _():
            z_left(m, k).start()

    def forward_step(m, s):
        left = k - 1 - s
        right = k + 1 + s

        @pl.when(left >= 0)
        def _():
            z_right(m, left).wait_recv()

            @pl.when(k < n_kv - 1)
            def _():
                z_right(m, left).start()

            for d in range(1, n_grp):
                y_copy(m, left, d).start()

        @pl.when(right < n_kv)
        def _():
            z_left(m, right).wait_recv()

            @pl.when(k > 0)
            def _():
                z_left(m, right).start()

            for d in range(1, n_grp):
                y_copy(m, right, d).start()

    def forward(m):
        def step(s, carry):
            forward_step(m, s)
            return carry

        lax.fori_loop(0, n_kv - 1, step, 0)

    def wait_y(m):
        def step(o, carry):
            @pl.when(o != k)
            def _():
                for d in range(1, n_grp):
                    y_wait(m, o, d)

            return carry

        lax.fori_loop(0, n_kv, step, 0)

    def t_copy(d):
        return pltpu.make_async_remote_copy(
            tok.at[t_me], tok.at[t_me], t_send.at[d - 1], t_recv.at[d - 1],
            device_id={"tp": lax.rem(t_me + d, n_tp)}, device_id_type=MESH)

    def t_wait(d):
        origin = lax.rem(t_me + n_tp - d, n_tp)
        pltpu.make_async_remote_copy(
            tok.at[origin], tok.at[origin], t_send.at[d - 1], t_recv.at[d - 1],
            device_id={"tp": lax.rem(t_me + d, n_tp)}, device_id_type=MESH).wait_recv()

    send_own(0)
    tok_in.wait()
    for d in range(1, n_tp):
        t_copy(d).start()
    send_own(1)
    send_own(2)

    blk = (
        lax.broadcasted_iota(jnp.int32, (width, width), 0) // hd
        == lax.broadcasted_iota(jnp.int32, (width, width), 1) // hd
    ).astype(F32).astype(BF16)
    lane_head = lax.broadcasted_iota(jnp.int32, (1, width), 1) // hd
    masks = [(lane_head == h).astype(F32) for h in range(heads)]

    def head_sum(x):
        hi = x.astype(BF16)
        lo = (x - hi.astype(F32)).astype(BF16)
        return jnp.dot(hi, blk, preferred_element_type=F32) + jnp.dot(
            lo, blk, preferred_element_type=F32)

    lanes = 128
    blocks = width // lanes

    def rd(ref, at, *lead):
        return jnp.concatenate([ref[(*lead, c, at)] for c in range(blocks)], axis=-1)

    def wr(ref, at, x, *lead):
        for c in range(blocks):
            ref[(*lead, c, at)] = x[:, c * lanes : (c + 1) * lanes]

    every = pl.ds(0, rows)

    pad = 2 * props

    def by_state(s, carry):
        tile = st[pl.ds(pl.multiple_of(s * hd, hd), hd), :]
        stacked = jnp.concatenate([(tile * mask).astype(BF16) for mask in masks], axis=0)
        at = pl.ds(pl.multiple_of(s * pad, pad), pad)
        lhs = rd(kq, at).astype(BF16)
        wr(res, at, jnp.dot(lhs, stacked, preferred_element_type=F32))
        return carry

    def solve(keys, values, weights, logs, queries):
        cumul = []
        run = None
        for t in range(props):
            run = logs[t] if run is None else run + logs[t]
            cumul.append(run)
        low = [(i, j) for i in range(props) for j in range(i)]
        products = [keys[i] * keys[j] for i, j in low]
        full = []
        if queries is not None:
            full = [(i, j) for i in range(props) for j in range(i + 1)]
            products += [queries[i] * keys[j] for i, j in full]
        sums = head_sum(jnp.concatenate(products, axis=0))
        sums = [sums[i * seqs : (i + 1) * seqs] for i in range(len(products))]
        kk = dict(zip(low, sums))
        qk = dict(zip(full, sums[len(low):]))
        dec = {pair: jnp.exp(cumul[pair[0]] - cumul[pair[1]]) for pair in low}
        growth = [jnp.exp(c) for c in cumul]
        update = []
        for t in range(props):
            seen = rd(res, pl.ds(t, seqs, stride=pad))
            term = values[t] - growth[t] * seen
            for j in range(t):
                term = term - kk[t, j] * dec[t, j] * update[j]
            update.append(weights[t] * term)
        outs = []
        if queries is not None:
            for t in range(props):
                out = growth[t] * rd(res, pl.ds(props + t, seqs, stride=pad))
                for j in range(t + 1):
                    score = qk[t, j] if j == t else qk[t, j] * dec[t, j]
                    out = out + score * update[j]
                outs.append(out)
        return cumul, growth, update, outs

    def split(ref):
        return [rd(ref, pl.ds(t, seqs, stride=props)) for t in range(props)]

    for copy in early:
        copy.wait()
    pk = pk_ref[...].astype(F32).reshape(rows, width)
    wr(rows_a, every, pk * lax.rsqrt(head_sum(pk * pk) + EPS))
    wr(rows_b, every, pv_ref[...].astype(F32).reshape(rows, width))
    keys = split(rows_a)
    values = split(rows_b)
    own_head = (
        lax.broadcasted_iota(jnp.int32, (heads, width), 0)
        == lax.broadcasted_iota(jnp.int32, (heads, width), 1) // hd
    ).astype(F32)

    def over_lanes(x):
        return lax.dot_general(
            x, own_head, (((0,), (0,)), ((), ())),
            precision=lax.Precision.HIGHEST, preferred_element_type=F32)

    weights, logs = [], []
    for t in range(props):
        live = (acc_ref[...] > t).astype(F32)
        weights.append(over_lanes(jax.nn.sigmoid(pb_ref[t]) * live))
        logs.append(over_lanes(pd_ref[t] * live))
        wr(kq, pl.ds(t, seqs, stride=pad), keys[t])
        wr(kq, pl.ds(props + t, seqs, stride=pad), keys[t])
    state_in.wait()
    lax.fori_loop(0, seqs, by_state, 0, unroll=4)
    cumul, growth, update, _ = solve(keys, values, weights, logs, None)
    al[...] = growth[-1]
    for t in range(props):
        wr(tk, pl.ds(t, seqs, stride=pad), jnp.exp(cumul[-1] - cumul[t]) * keys[t])
        wr(up, pl.ds(t, seqs, stride=pad), update[t])
        wr(tk, pl.ds(props + t, seqs, stride=pad), jnp.zeros((seqs, width), F32))
        wr(up, pl.ds(props + t, seqs, stride=pad), jnp.zeros((seqs, width), F32))

    def renew(s, carry):
        at = pl.ds(pl.multiple_of(s * pad, pad), pad)
        outer = lax.dot_general(
            rd(tk, at), rd(up, at), (((0,), (0,)), ((), ())), preferred_element_type=F32)
        where = pl.ds(pl.multiple_of(s * hd, hd), hd)
        tile = al[pl.ds(s, 1), :] * st[where, :]
        for h in range(heads):
            tile = tile + masks[h] * outer[h * hd : (h + 1) * hd, :]
        st[where, :] = tile
        return carry

    forward(0)
    send_own(3)
    lax.fori_loop(0, seqs // 2, renew, 0, unroll=2)
    forward(1)
    if gather_out:
        send_own(n_mat - 1)
    lax.fori_loop(seqs // 2, seqs, renew, 0, unroll=2)
    state_out = pltpu.make_async_copy(st, new_hbm, out_sem)
    state_out.start()

    for d in range(1, n_tp):
        t_wait(d)
    for copy in late:
        copy.wait()
    square = jnp.zeros((rows, 1), F32)
    for i in range(n_tp):
        wide = tok[i].astype(F32).reshape(rows, -1)
        square = square + jnp.sum(wide * wide, -1, keepdims=True)
    feats = tok.shape[3]
    scale = lax.rsqrt(square / (n_tp * feats) + EPS)
    for i in range(n_tp):
        cols = slice(i * feats, (i + 1) * feats)
        normed[:, cols] = (tok[i].astype(F32).reshape(rows, -1) * scale * gain_ref[:, cols]).astype(BF16)
    all_heads = wb_ref.shape[0]
    pick = (
        lax.broadcasted_iota(jnp.int32, (all_heads, width), 0)
        == t_me * heads + lax.broadcasted_iota(jnp.int32, (all_heads, width), 1) // hd
    ).astype(F32)

    def per_head(ref):
        raw = lax.dot_general(
            normed[...], ref[...], (((1,), (1,)), ((), ())), preferred_element_type=F32)
        return jnp.dot(raw, pick, precision=lax.Precision.HIGHEST, preferred_element_type=F32)

    wr(rows_a, every, jax.nn.sigmoid(per_head(wb_ref)))
    weights = split(rows_a)
    base = jnp.zeros((1, width), F32)
    for h in range(heads):
        base = jnp.where(lane_head == h, base_ref[:, h : h + 1], base)
    wr(rows_b, every, -base * jax.nn.softplus(per_head(wd_ref)))
    logs = split(rows_b)

    def project(m):
        return jnp.dot(normed[...], wp[m], preferred_element_type=F32)

    def finish(m):
        wait_y(m)
        if m < len(sources):
            value = project(m)
            if m == 0:
                value = value * lax.rsqrt(head_sum(value * value) + EPS)
            elif m == 1:
                value = value * lax.rsqrt(head_sum(value * value) + EPS) * hd ** (-0.5)
            wr(proj, every, value, m)

    outs = None
    def r_copy(dest):
        return pltpu.make_async_remote_copy(
            send_buf.at[dest], recv_buf.at[t_me], r_send.at[dest], r_recv.at[t_me],
            device_id={"tp": dest}, device_id_type=MESH)

    def r_wait(origin):
        pltpu.make_async_remote_copy(
            send_buf.at[origin], recv_buf.at[origin], r_send.at[origin], r_recv.at[origin],
            device_id={"tp": origin}, device_id_type=MESH).wait_recv()

    def send_share(dest):
        share = jnp.dot(gate_buf[...], wo[dest], preferred_element_type=F32)

        @pl.when(dest == t_me)
        def _():
            own_share[...] = share

        @pl.when(dest != t_me)
        def _():
            send_buf[dest] = share.astype(BF16)
            r_copy(dest).start()

    for m in range(len(sources)):
        if m >= 2:
            forward(m)
        if m >= 1:
            finish(m - 1)
        if m == 3:
            keys = [rd(proj, pl.ds(t, seqs, stride=props), 0) for t in range(props)]
            queries = [rd(proj, pl.ds(t, seqs, stride=props), 1) for t in range(props)]
            values = [rd(proj, pl.ds(t, seqs, stride=props), 2) for t in range(props)]
            for t in range(props):
                wr(kq, pl.ds(t, seqs, stride=pad), keys[t])
                wr(kq, pl.ds(props + t, seqs, stride=pad), queries[t])
            lax.fori_loop(0, seqs, by_state, 0, unroll=4)
            outs = solve(keys, values, weights, logs, queries)[3]
            for t in range(props):
                wr(rows_a, pl.ds(t, seqs, stride=props), outs[t])
            out = rd(rows_a, every)
            out = out * lax.rsqrt(head_sum(out * out) / hd + EPS)
            tile_gain = (
                lax.broadcasted_iota(jnp.int32, (hd, width), 0)
                == lax.broadcasted_iota(jnp.int32, (hd, width), 1) % hd
            ).astype(F32)
            gain = jnp.dot(
                jnp.broadcast_to(og_ref[...], (8, hd)), tile_gain,
                precision=lax.Precision.HIGHEST, preferred_element_type=F32)[:1]
            wr(rows_a, every, out * gain)
    finish(len(sources) - 1)
    gate = rd(proj, every, 3)
    gate_buf[...] = (rd(rows_a, every) * (gate / (1.0 + jnp.exp(-gate)))).astype(BF16)
    if gather_out:
        m = n_mat - 1

        def take(s, carry):
            @pl.when(s < n_kv - 1)
            def _():
                forward_step(m, s)

            @pl.when(k - s >= 0)
            def _():
                @pl.when(s > 0)
                def _():
                    for d in range(1, n_grp):
                        y_wait(m, k - s, d)

                send_share(k - s)

            @pl.when(jnp.logical_and(s > 0, k + s < n_kv))
            def _():
                for d in range(1, n_grp):
                    y_wait(m, k + s, d)
                send_share(k + s)

            return carry

        lax.fori_loop(0, n_kv, take, 0)
    else:
        out_in.wait()
        for d in range(n_tp):
            send_share(lax.rem(t_me + d, n_tp))
    total = own_share[...]
    for d in range(1, n_tp):
        origin = lax.rem(t_me + d, n_tp)
        r_wait(origin)
        total = total + recv_buf[origin].astype(F32)
    mixed_ref[...] = total.reshape(seqs, props, feats).astype(BF16)

    for d in range(1, n_tp):
        t_copy(d).wait_send()
        r_copy(lax.rem(t_me + d, n_tp)).wait_send()

    def drain(m):
        def step(o, carry):
            @pl.when(jnp.logical_and(o <= k, k < n_kv - 1))
            def _():
                z_right(m, o).wait_send()

            @pl.when(jnp.logical_and(o >= k, k > 0))
            def _():
                z_left(m, o).wait_send()

            @pl.when(o != k)
            def _():
                for d in range(1, n_grp):
                    y_copy(m, o, d).wait_send()

            return carry

        lax.fori_loop(0, n_kv, step, 0)

    for m in range(n_mat):
        drain(m)
    state_out.wait()


def pair_kernel(
    cfg,
    tok_hbm, gain_hbm, wq_hbm, wk_hbm, wv_hbm, wg_hbm, wb_hbm, wd_hbm, base_hbm, og_hbm, wo_hbm,
    state_hbm, pk_hbm, pv_hbm, pb_hbm, pd_hbm, acc_hbm,
    mixed_ref, new_hbm,
    gain_ref, wbd_ref, base_ref, og_ref, pk_ref, pv_ref, pb_ref, pd_ref, acc_ref, tok, wp, wo, st, normed, kq, res, tk, up, al, rows_a, rows_b, proj, own_part, part_send, part_recv, small_own, small_send, small_recv, send_buf, recv_buf, gate_buf, own_share,
    in_sem, own_sem, wz_send, wz_recv, wy_send, wy_recv, t_send, f_send, t_recv, zr_send, zl_send, z_recv, y_send, y_recv, p_send, p_recv, r_send, r_recv,
    out_sem, small_sem,
):
    n_grp, n_kv, n_tp, seqs, props, heads, hd = cfg
    width = heads * hd
    g = lax.axis_index("grp")
    k = lax.axis_index("kv")
    t_me = lax.axis_index("tp")
    rows = seqs * props
    own_rows = wk_hbm.shape[0]
    piece = own_rows // n_grp
    out_piece = wo.shape[1] // n_grp
    feats = tok_hbm.shape[2]
    sources = [wk_hbm, wq_hbm, wv_hbm, wg_hbm]
    n_src = len(sources)
    all_heads = wb_hbm.shape[0]
    pair = k // 2
    side = lax.rem(k, 2)
    mate = k + 1 - 2 * side
    partner = lax.rem(k + n_kv // 2, n_kv)
    chip = t_me // 2
    core = lax.rem(t_me, 2)
    beside_core = 2 * chip + 1 - core
    home = lax.rem(pair + chip + 1, 2)
    g_other = lax.rem(g + 1, n_grp)
    half_feats = 2 * feats

    own_slot = home * (2 + core) + (1 - home) * 4
    tok_in = pltpu.make_async_copy(tok_hbm, tok.at[own_slot], in_sem.at[0])
    tok_in.start()
    own_copies = []
    for m in range(n_src + 1):
        if m < n_src:
            dst = wp.at[m, pl.ds(side * own_rows, own_rows), :]
            copy = pltpu.make_async_copy(sources[m], dst, own_sem.at[m])
        else:
            copy = pltpu.make_async_copy(wo_hbm, wo.at[k], own_sem.at[m])
        copy.start()
        own_copies.append(copy)
    early, late = [], []
    ours = pl.ds(pl.multiple_of(pair * half_feats, half_feats), half_feats)
    pairs = [
        (pk_hbm, pk_ref, early), (pv_hbm, pv_ref, early), (pb_hbm, pb_ref, early),
        (pd_hbm, pd_ref, early), (acc_hbm, acc_ref, early),
        (gain_hbm.at[:, ours], gain_ref, late),
        (wb_hbm.at[:, ours], wbd_ref.at[pl.ds(0, all_heads), :], late),
        (wd_hbm.at[:, ours], wbd_ref.at[pl.ds(all_heads, all_heads), :], late),
        (base_hbm, base_ref, late), (og_hbm, og_ref, late),
    ]
    for i, (src, dst, group) in enumerate(pairs):
        copy = pltpu.make_async_copy(src, dst, small_sem.at[i])
        copy.start()
        group.append(copy)
    state_in = pltpu.make_async_copy(state_hbm, st, in_sem.at[1])
    state_in.start()

    barrier = pltpu.get_barrier_semaphore()

    def greet(dev):
        pl.semaphore_signal(barrier, inc=1, device_id=dev, device_id_type=MESH)

    for d in range(1, n_kv):
        greet({"kv": lax.rem(k + d, n_kv)})
    for d in range(1, n_tp):
        greet({"tp": lax.rem(t_me + d, n_tp)})
    greet({"grp": g_other})
    far_tp = 2 * (1 - chip) + core
    greet({"kv": partner, "tp": far_tp})
    pl.semaphore_wait(barrier, n_kv + n_tp)

    def remote(src, dst, send, recv, dev):
        return pltpu.make_async_remote_copy(
            src, dst, send, recv, device_id=dev, device_id_type=MESH)

    to_slot = core + 2 * home
    to_kv = lax.rem(k + (1 - home) * (n_kv // 2), n_kv)
    to_tp = 2 * chip + home * (1 - core) + (1 - home) * core

    def tok_far():
        return remote(tok.at[own_slot], tok.at[to_slot], t_send.at[0], t_recv.at[to_slot],
                      {"kv": to_kv, "tp": far_tp})

    def tok_near():
        return remote(tok.at[own_slot], tok.at[to_slot], t_send.at[1], t_recv.at[to_slot],
                      {"kv": to_kv, "tp": to_tp})

    def tok_relay(j):
        slot = 2 * j + core
        return remote(tok.at[slot], tok.at[slot], f_send.at[j], t_recv.at[slot],
                      {"tp": beside_core})

    def tok_wait(slot):
        remote(tok.at[slot], tok.at[slot], f_send.at[0], t_recv.at[slot],
               {"tp": beside_core}).wait_recv()

    def w_slot(m, block, half):
        return wp.at[m, pl.ds(block * own_rows + half * piece, piece), :]

    def w_mate(m):
        ref = w_slot(m, side, g)
        return remote(ref, ref, wz_send.at[m], wz_recv.at[m], {"kv": mate})

    def w_share(m):
        ref = w_slot(m, 1 - side, g)
        return remote(ref, ref, wy_send.at[m], wy_recv.at[m], {"grp": g_other})

    def w_pass(m):
        ref = w_slot(m, 1 - side, g)
        remote(ref, ref, wz_send.at[m], wz_recv.at[m], {"kv": mate}).wait_recv()
        w_share(m).start()

    def w_ready(m):
        ref = w_slot(m, 1 - side, g_other)
        remote(ref, ref, wy_send.at[m], wy_recv.at[m], {"grp": g_other}).wait_recv()

    def o_slot(origin, part):
        return wo.at[origin, pl.ds(part * out_piece, out_piece), :]

    def z_right(origin):
        ref = o_slot(origin, g)
        return remote(ref, ref, zr_send.at[origin], z_recv.at[origin], {"kv": k + 1})

    def z_left(origin):
        ref = o_slot(origin, g)
        return remote(ref, ref, zl_send.at[origin], z_recv.at[origin], {"kv": k - 1})

    def y_copy(origin):
        ref = o_slot(origin, g)
        return remote(ref, ref, y_send.at[origin], y_recv.at[origin], {"grp": g_other})

    def y_wait(origin):
        ref = o_slot(origin, g_other)
        remote(ref, ref, y_send.at[origin], y_recv.at[origin], {"grp": g_other}).wait_recv()

    def forward_step(s):
        left = k - 1 - s
        right = k + 1 + s

        @pl.when(left >= 0)
        def _():
            z_right(left).wait_recv()

            @pl.when(k < n_kv - 1)
            def _():
                z_right(left).start()

            y_copy(left).start()

        @pl.when(right < n_kv)
        def _():
            z_left(right).wait_recv()

            @pl.when(k > 0)
            def _():
                z_left(right).start()

            y_copy(right).start()

    def p_copy(m):
        return remote(part_send.at[m], part_recv.at[m], p_send.at[m], p_recv.at[m],
                      {"kv": partner})

    def small_copy():
        return remote(small_send, small_recv, p_send.at[n_src], p_recv.at[n_src],
                      {"kv": partner})

    tok_in.wait()
    tok_far().start()
    tok_near().start()
    for m in range(n_src):
        own_copies[m].wait()
        w_mate(m).start()
    own_copies[n_src].wait()

    @pl.when(k < n_kv - 1)
    def _():
        z_right(k).start()

    @pl.when(k > 0)
    def _():
        z_left(k).start()

    blk = (
        lax.broadcasted_iota(jnp.int32, (width, width), 0) // hd
        == lax.broadcasted_iota(jnp.int32, (width, width), 1) // hd
    ).astype(F32).astype(BF16)
    lane_head = lax.broadcasted_iota(jnp.int32, (1, width), 1) // hd
    masks = [(lane_head == h).astype(F32) for h in range(heads)]

    def head_sum(x):
        hi = x.astype(BF16)
        lo = (x - hi.astype(F32)).astype(BF16)
        return jnp.dot(hi, blk, preferred_element_type=F32) + jnp.dot(
            lo, blk, preferred_element_type=F32)

    lanes = 128
    blocks = width // lanes

    def rd(ref, at, *lead):
        return jnp.concatenate([ref[(*lead, c, at)] for c in range(blocks)], axis=-1)

    def wr(ref, at, x, *lead):
        for c in range(blocks):
            ref[(*lead, c, at)] = x[:, c * lanes : (c + 1) * lanes]

    every = pl.ds(0, rows)

    pad = 2 * props

    def by_state(s, carry):
        tile = st[pl.ds(pl.multiple_of(s * hd, hd), hd), :]
        stacked = jnp.concatenate([(tile * mask).astype(BF16) for mask in masks], axis=0)
        at = pl.ds(pl.multiple_of(s * pad, pad), pad)
        lhs = rd(kq, at).astype(BF16)
        wr(res, at, jnp.dot(lhs, stacked, preferred_element_type=F32))
        return carry

    def solve(keys, values, weights, logs, queries):
        cumul = []
        run = None
        for t in range(props):
            run = logs[t] if run is None else run + logs[t]
            cumul.append(run)
        low = [(i, j) for i in range(props) for j in range(i)]
        products = [keys[i] * keys[j] for i, j in low]
        full = []
        if queries is not None:
            full = [(i, j) for i in range(props) for j in range(i + 1)]
            products += [queries[i] * keys[j] for i, j in full]
        sums = head_sum(jnp.concatenate(products, axis=0))
        sums = [sums[i * seqs : (i + 1) * seqs] for i in range(len(products))]
        kk = dict(zip(low, sums))
        qk = dict(zip(full, sums[len(low):]))
        dec = {pair: jnp.exp(cumul[pair[0]] - cumul[pair[1]]) for pair in low}
        growth = [jnp.exp(c) for c in cumul]
        update = []
        for t in range(props):
            seen = rd(res, pl.ds(t, seqs, stride=pad))
            term = values[t] - growth[t] * seen
            for j in range(t):
                term = term - kk[t, j] * dec[t, j] * update[j]
            update.append(weights[t] * term)
        outs = []
        if queries is not None:
            for t in range(props):
                out = growth[t] * rd(res, pl.ds(props + t, seqs, stride=pad))
                for j in range(t + 1):
                    score = qk[t, j] if j == t else qk[t, j] * dec[t, j]
                    out = out + score * update[j]
                outs.append(out)
        return cumul, growth, update, outs

    def split(ref):
        return [rd(ref, pl.ds(t, seqs, stride=props)) for t in range(props)]

    for copy in early:
        copy.wait()
    pk = pk_ref[...].astype(F32).reshape(rows, width)
    wr(rows_a, every, pk * lax.rsqrt(head_sum(pk * pk) + EPS))
    wr(rows_b, every, pv_ref[...].astype(F32).reshape(rows, width))
    keys = split(rows_a)
    values = split(rows_b)
    own_head = (
        lax.broadcasted_iota(jnp.int32, (heads, width), 0)
        == lax.broadcasted_iota(jnp.int32, (heads, width), 1) // hd
    ).astype(F32)

    def over_lanes(x):
        return lax.dot_general(
            x, own_head, (((0,), (0,)), ((), ())),
            precision=lax.Precision.HIGHEST, preferred_element_type=F32)

    weights, logs = [], []
    for t in range(props):
        live = (acc_ref[...] > t).astype(F32)
        weights.append(over_lanes(jax.nn.sigmoid(pb_ref[t]) * live))
        logs.append(over_lanes(pd_ref[t] * live))
        wr(kq, pl.ds(t, seqs, stride=pad), keys[t])
        wr(kq, pl.ds(props + t, seqs, stride=pad), keys[t])
    state_in.wait()
    lax.fori_loop(0, seqs, by_state, 0, unroll=4)
    cumul, growth, update, _ = solve(keys, values, weights, logs, None)
    al[...] = growth[-1]
    for t in range(props):
        wr(tk, pl.ds(t, seqs, stride=pad), jnp.exp(cumul[-1] - cumul[t]) * keys[t])
        wr(up, pl.ds(t, seqs, stride=pad), update[t])
        wr(tk, pl.ds(props + t, seqs, stride=pad), jnp.zeros((seqs, width), F32))
        wr(up, pl.ds(props + t, seqs, stride=pad), jnp.zeros((seqs, width), F32))

    def renew(s, carry):
        at = pl.ds(pl.multiple_of(s * pad, pad), pad)
        outer = lax.dot_general(
            rd(tk, at), rd(up, at), (((0,), (0,)), ((), ())), preferred_element_type=F32)
        where = pl.ds(pl.multiple_of(s * hd, hd), hd)
        tile = al[pl.ds(s, 1), :] * st[where, :]
        for h in range(heads):
            tile = tile + masks[h] * outer[h * hd : (h + 1) * hd, :]
        st[where, :] = tile
        return carry

    w_pass(0)

    @pl.when(home == 0)
    def _():
        tok_wait(2 + core)
        tok_relay(1).start()

    lax.fori_loop(0, seqs // 2, renew, 0, unroll=2)
    w_pass(1)
    tok_wait(core)
    tok_relay(0).start()
    lax.fori_loop(seqs // 2, seqs, renew, 0, unroll=2)
    state_out = pltpu.make_async_copy(st, new_hbm, out_sem)
    state_out.start()
    for copy in late:
        copy.wait()
    w_pass(2)
    tok_wait(1 - core)
    tok_wait(3 - core)
    ones = jnp.ones((8, feats), BF16)
    squares = jnp.zeros((8, 2 * rows), F32)
    last = (((1,), (1,)), ((), ()))
    for c in range(2):
        cols = slice(c * feats, (c + 1) * feats)
        wide = jnp.concatenate(
            [tok[c].astype(F32).reshape(rows, feats), tok[2 + c].astype(F32).reshape(rows, feats)],
            axis=0)
        normed[:, cols] = (wide * gain_ref[:, cols]).astype(BF16)
        sq = wide * wide
        hi = sq.astype(BF16)
        lo = (sq - hi.astype(F32)).astype(BF16)
        squares = squares + lax.dot_general(ones, hi, last, preferred_element_type=F32)
        squares = squares + lax.dot_general(ones, lo, last, preferred_element_type=F32)
    raw = lax.dot_general(wbd_ref[...], normed[...], last, preferred_element_type=F32)
    small = jnp.concatenate([raw, squares], axis=0)
    small_send[...] = small[:, :rows]
    small_copy().start()
    small_own[...] = small[:, rows:]

    def project(m):
        both = jnp.dot(normed[...], wp[m], preferred_element_type=F32)
        part_send[m] = both[:rows].astype(BF16)
        p_copy(m).start()
        own_part[m] = both[rows:]

    for m in range(n_src):
        w_ready(m)
        project(m)
        if m == 0:
            w_pass(3)
        else:
            forward_step(m - 1)

    pick = (
        lax.broadcasted_iota(jnp.int32, (all_heads, width), 0)
        == t_me * heads + lax.broadcasted_iota(jnp.int32, (all_heads, width), 1) // hd
    ).astype(F32)
    small_copy().wait_recv()
    small = small_own[...] + small_recv[...]
    scale = lax.rsqrt(small[2 * all_heads :] / (n_tp * feats) + EPS)
    beta = small[:all_heads] * scale[:1]
    decay = small[all_heads : 2 * all_heads] * scale[:1]

    def spread(x, over):
        return lax.dot_general(
            x, over, (((0,), (0,)), ((), ())),
            precision=lax.Precision.HIGHEST, preferred_element_type=F32)

    wr(rows_a, every, spread(jax.nn.sigmoid(beta), pick))
    weights = split(rows_a)
    base = jnp.zeros((1, width), F32)
    for h in range(heads):
        base = jnp.where(lane_head == h, base_ref[:, h : h + 1], base)
    wr(rows_b, every, -base * spread(jax.nn.softplus(decay), pick))
    logs = split(rows_b)
    row_scale = spread(
        scale, (lax.broadcasted_iota(jnp.int32, (8, width), 0) == 0).astype(F32))

    def finish(m):
        p_copy(m).wait_recv()
        value = (own_part[m] + part_recv[m].astype(F32)) * row_scale
        if m == 0:
            value = value * lax.rsqrt(head_sum(value * value) + EPS)
        elif m == 1:
            value = value * lax.rsqrt(head_sum(value * value) + EPS) * hd ** (-0.5)
        wr(proj, every, value, m)

    def r_copy(dest):
        return pltpu.make_async_remote_copy(
            send_buf.at[dest], recv_buf.at[t_me], r_send.at[dest], r_recv.at[t_me],
            device_id={"tp": dest}, device_id_type=MESH)

    def r_wait(origin):
        pltpu.make_async_remote_copy(
            send_buf.at[origin], recv_buf.at[origin], r_send.at[origin], r_recv.at[origin],
            device_id={"tp": origin}, device_id_type=MESH).wait_recv()

    def send_share(dest):
        share = jnp.dot(gate_buf[...], wo[dest], preferred_element_type=F32)

        @pl.when(dest == t_me)
        def _():
            own_share[...] = share

        @pl.when(dest != t_me)
        def _():
            send_buf[dest] = share.astype(BF16)
            r_copy(dest).start()

    for m in range(3):
        finish(m)
    keys = [rd(proj, pl.ds(t, seqs, stride=props), 0) for t in range(props)]
    queries = [rd(proj, pl.ds(t, seqs, stride=props), 1) for t in range(props)]
    values = [rd(proj, pl.ds(t, seqs, stride=props), 2) for t in range(props)]
    for t in range(props):
        wr(kq, pl.ds(t, seqs, stride=pad), keys[t])
        wr(kq, pl.ds(props + t, seqs, stride=pad), queries[t])
    lax.fori_loop(0, seqs, by_state, 0, unroll=4)
    outs = solve(keys, values, weights, logs, queries)[3]
    for t in range(props):
        wr(rows_a, pl.ds(t, seqs, stride=props), outs[t])
    out = rd(rows_a, every)
    out = out * lax.rsqrt(head_sum(out * out) / hd + EPS)
    tile_gain = (
        lax.broadcasted_iota(jnp.int32, (hd, width), 0)
        == lax.broadcasted_iota(jnp.int32, (hd, width), 1) % hd
    ).astype(F32)
    gain = jnp.dot(
        jnp.broadcast_to(og_ref[...], (8, hd)), tile_gain,
        precision=lax.Precision.HIGHEST, preferred_element_type=F32)[:1]
    wr(rows_a, every, out * gain)
    finish(n_src - 1)
    gate = rd(proj, every, 3)
    gate_buf[...] = (rd(rows_a, every) * (gate / (1.0 + jnp.exp(-gate)))).astype(BF16)

    def take(s, carry):
        @pl.when(k - s >= 0)
        def _():
            @pl.when(s > 0)
            def _():
                y_wait(k - s)

            send_share(k - s)

        @pl.when(jnp.logical_and(s > 0, k + s < n_kv))
        def _():
            y_wait(k + s)
            send_share(k + s)

        return carry

    lax.fori_loop(0, n_kv, take, 0)
    total = own_share[...]
    for d in range(1, n_tp):
        origin = lax.rem(t_me + d, n_tp)
        r_wait(origin)
        total = total + recv_buf[origin].astype(F32)
    mixed_ref[...] = total.reshape(seqs, props, feats).astype(BF16)

    tok_far().wait_send()
    tok_near().wait_send()
    tok_relay(0).wait_send()

    @pl.when(home == 0)
    def _():
        tok_relay(1).wait_send()

    for m in range(n_src):
        w_mate(m).wait_send()
        w_share(m).wait_send()
        p_copy(m).wait_send()
    small_copy().wait_send()
    for d in range(1, n_tp):
        r_copy(lax.rem(t_me + d, n_tp)).wait_send()

    def drain(o, carry):
        @pl.when(jnp.logical_and(o <= k, k < n_kv - 1))
        def _():
            z_right(o).wait_send()

        @pl.when(jnp.logical_and(o >= k, k > 0))
        def _():
            z_left(o).wait_send()

        @pl.when(o != k)
        def _():
            y_copy(o).wait_send()

        return carry

    lax.fori_loop(0, n_kv, drain, 0)
    state_out.wait()


def pair_call(sizes, args, seqs, props, feats, heads, hd, width, rows, pad):
    n_grp, n_kv, n_tp = sizes
    cfg = (n_grp, n_kv, n_tp, seqs, props, heads, hd)
    vmem = pl.BlockSpec(memory_space=pltpu.VMEM)
    hbm = pl.BlockSpec(memory_space=pltpu.HBM)
    dma = pltpu.SemaphoreType.DMA
    own_rows = args[2].shape[0]
    all_heads = args[6].shape[0]
    n_src = 4
    small = (2 * all_heads + 8, rows)
    return pl.pallas_call(
        functools.partial(pair_kernel, cfg),
        out_shape=(
            jax.ShapeDtypeStruct((seqs, props, feats), BF16),
            jax.ShapeDtypeStruct((seqs * hd, width), F32),
        ),
        in_specs=[hbm] * len(args),
        out_specs=(vmem, pl.BlockSpec(memory_space=pl.ANY)),
        scratch_shapes=[
            pltpu.VMEM((1, 2 * feats), F32),
            pltpu.VMEM((2 * all_heads, 2 * feats), BF16),
            *[pltpu.VMEM(args[i].shape, args[i].dtype) for i in (8, 9, 12, 13, 14, 15, 16)],
            pltpu.VMEM((5, seqs, props, feats), BF16),
            pltpu.VMEM((n_src, 2 * own_rows, width), BF16),
            pltpu.VMEM((n_tp, width, feats), BF16),
            pltpu.VMEM((seqs * hd, width), F32),
            pltpu.VMEM((2 * rows, 2 * feats), BF16),
            pltpu.VMEM((width // 128, seqs * pad, 128), F32),
            pltpu.VMEM((width // 128, seqs * pad, 128), F32),
            pltpu.VMEM((width // 128, seqs * pad, 128), F32),
            pltpu.VMEM((width // 128, seqs * pad, 128), F32),
            pltpu.VMEM((seqs, width), F32),
            pltpu.VMEM((width // 128, rows, 128), F32),
            pltpu.VMEM((width // 128, rows, 128), F32),
            pltpu.VMEM((n_src, width // 128, rows, 128), F32),
            pltpu.VMEM((n_src, rows, width), F32),
            pltpu.VMEM((n_src, rows, width), BF16),
            pltpu.VMEM((n_src, rows, width), BF16),
            pltpu.VMEM(small, F32),
            pltpu.VMEM(small, F32),
            pltpu.VMEM(small, F32),
            pltpu.VMEM((n_tp, rows, feats), BF16),
            pltpu.VMEM((n_tp, rows, feats), BF16),
            pltpu.VMEM((rows, width), BF16),
            pltpu.VMEM((rows, feats), F32),
            dma((2,)),
            dma((n_src + 1,)),
            *[dma((n_src,)) for _ in range(4)],
            dma((2,)),
            dma((2,)),
            dma((4,)),
            *[dma((n_kv,)) for _ in range(5)],
            dma((n_src + 1,)),
            dma((n_src + 1,)),
            dma((n_tp,)),
            dma((n_tp,)),
            dma(()),
            dma((10,)),
        ],
        compiler_params=pltpu.CompilerParams(
            collective_id=1, has_side_effects=True, vmem_limit_bytes=67043328),
    )(*args)


def body(
    sizes,
    tokens, in_gain, w_query, w_key, w_value, w_gate, w_beta, w_decay, decay_base, out_gain, w_out,
    state, prev_keys, prev_values, prev_beta, prev_decay, accepted,
):
    n_grp, n_kv, n_tp = sizes
    seqs, props, feats = tokens.shape
    heads = decay_base.shape[0]
    hd = out_gain.shape[0]
    width = heads * hd
    rows = seqs * props
    pad = 2 * props
    paired = (
        n_grp == 2 and n_kv == n_tp and n_kv // 2 == 2
        and w_query.shape[0] == feats and w_query.shape[0] * n_kv == in_gain.shape[0])
    gather_out = n_kv == n_tp
    if not gather_out:
        w_out = lax.all_gather(w_out, "kv", axis=1, tiled=True)
        w_out = jnp.transpose(w_out.reshape(width, n_tp, feats), (1, 0, 2))
    n_mat = 5 if gather_out else 4
    cfg = (n_grp, n_kv, n_tp, seqs, props, heads, hd, gather_out)
    vmem = pl.BlockSpec(memory_space=pltpu.VMEM)
    hbm = pl.BlockSpec(memory_space=pltpu.HBM)
    args = (
        tokens, in_gain.reshape(1, -1), w_query, w_key, w_value, w_gate,
        w_beta.T, w_decay.T, decay_base.reshape(1, -1), out_gain.reshape(1, -1), w_out,
        state.reshape(seqs * hd, width), prev_keys, prev_values,
        jnp.transpose(prev_beta, (1, 2, 0)), jnp.transpose(prev_decay, (1, 2, 0)),
        accepted.reshape(1, seqs),
    )
    if paired:
        mixed, new_state = pair_call(
            sizes, args, seqs, props, feats, heads, hd, width, rows, pad)
        return mixed, new_state.reshape(seqs, hd, width)
    dma = pltpu.SemaphoreType.DMA
    mixed, new_state = pl.pallas_call(
        functools.partial(kernel, cfg),
        out_shape=(
            jax.ShapeDtypeStruct((seqs, props, feats), BF16),
            jax.ShapeDtypeStruct((seqs * hd, width), F32),
        ),
        in_specs=[hbm] * len(args),
        out_specs=(vmem, pl.BlockSpec(memory_space=pl.ANY)),
        scratch_shapes=[
            *[pltpu.VMEM(args[i].shape, args[i].dtype) for i in (1, 6, 7, 8, 9, 12, 13, 14, 15, 16)],
            pltpu.VMEM((n_tp, seqs, props, feats), BF16),
            pltpu.VMEM((4, n_kv * w_key.shape[0], width), BF16),
            pltpu.VMEM((n_tp, width, feats), BF16),
            pltpu.VMEM((seqs * hd, width), F32),
            pltpu.VMEM((rows, n_tp * feats), BF16),
            pltpu.VMEM((width // 128, seqs * pad, 128), F32),
            pltpu.VMEM((width // 128, seqs * pad, 128), F32),
            pltpu.VMEM((width // 128, seqs * pad, 128), F32),
            pltpu.VMEM((width // 128, seqs * pad, 128), F32),
            pltpu.VMEM((seqs, width), F32),
            pltpu.VMEM((width // 128, rows, 128), F32),
            pltpu.VMEM((width // 128, rows, 128), F32),
            pltpu.VMEM((4, width // 128, rows, 128), F32),
            pltpu.VMEM((n_tp, rows, feats), BF16),
            pltpu.VMEM((n_tp, rows, feats), BF16),
            pltpu.VMEM((rows, width), BF16),
            pltpu.VMEM((rows, feats), F32),
            dma((2,)),
            dma((6,)),
            dma((n_mat, n_kv)),
            dma((n_mat, n_kv)),
            dma((n_mat, n_kv)),
            dma((max(n_grp - 1, 1), n_mat, n_kv)),
            dma((max(n_grp - 1, 1), n_mat, n_kv)),
            dma((n_tp - 1,)),
            dma((n_tp - 1,)),
            dma((n_tp,)),
            dma((n_tp,)),
            dma(()),
            dma((10,)),
        ],
        compiler_params=pltpu.CompilerParams(
            collective_id=0, has_side_effects=True, vmem_limit_bytes=67043328),
    )(*args)
    return mixed, new_state.reshape(seqs, hd, width)


def solution(mesh):
    sizes = (mesh.shape["grp"], mesh.shape["kv"], mesh.shape["tp"])
    tokens = P(("grp", "kv"), None, "tp")
    placed = (
        tokens, P(), P("kv", "tp"), P("kv", "tp"), P("kv", "tp"), P("kv", "tp"), P(), P(),
        P("tp"), P(), P("tp", "kv"), tokens, tokens, tokens, tokens, tokens, P(("grp", "kv")),
    )
    return jax.shard_map(
        functools.partial(body, sizes),
        mesh=mesh,
        in_specs=placed,
        out_specs=(tokens, tokens),
        check_vma=False,
    )
```

```python
import functools

import jax
import jax.numpy as jnp
from jax import lax
from jax.experimental import pallas as pl
from jax.experimental.pallas import tpu as pltpu
from jax.sharding import PartitionSpec as P

EPS = 1e-06
F32 = jnp.float32
BF16 = jnp.bfloat16
MESH = pl.DeviceIdType.MESH


def kernel(
    cfg,
    tok_hbm, gain_hbm, wq_hbm, wk_hbm, wv_hbm, wg_hbm, wb_hbm, wd_hbm, base_hbm, og_hbm, wo_hbm,
    state_hbm, pk_hbm, pv_hbm, pb_hbm, pd_hbm, acc_hbm,
    mixed_ref, new_hbm,
    gain_ref, wb_ref, wd_ref, base_ref, og_ref, pk_ref, pv_ref, pb_ref, pd_ref, acc_ref, tok, wp, wo, st, normed, kq, res, tk, up, al, rows_a, rows_b, proj, send_buf, recv_buf, gate_buf, own_share,
    in_sem, own_sem, zr_send, zl_send, z_recv, y_send, y_recv, t_send, t_recv, r_send, r_recv,
    out_sem, small_sem,
):
    n_grp, n_kv, n_tp, seqs, props, heads, hd, gather_out = cfg
    width = heads * hd
    g = lax.axis_index("grp")
    k = lax.axis_index("kv")
    t_me = lax.axis_index("tp")
    rows = seqs * props
    own_rows = wk_hbm.shape[0]
    piece = own_rows // n_grp
    out_piece = wo.shape[1] // n_grp
    sources = [wk_hbm, wq_hbm, wv_hbm, wg_hbm]
    n_mat = len(sources) + (1 if gather_out else 0)

    tok_in = pltpu.make_async_copy(tok_hbm, tok.at[t_me], in_sem.at[0])
    tok_in.start()
    own_copies = []
    for m in range(n_mat):
        if m < len(sources):
            dst = wp.at[m, pl.ds(k * own_rows, own_rows), :]
            copy = pltpu.make_async_copy(sources[m], dst, own_sem.at[m])
        else:
            copy = pltpu.make_async_copy(wo_hbm, wo.at[k], own_sem.at[m])
        copy.start()
        own_copies.append(copy)
    early, late = [], []
    pairs = [
        (pk_hbm, pk_ref, early), (pv_hbm, pv_ref, early), (pb_hbm, pb_ref, early),
        (pd_hbm, pd_ref, early), (acc_hbm, acc_ref, early), (gain_hbm, gain_ref, late),
        (wb_hbm, wb_ref, late), (wd_hbm, wd_ref, late), (base_hbm, base_ref, late),
        (og_hbm, og_ref, late),
    ]
    for i, (src, dst, group) in enumerate(pairs):
        copy = pltpu.make_async_copy(src, dst, small_sem.at[i])
        copy.start()
        group.append(copy)
    state_in = pltpu.make_async_copy(state_hbm, st, in_sem.at[1])
    state_in.start()
    out_in = None
    if not gather_out:
        out_in = pltpu.make_async_copy(wo_hbm, wo, own_sem.at[n_mat])
        out_in.start()

    barrier = pltpu.get_barrier_semaphore()

    def greet(dev):
        pl.semaphore_signal(barrier, inc=1, device_id=dev, device_id_type=MESH)

    @pl.when(k > 0)
    def _():
        greet({"kv": k - 1})

    @pl.when(k < n_kv - 1)
    def _():
        greet({"kv": k + 1})

    for d in range(1, n_grp):
        greet({"grp": lax.rem(g + d, n_grp)})
    for d in range(1, n_tp):
        greet({"tp": lax.rem(t_me + d, n_tp)})

    beside = jnp.minimum(k, 1) + jnp.minimum(n_kv - 1 - k, 1)
    pl.semaphore_wait(barrier, n_grp + n_tp - 2 + beside)

    def slot(m, origin, part):
        if m < len(sources):
            return wp.at[m, pl.ds(origin * own_rows + part * piece, piece), :]
        return wo.at[origin, pl.ds(part * out_piece, out_piece), :]

    def z_right(m, origin):
        ref = slot(m, origin, g)
        return pltpu.make_async_remote_copy(
            ref, ref, zr_send.at[m, origin], z_recv.at[m, origin],
            device_id={"kv": k + 1}, device_id_type=MESH)

    def z_left(m, origin):
        ref = slot(m, origin, g)
        return pltpu.make_async_remote_copy(
            ref, ref, zl_send.at[m, origin], z_recv.at[m, origin],
            device_id={"kv": k - 1}, device_id_type=MESH)

    def y_copy(m, origin, d):
        ref = slot(m, origin, g)
        return pltpu.make_async_remote_copy(
            ref, ref, y_send.at[d - 1, m, origin], y_recv.at[d - 1, m, origin],
            device_id={"grp": lax.rem(g + d, n_grp)}, device_id_type=MESH)

    def y_wait(m, origin, d):
        ref = slot(m, origin, lax.rem(g + n_grp - d, n_grp))
        pltpu.make_async_remote_copy(
            ref, ref, y_send.at[d - 1, m, origin], y_recv.at[d - 1, m, origin],
            device_id={"grp": lax.rem(g + d, n_grp)}, device_id_type=MESH).wait_recv()

    def send_own(m):
        own_copies[m].wait()

        @pl.when(k < n_kv - 1)
        def _():
            z_right(m, k).start()

        @pl.when(k > 0)
        def _():
            z_left(m, k).start()

    def forward_step(m, s):
        left = k - 1 - s
        right = k + 1 + s

        @pl.when(left >= 0)
        def _():
            z_right(m, left).wait_recv()

            @pl.when(k < n_kv - 1)
            def _():
                z_right(m, left).start()

            for d in range(1, n_grp):
                y_copy(m, left, d).start()

        @pl.when(right < n_kv)
        def _():
            z_left(m, right).wait_recv()

            @pl.when(k > 0)
            def _():
                z_left(m, right).start()

            for d in range(1, n_grp):
                y_copy(m, right, d).start()

    def forward(m):
        def step(s, carry):
            forward_step(m, s)
            return carry

        lax.fori_loop(0, n_kv - 1, step, 0)

    def wait_y(m):
        def step(o, carry):
            @pl.when(o != k)
            def _():
                for d in range(1, n_grp):
                    y_wait(m, o, d)

            return carry

        lax.fori_loop(0, n_kv, step, 0)

    def t_copy(d):
        return pltpu.make_async_remote_copy(
            tok.at[t_me], tok.at[t_me], t_send.at[d - 1], t_recv.at[d - 1],
            device_id={"tp": lax.rem(t_me + d, n_tp)}, device_id_type=MESH)

    def t_wait(d):
        origin = lax.rem(t_me + n_tp - d, n_tp)
        pltpu.make_async_remote_copy(
            tok.at[origin], tok.at[origin], t_send.at[d - 1], t_recv.at[d - 1],
            device_id={"tp": lax.rem(t_me + d, n_tp)}, device_id_type=MESH).wait_recv()

    send_own(0)
    tok_in.wait()
    for d in range(1, n_tp):
        t_copy(d).start()
    send_own(1)
    send_own(2)

    blk = (
        lax.broadcasted_iota(jnp.int32, (width, width), 0) // hd
        == lax.broadcasted_iota(jnp.int32, (width, width), 1) // hd
    ).astype(F32).astype(BF16)
    lane_head = lax.broadcasted_iota(jnp.int32, (1, width), 1) // hd
    masks = [(lane_head == h).astype(F32) for h in range(heads)]

    def head_sum(x):
        hi = x.astype(BF16)
        lo = (x - hi.astype(F32)).astype(BF16)
        return jnp.dot(hi, blk, preferred_element_type=F32) + jnp.dot(
            lo, blk, preferred_element_type=F32)

    lanes = 128
    blocks = width // lanes

    def rd(ref, at, *lead):
        return jnp.concatenate([ref[(*lead, c, at)] for c in range(blocks)], axis=-1)

    def wr(ref, at, x, *lead):
        for c in range(blocks):
            ref[(*lead, c, at)] = x[:, c * lanes : (c + 1) * lanes]

    every = pl.ds(0, rows)

    pad = 2 * props

    def by_state(s, carry):
        tile = st[pl.ds(pl.multiple_of(s * hd, hd), hd), :]
        stacked = jnp.concatenate([(tile * mask).astype(BF16) for mask in masks], axis=0)
        at = pl.ds(pl.multiple_of(s * pad, pad), pad)
        lhs = rd(kq, at).astype(BF16)
        wr(res, at, jnp.dot(lhs, stacked, preferred_element_type=F32))
        return carry

    def solve(keys, values, weights, logs, queries):
        cumul = []
        run = None
        for t in range(props):
            run = logs[t] if run is None else run + logs[t]
            cumul.append(run)
        low = [(i, j) for i in range(props) for j in range(i)]
        products = [keys[i] * keys[j] for i, j in low]
        full = []
        if queries is not None:
            full = [(i, j) for i in range(props) for j in range(i + 1)]
            products += [queries[i] * keys[j] for i, j in full]
        sums = head_sum(jnp.concatenate(products, axis=0))
        sums = [sums[i * seqs : (i + 1) * seqs] for i in range(len(products))]
        kk = dict(zip(low, sums))
        qk = dict(zip(full, sums[len(low):]))
        dec = {pair: jnp.exp(cumul[pair[0]] - cumul[pair[1]]) for pair in low}
        growth = [jnp.exp(c) for c in cumul]
        update = []
        for t in range(props):
            seen = rd(res, pl.ds(t, seqs, stride=pad))
            term = values[t] - growth[t] * seen
            for j in range(t):
                term = term - kk[t, j] * dec[t, j] * update[j]
            update.append(weights[t] * term)
        outs = []
        if queries is not None:
            for t in range(props):
                out = growth[t] * rd(res, pl.ds(props + t, seqs, stride=pad))
                for j in range(t + 1):
                    score = qk[t, j] if j == t else qk[t, j] * dec[t, j]
                    out = out + score * update[j]
                outs.append(out)
        return cumul, growth, update, outs

    def split(ref):
        return [rd(ref, pl.ds(t, seqs, stride=props)) for t in range(props)]

    for copy in early:
        copy.wait()
    pk = pk_ref[...].astype(F32).reshape(rows, width)
    wr(rows_a, every, pk * lax.rsqrt(head_sum(pk * pk) + EPS))
    wr(rows_b, every, pv_ref[...].astype(F32).reshape(rows, width))
    keys = split(rows_a)
    values = split(rows_b)
    own_head = (
        lax.broadcasted_iota(jnp.int32, (heads, width), 0)
        == lax.broadcasted_iota(jnp.int32, (heads, width), 1) // hd
    ).astype(F32)

    def over_lanes(x):
        return lax.dot_general(
            x, own_head, (((0,), (0,)), ((), ())),
            precision=lax.Precision.HIGHEST, preferred_element_type=F32)

    weights, logs = [], []
    for t in range(props):
        live = (acc_ref[...] > t).astype(F32)
        weights.append(over_lanes(jax.nn.sigmoid(pb_ref[t]) * live))
        logs.append(over_lanes(pd_ref[t] * live))
        wr(kq, pl.ds(t, seqs, stride=pad), keys[t])
        wr(kq, pl.ds(props + t, seqs, stride=pad), keys[t])
    state_in.wait()
    lax.fori_loop(0, seqs, by_state, 0, unroll=4)
    cumul, growth, update, _ = solve(keys, values, weights, logs, None)
    al[...] = growth[-1]
    for t in range(props):
        wr(tk, pl.ds(t, seqs, stride=pad), jnp.exp(cumul[-1] - cumul[t]) * keys[t])
        wr(up, pl.ds(t, seqs, stride=pad), update[t])
        wr(tk, pl.ds(props + t, seqs, stride=pad), jnp.zeros((seqs, width), F32))
        wr(up, pl.ds(props + t, seqs, stride=pad), jnp.zeros((seqs, width), F32))

    def renew(s, carry):
        at = pl.ds(pl.multiple_of(s * pad, pad), pad)
        outer = lax.dot_general(
            rd(tk, at), rd(up, at), (((0,), (0,)), ((), ())), preferred_element_type=F32)
        where = pl.ds(pl.multiple_of(s * hd, hd), hd)
        tile = al[pl.ds(s, 1), :] * st[where, :]
        for h in range(heads):
            tile = tile + masks[h] * outer[h * hd : (h + 1) * hd, :]
        st[where, :] = tile
        return carry

    forward(0)
    send_own(3)
    lax.fori_loop(0, seqs // 2, renew, 0, unroll=2)
    forward(1)
    if gather_out:
        send_own(n_mat - 1)
    lax.fori_loop(seqs // 2, seqs, renew, 0, unroll=2)
    state_out = pltpu.make_async_copy(st, new_hbm, out_sem)
    state_out.start()

    for d in range(1, n_tp):
        t_wait(d)
    for copy in late:
        copy.wait()
    square = jnp.zeros((rows, 1), F32)
    for i in range(n_tp):
        wide = tok[i].astype(F32).reshape(rows, -1)
        square = square + jnp.sum(wide * wide, -1, keepdims=True)
    feats = tok.shape[3]
    scale = lax.rsqrt(square / (n_tp * feats) + EPS)
    for i in range(n_tp):
        cols = slice(i * feats, (i + 1) * feats)
        normed[:, cols] = (tok[i].astype(F32).reshape(rows, -1) * scale * gain_ref[:, cols]).astype(BF16)
    all_heads = wb_ref.shape[0]
    pick = (
        lax.broadcasted_iota(jnp.int32, (all_heads, width), 0)
        == t_me * heads + lax.broadcasted_iota(jnp.int32, (all_heads, width), 1) // hd
    ).astype(F32)

    def per_head(ref):
        raw = lax.dot_general(
            normed[...], ref[...], (((1,), (1,)), ((), ())), preferred_element_type=F32)
        return jnp.dot(raw, pick, precision=lax.Precision.HIGHEST, preferred_element_type=F32)

    wr(rows_a, every, jax.nn.sigmoid(per_head(wb_ref)))
    weights = split(rows_a)
    base = jnp.zeros((1, width), F32)
    for h in range(heads):
        base = jnp.where(lane_head == h, base_ref[:, h : h + 1], base)
    wr(rows_b, every, -base * jax.nn.softplus(per_head(wd_ref)))
    logs = split(rows_b)

    def project(m):
        return jnp.dot(normed[...], wp[m], preferred_element_type=F32)

    def finish(m):
        wait_y(m)
        if m < len(sources):
            value = project(m)
            if m == 0:
                value = value * lax.rsqrt(head_sum(value * value) + EPS)
            elif m == 1:
                value = value * lax.rsqrt(head_sum(value * value) + EPS) * hd ** (-0.5)
            wr(proj, every, value, m)

    outs = None
    def r_copy(dest):
        return pltpu.make_async_remote_copy(
            send_buf.at[dest], recv_buf.at[t_me], r_send.at[dest], r_recv.at[t_me],
            device_id={"tp": dest}, device_id_type=MESH)

    def r_wait(origin):
        pltpu.make_async_remote_copy(
            send_buf.at[origin], recv_buf.at[origin], r_send.at[origin], r_recv.at[origin],
            device_id={"tp": origin}, device_id_type=MESH).wait_recv()

    def send_share(dest):
        share = jnp.dot(gate_buf[...], wo[dest], preferred_element_type=F32)

        @pl.when(dest == t_me)
        def _():
            own_share[...] = share

        @pl.when(dest != t_me)
        def _():
            send_buf[dest] = share.astype(BF16)
            r_copy(dest).start()

    for m in range(len(sources)):
        if m >= 2:
            forward(m)
        if m >= 1:
            finish(m - 1)
        if m == 3:
            keys = [rd(proj, pl.ds(t, seqs, stride=props), 0) for t in range(props)]
            queries = [rd(proj, pl.ds(t, seqs, stride=props), 1) for t in range(props)]
            values = [rd(proj, pl.ds(t, seqs, stride=props), 2) for t in range(props)]
            for t in range(props):
                wr(kq, pl.ds(t, seqs, stride=pad), keys[t])
                wr(kq, pl.ds(props + t, seqs, stride=pad), queries[t])
            lax.fori_loop(0, seqs, by_state, 0, unroll=4)
            outs = solve(keys, values, weights, logs, queries)[3]
            for t in range(props):
                wr(rows_a, pl.ds(t, seqs, stride=props), outs[t])
            out = rd(rows_a, every)
            out = out * lax.rsqrt(head_sum(out * out) / hd + EPS)
            tile_gain = (
                lax.broadcasted_iota(jnp.int32, (hd, width), 0)
                == lax.broadcasted_iota(jnp.int32, (hd, width), 1) % hd
            ).astype(F32)
            gain = jnp.dot(
                jnp.broadcast_to(og_ref[...], (8, hd)), tile_gain,
                precision=lax.Precision.HIGHEST, preferred_element_type=F32)[:1]
            wr(rows_a, every, out * gain)
    finish(len(sources) - 1)
    gate = rd(proj, every, 3)
    gate_buf[...] = (rd(rows_a, every) * (gate / (1.0 + jnp.exp(-gate)))).astype(BF16)
    if gather_out:
        m = n_mat - 1

        def take(s, carry):
            @pl.when(s < n_kv - 1)
            def _():
                forward_step(m, s)

            @pl.when(k - s >= 0)
            def _():
                @pl.when(s > 0)
                def _():
                    for d in range(1, n_grp):
                        y_wait(m, k - s, d)

                send_share(k - s)

            @pl.when(jnp.logical_and(s > 0, k + s < n_kv))
            def _():
                for d in range(1, n_grp):
                    y_wait(m, k + s, d)
                send_share(k + s)

            return carry

        lax.fori_loop(0, n_kv, take, 0)
    else:
        out_in.wait()
        for d in range(n_tp):
            send_share(lax.rem(t_me + d, n_tp))
    total = own_share[...]
    for d in range(1, n_tp):
        origin = lax.rem(t_me + d, n_tp)
        r_wait(origin)
        total = total + recv_buf[origin].astype(F32)
    mixed_ref[...] = total.reshape(seqs, props, feats).astype(BF16)

    for d in range(1, n_tp):
        t_copy(d).wait_send()
        r_copy(lax.rem(t_me + d, n_tp)).wait_send()

    def drain(m):
        def step(o, carry):
            @pl.when(jnp.logical_and(o <= k, k < n_kv - 1))
            def _():
                z_right(m, o).wait_send()

            @pl.when(jnp.logical_and(o >= k, k > 0))
            def _():
                z_left(m, o).wait_send()

            @pl.when(o != k)
            def _():
                for d in range(1, n_grp):
                    y_copy(m, o, d).wait_send()

            return carry

        lax.fori_loop(0, n_kv, step, 0)

    for m in range(n_mat):
        drain(m)
    state_out.wait()


def pair_kernel(
    cfg,
    tok_hbm, gain_hbm, wq_hbm, wk_hbm, wv_hbm, wg_hbm, wb_hbm, wd_hbm, base_hbm, og_hbm, wo_hbm,
    state_hbm, pk_hbm, pv_hbm, pb_hbm, pd_hbm, acc_hbm,
    mixed_ref, st,
    gain_ref, wbd_ref, base_ref, og_ref, pk_ref, pv_ref, pb_ref, pd_ref, acc_ref, tok, wp, wo, normed, kq, res, tk, up, al, rows_a, rows_b, proj, own_part, part_send, part_recv, small_own, small_send, small_recv, send_buf, recv_buf, gate_buf, own_share,
    in_sem, own_sem, wz_send, wz_recv, wy_send, wy_recv, t_send, f_send, d_send, t_recv, zr_send, zl_send, z_recv, y_send, y_recv, p_send, p_recv, r_send, r_recv,
    small_sem,
):
    n_grp, n_kv, n_tp, seqs, props, heads, hd = cfg
    width = heads * hd
    g = lax.axis_index("grp")
    k = lax.axis_index("kv")
    t_me = lax.axis_index("tp")
    rows = seqs * props
    own_rows = wk_hbm.shape[0]
    piece = own_rows // n_grp
    out_piece = wo.shape[1] // n_grp
    feats = tok_hbm.shape[2]
    sources = [wk_hbm, wq_hbm, wv_hbm, wg_hbm]
    n_src = len(sources)
    all_heads = wb_hbm.shape[0]
    pair = k // 2
    side = lax.rem(k, 2)
    mate = k + 1 - 2 * side
    partner = lax.rem(k + n_kv // 2, n_kv)
    chip = t_me // 2
    core = lax.rem(t_me, 2)
    beside_core = 2 * chip + 1 - core
    home = lax.rem(pair + chip + 1, 2)
    g_other = lax.rem(g + 1, n_grp)
    half_feats = 2 * feats

    own_slot = home * (2 + core) + (1 - home) * 4
    tok_in = pltpu.make_async_copy(tok_hbm, tok.at[own_slot], in_sem.at[0])
    tok_in.start()
    own_copies = []
    for m in range(n_src + 1):
        if m < n_src:
            dst = wp.at[m, pl.ds(side * own_rows, own_rows), :]
            copy = pltpu.make_async_copy(sources[m], dst, own_sem.at[m])
        else:
            copy = pltpu.make_async_copy(wo_hbm, wo.at[k], own_sem.at[m])
        copy.start()
        own_copies.append(copy)
    early, late = [], []
    ours = pl.ds(pl.multiple_of(pair * half_feats, half_feats), half_feats)
    pairs = [
        (pk_hbm, pk_ref, early), (pv_hbm, pv_ref, early), (pb_hbm, pb_ref, early),
        (pd_hbm, pd_ref, early), (acc_hbm, acc_ref, early),
        (gain_hbm.at[:, ours], gain_ref, late),
        (wb_hbm.at[:, ours], wbd_ref.at[pl.ds(0, all_heads), :], late),
        (wd_hbm.at[:, ours], wbd_ref.at[pl.ds(all_heads, all_heads), :], late),
        (base_hbm, base_ref, late), (og_hbm, og_ref, late),
    ]
    for i, (src, dst, group) in enumerate(pairs):
        copy = pltpu.make_async_copy(src, dst, small_sem.at[i])
        copy.start()
        group.append(copy)
    state_in = pltpu.make_async_copy(state_hbm, st, in_sem.at[1])
    state_in.start()

    barrier = pltpu.get_barrier_semaphore()

    def greet(dev):
        pl.semaphore_signal(barrier, inc=1, device_id=dev, device_id_type=MESH)

    for d in range(1, n_kv):
        greet({"kv": lax.rem(k + d, n_kv)})
    for d in range(1, n_tp):
        greet({"tp": lax.rem(t_me + d, n_tp)})
    greet({"grp": g_other})
    far_tp = 2 * (1 - chip) + core
    pl.semaphore_wait(barrier, n_kv + n_tp - 1)

    def remote(src, dst, send, recv, dev):
        return pltpu.make_async_remote_copy(
            src, dst, send, recv, device_id=dev, device_id_type=MESH)

    part = seqs // 2

    def tok_piece(slot, half):
        return tok.at[slot, pl.ds(half * part, part)]

    def tok_partner(half):
        return remote(tok_piece(own_slot, half), tok_piece(core, half), t_send.at[half],
                      t_recv.at[core, half], {"kv": partner})

    def tok_far(slot, half):
        ref = tok_piece(slot, half)
        return remote(ref, ref, f_send.at[slot // 2, half], t_recv.at[slot, half],
                      {"tp": far_tp})

    def tok_beside(slot, half):
        ref = tok_piece(slot, half)
        return remote(ref, ref, d_send.at[slot // 2, half], t_recv.at[slot, half],
                      {"tp": beside_core})

    def tok_wait(slot, half):
        ref = tok_piece(slot, half)
        remote(ref, ref, d_send.at[0, half], t_recv.at[slot, half],
               {"tp": beside_core}).wait_recv()

    def tok_land(half):
        tok_wait(core, half)

        @pl.when(home == 1)
        def _():
            tok_far(core, half).start()

        tok_beside(core, half).start()

    def w_slot(m, block, half):
        return wp.at[m, pl.ds(block * own_rows + half * piece, piece), :]

    def w_mate(m):
        ref = w_slot(m, side, g)
        return remote(ref, ref, wz_send.at[m], wz_recv.at[m], {"kv": mate})

    def w_share(m):
        ref = w_slot(m, 1 - side, g)
        return remote(ref, ref, wy_send.at[m], wy_recv.at[m], {"grp": g_other})

    def w_pass(m):
        ref = w_slot(m, 1 - side, g)
        remote(ref, ref, wz_send.at[m], wz_recv.at[m], {"kv": mate}).wait_recv()
        w_share(m).start()

    def w_ready(m):
        ref = w_slot(m, 1 - side, g_other)
        remote(ref, ref, wy_send.at[m], wy_recv.at[m], {"grp": g_other}).wait_recv()

    def o_slot(origin, part):
        return wo.at[origin, pl.ds(part * out_piece, out_piece), :]

    def z_right(origin):
        ref = o_slot(origin, g)
        return remote(ref, ref, zr_send.at[origin], z_recv.at[origin], {"kv": k + 1})

    def z_left(origin):
        ref = o_slot(origin, g)
        return remote(ref, ref, zl_send.at[origin], z_recv.at[origin], {"kv": k - 1})

    def y_copy(origin):
        ref = o_slot(origin, g)
        return remote(ref, ref, y_send.at[origin], y_recv.at[origin], {"grp": g_other})

    def y_wait(origin):
        ref = o_slot(origin, g_other)
        remote(ref, ref, y_send.at[origin], y_recv.at[origin], {"grp": g_other}).wait_recv()

    def from_left(origin):
        z_right(origin).wait_recv()

        @pl.when(k < n_kv - 1)
        def _():
            z_right(origin).start()

        y_copy(origin).start()

    def from_right(origin):
        z_left(origin).wait_recv()

        @pl.when(k > 0)
        def _():
            z_left(origin).start()

        y_copy(origin).start()

    def middle_pass(s):
        @pl.when(jnp.logical_and(side == 1, pair == 0))
        def _():
            if s == 0:
                from_left(k - 1)
            else:
                from_right(k + s)

        @pl.when(jnp.logical_and(side == 0, pair == 1))
        def _():
            if s == 0:
                from_right(k + 1)
            else:
                from_left(k - s)

    def end_pass(s):
        @pl.when(k == 0)
        def _():
            from_right(k + s)

        @pl.when(k == n_kv - 1)
        def _():
            from_left(k - s)

    def p_copy(m):
        return remote(part_send.at[m], part_recv.at[m], p_send.at[m], p_recv.at[m],
                      {"kv": partner})

    def small_copy():
        return remote(small_send, small_recv, p_send.at[n_src], p_recv.at[n_src],
                      {"kv": partner})

    at_end = jnp.logical_or(k == 0, k == n_kv - 1)
    tok_in.wait()

    @pl.when(home == 0)
    def _():
        for half in range(2):
            tok_partner(half).start()

    @pl.when(home == 1)
    def _():
        for half in range(2):
            tok_far(2 + core, half).start()
            tok_beside(2 + core, half).start()

    def w_first(m):
        own_copies[m].wait()
        w_mate(m).start()

    w_first(0)
    w_first(1)
    own_copies[n_src].wait()

    @pl.when(k == 0)
    def _():
        z_right(k).start()

    @pl.when(k == n_kv - 1)
    def _():
        z_left(k).start()

    w_first(2)
    w_first(3)

    blk = (
        lax.broadcasted_iota(jnp.int32, (width, width), 0) // hd
        == lax.broadcasted_iota(jnp.int32, (width, width), 1) // hd
    ).astype(F32).astype(BF16)
    lane_head = lax.broadcasted_iota(jnp.int32, (1, width), 1) // hd
    masks = [(lane_head == h).astype(F32) for h in range(heads)]

    def head_sum(x):
        hi = x.astype(BF16)
        lo = (x - hi.astype(F32)).astype(BF16)
        return jnp.dot(hi, blk, preferred_element_type=F32) + jnp.dot(
            lo, blk, preferred_element_type=F32)

    lanes = 128
    blocks = width // lanes

    def rd(ref, at, *lead):
        return jnp.concatenate([ref[(*lead, c, at)] for c in range(blocks)], axis=-1)

    def wr(ref, at, x, *lead):
        for c in range(blocks):
            ref[(*lead, c, at)] = x[:, c * lanes : (c + 1) * lanes]

    every = pl.ds(0, rows)

    pad = 2 * props

    def by_state(s, carry):
        tile = st[pl.ds(pl.multiple_of(s * hd, hd), hd), :]
        stacked = jnp.concatenate([(tile * mask).astype(BF16) for mask in masks], axis=0)
        at = pl.ds(pl.multiple_of(s * pad, pad), pad)
        lhs = rd(kq, at).astype(BF16)
        wr(res, at, jnp.dot(lhs, stacked, preferred_element_type=F32))
        return carry

    def solve(keys, values, weights, logs, queries):
        cumul = []
        run = None
        for t in range(props):
            run = logs[t] if run is None else run + logs[t]
            cumul.append(run)
        low = [(i, j) for i in range(props) for j in range(i)]
        products = [keys[i] * keys[j] for i, j in low]
        full = []
        if queries is not None:
            full = [(i, j) for i in range(props) for j in range(i + 1)]
            products += [queries[i] * keys[j] for i, j in full]
        sums = head_sum(jnp.concatenate(products, axis=0))
        sums = [sums[i * seqs : (i + 1) * seqs] for i in range(len(products))]
        kk = dict(zip(low, sums))
        qk = dict(zip(full, sums[len(low):]))
        dec = {pair: jnp.exp(cumul[pair[0]] - cumul[pair[1]]) for pair in low}
        growth = [jnp.exp(c) for c in cumul]
        update = []
        for t in range(props):
            seen = rd(res, pl.ds(t, seqs, stride=pad))
            term = values[t] - growth[t] * seen
            for j in range(t):
                term = term - kk[t, j] * dec[t, j] * update[j]
            update.append(weights[t] * term)
        outs = []
        if queries is not None:
            for t in range(props):
                out = growth[t] * rd(res, pl.ds(props + t, seqs, stride=pad))
                for j in range(t + 1):
                    score = qk[t, j] if j == t else qk[t, j] * dec[t, j]
                    out = out + score * update[j]
                outs.append(out)
        return cumul, growth, update, outs

    def split(ref):
        return [rd(ref, pl.ds(t, seqs, stride=props)) for t in range(props)]

    for copy in early:
        copy.wait()
    pk = pk_ref[...].astype(F32).reshape(rows, width)
    wr(rows_a, every, pk * lax.rsqrt(head_sum(pk * pk) + EPS))
    wr(rows_b, every, pv_ref[...].astype(F32).reshape(rows, width))
    keys = split(rows_a)
    values = split(rows_b)
    own_head = (
        lax.broadcasted_iota(jnp.int32, (heads, width), 0)
        == lax.broadcasted_iota(jnp.int32, (heads, width), 1) // hd
    ).astype(F32)

    def over_lanes(x):
        return lax.dot_general(
            x, own_head, (((0,), (0,)), ((), ())),
            precision=lax.Precision.HIGHEST, preferred_element_type=F32)

    weights, logs = [], []
    for t in range(props):
        live = (acc_ref[...] > t).astype(F32)
        weights.append(over_lanes(jax.nn.sigmoid(pb_ref[t]) * live))
        logs.append(over_lanes(pd_ref[t] * live))
        wr(kq, pl.ds(t, seqs, stride=pad), keys[t])
        wr(kq, pl.ds(props + t, seqs, stride=pad), keys[t])
    state_in.wait()
    lax.fori_loop(0, seqs, by_state, 0, unroll=4)
    cumul, growth, update, _ = solve(keys, values, weights, logs, None)
    al[...] = growth[-1]
    for t in range(props):
        wr(tk, pl.ds(t, seqs, stride=pad), jnp.exp(cumul[-1] - cumul[t]) * keys[t])
        wr(up, pl.ds(t, seqs, stride=pad), update[t])
        wr(tk, pl.ds(props + t, seqs, stride=pad), jnp.zeros((seqs, width), F32))
        wr(up, pl.ds(props + t, seqs, stride=pad), jnp.zeros((seqs, width), F32))

    def renew(s, carry):
        at = pl.ds(pl.multiple_of(s * pad, pad), pad)
        outer = lax.dot_general(
            rd(tk, at), rd(up, at), (((0,), (0,)), ((), ())), preferred_element_type=F32)
        where = pl.ds(pl.multiple_of(s * hd, hd), hd)
        tile = al[pl.ds(s, 1), :] * st[where, :]
        for h in range(heads):
            tile = tile + masks[h] * outer[h * hd : (h + 1) * hd, :]
        st[where, :] = tile
        return carry


    @pl.when(home == 0)
    def _():
        for half in range(2):
            tok_wait(2 + core, half)
            tok_beside(2 + core, half).start()

    @pl.when(home == 1)
    def _():
        tok_land(0)

    w_pass(0)

    @pl.when(jnp.logical_not(at_end))
    def _():
        z_right(k).start()
        z_left(k).start()

    @pl.when(home == 1)
    def _():
        tok_land(1)

    @pl.when(home == 0)
    def _():
        tok_land(0)

    w_pass(1)

    @pl.when(home == 0)
    def _():
        tok_land(1)

    for copy in late:
        copy.wait()
    for half in range(2):
        tok_wait(3 - core, half)
        tok_wait(1 - core, half)
    ones = jnp.ones((8, feats), BF16)
    squares = jnp.zeros((8, 2 * rows), F32)
    last = (((1,), (1,)), ((), ()))
    for c in range(2):
        cols = slice(c * feats, (c + 1) * feats)
        wide = jnp.concatenate(
            [tok[c].astype(F32).reshape(rows, feats), tok[2 + c].astype(F32).reshape(rows, feats)],
            axis=0)
        normed[:, cols] = (wide * gain_ref[:, cols]).astype(BF16)
        sq = wide * wide
        hi = sq.astype(BF16)
        lo = (sq - hi.astype(F32)).astype(BF16)
        squares = squares + lax.dot_general(ones, hi, last, preferred_element_type=F32)
        squares = squares + lax.dot_general(ones, lo, last, preferred_element_type=F32)
    raw = lax.dot_general(wbd_ref[...], normed[...], last, preferred_element_type=F32)
    small = jnp.concatenate([raw, squares], axis=0)
    small_send[...] = small[:, :rows]
    small_copy().start()
    small_own[...] = small[:, rows:]

    def project(m):
        both = jnp.dot(normed[...], wp[m], preferred_element_type=F32)
        part_send[m] = both[:rows].astype(BF16)
        p_copy(m).start()
        own_part[m] = both[rows:]

    w_ready(0)
    project(0)
    middle_pass(0)
    w_pass(2)
    w_ready(1)
    project(1)
    middle_pass(1)
    w_pass(3)
    w_ready(2)
    project(2)
    lax.fori_loop(0, seqs // 2, renew, 0, unroll=2)
    w_ready(3)
    project(3)
    middle_pass(2)
    end_pass(1)
    lax.fori_loop(seqs // 2, seqs, renew, 0, unroll=2)

    pick = (
        lax.broadcasted_iota(jnp.int32, (all_heads, width), 0)
        == t_me * heads + lax.broadcasted_iota(jnp.int32, (all_heads, width), 1) // hd
    ).astype(F32)
    small_copy().wait_recv()
    small = small_own[...] + small_recv[...]
    scale = lax.rsqrt(small[2 * all_heads :] / (n_tp * feats) + EPS)
    beta = small[:all_heads] * scale[:1]
    decay = small[all_heads : 2 * all_heads] * scale[:1]

    def spread(x, over):
        return lax.dot_general(
            x, over, (((0,), (0,)), ((), ())),
            precision=lax.Precision.HIGHEST, preferred_element_type=F32)

    wr(rows_a, every, spread(jax.nn.sigmoid(beta), pick))
    weights = split(rows_a)
    base = jnp.zeros((1, width), F32)
    for h in range(heads):
        base = jnp.where(lane_head == h, base_ref[:, h : h + 1], base)
    wr(rows_b, every, -base * spread(jax.nn.softplus(decay), pick))
    logs = split(rows_b)
    row_scale = spread(
        scale, (lax.broadcasted_iota(jnp.int32, (8, width), 0) == 0).astype(F32))

    def finish(m):
        p_copy(m).wait_recv()
        value = (own_part[m] + part_recv[m].astype(F32)) * row_scale
        if m == 0:
            value = value * lax.rsqrt(head_sum(value * value) + EPS)
        elif m == 1:
            value = value * lax.rsqrt(head_sum(value * value) + EPS) * hd ** (-0.5)
        wr(proj, every, value, m)

    def r_copy(dest):
        return pltpu.make_async_remote_copy(
            send_buf.at[dest], recv_buf.at[t_me], r_send.at[dest], r_recv.at[t_me],
            device_id={"tp": dest}, device_id_type=MESH)

    def r_wait(origin):
        pltpu.make_async_remote_copy(
            send_buf.at[origin], recv_buf.at[origin], r_send.at[origin], r_recv.at[origin],
            device_id={"tp": origin}, device_id_type=MESH).wait_recv()

    def send_share(dest):
        share = jnp.dot(gate_buf[...], wo[dest], preferred_element_type=F32)

        @pl.when(dest == t_me)
        def _():
            own_share[...] = share

        @pl.when(dest != t_me)
        def _():
            send_buf[dest] = share.astype(BF16)
            r_copy(dest).start()

    finish(0)
    end_pass(2)
    finish(1)
    finish(2)
    keys = [rd(proj, pl.ds(t, seqs, stride=props), 0) for t in range(props)]
    queries = [rd(proj, pl.ds(t, seqs, stride=props), 1) for t in range(props)]
    values = [rd(proj, pl.ds(t, seqs, stride=props), 2) for t in range(props)]
    for t in range(props):
        wr(kq, pl.ds(t, seqs, stride=pad), keys[t])
        wr(kq, pl.ds(props + t, seqs, stride=pad), queries[t])
    lax.fori_loop(0, seqs, by_state, 0, unroll=4)
    outs = solve(keys, values, weights, logs, queries)[3]
    for t in range(props):
        wr(rows_a, pl.ds(t, seqs, stride=props), outs[t])
    out = rd(rows_a, every)
    out = out * lax.rsqrt(head_sum(out * out) / hd + EPS)
    tile_gain = (
        lax.broadcasted_iota(jnp.int32, (hd, width), 0)
        == lax.broadcasted_iota(jnp.int32, (hd, width), 1) % hd
    ).astype(F32)
    gain = jnp.dot(
        jnp.broadcast_to(og_ref[...], (8, hd)), tile_gain,
        precision=lax.Precision.HIGHEST, preferred_element_type=F32)[:1]
    wr(rows_a, every, out * gain)
    end_pass(3)
    finish(n_src - 1)
    gate = rd(proj, every, 3)
    gate_buf[...] = (rd(rows_a, every) * (gate / (1.0 + jnp.exp(-gate)))).astype(BF16)

    def take(s, carry):
        @pl.when(k - s >= 0)
        def _():
            @pl.when(s > 0)
            def _():
                y_wait(k - s)

            send_share(k - s)

        @pl.when(jnp.logical_and(s > 0, k + s < n_kv))
        def _():
            y_wait(k + s)
            send_share(k + s)

        return carry

    lax.fori_loop(0, n_kv, take, 0)
    total = own_share[...]
    for d in range(1, n_tp):
        origin = lax.rem(t_me + d, n_tp)
        r_wait(origin)
        total = total + recv_buf[origin].astype(F32)
    mixed_ref[...] = total.reshape(seqs, props, feats).astype(BF16)

    for half in range(2):
        tok_beside(core, half).wait_send()
        tok_beside(2 + core, half).wait_send()

        @pl.when(home == 1)
        def _():
            tok_far(core, half).wait_send()
            tok_far(2 + core, half).wait_send()

        @pl.when(home == 0)
        def _():
            tok_partner(half).wait_send()

    for m in range(n_src):
        w_mate(m).wait_send()
        w_share(m).wait_send()
        p_copy(m).wait_send()
    small_copy().wait_send()
    for d in range(1, n_tp):
        r_copy(lax.rem(t_me + d, n_tp)).wait_send()

    def drain(o, carry):
        @pl.when(jnp.logical_and(o <= k, k < n_kv - 1))
        def _():
            z_right(o).wait_send()

        @pl.when(jnp.logical_and(o >= k, k > 0))
        def _():
            z_left(o).wait_send()

        @pl.when(o != k)
        def _():
            y_copy(o).wait_send()

        return carry

    lax.fori_loop(0, n_kv, drain, 0)


def pair_call(sizes, args, seqs, props, feats, heads, hd, width, rows, pad):
    n_grp, n_kv, n_tp = sizes
    cfg = (n_grp, n_kv, n_tp, seqs, props, heads, hd)
    vmem = pl.BlockSpec(memory_space=pltpu.VMEM)
    hbm = pl.BlockSpec(memory_space=pltpu.HBM)
    dma = pltpu.SemaphoreType.DMA
    own_rows = args[2].shape[0]
    all_heads = args[6].shape[0]
    n_src = 4
    small = (2 * all_heads + 8, rows)
    return pl.pallas_call(
        functools.partial(pair_kernel, cfg),
        out_shape=(
            pltpu.VMEM((seqs, props, feats), BF16),
            pltpu.VMEM((seqs * hd, width), F32),
        ),
        in_specs=[hbm] * len(args),
        out_specs=(vmem, vmem),
        scratch_shapes=[
            pltpu.VMEM((1, 2 * feats), F32),
            pltpu.VMEM((2 * all_heads, 2 * feats), BF16),
            *[pltpu.VMEM(args[i].shape, args[i].dtype) for i in (8, 9, 12, 13, 14, 15, 16)],
            pltpu.VMEM((5, seqs, props, feats), BF16),
            pltpu.VMEM((n_src, 2 * own_rows, width), BF16),
            pltpu.VMEM((n_tp, width, feats), BF16),
            pltpu.VMEM((2 * rows, 2 * feats), BF16),
            pltpu.VMEM((width // 128, seqs * pad, 128), F32),
            pltpu.VMEM((width // 128, seqs * pad, 128), F32),
            pltpu.VMEM((width // 128, seqs * pad, 128), F32),
            pltpu.VMEM((width // 128, seqs * pad, 128), F32),
            pltpu.VMEM((seqs, width), F32),
            pltpu.VMEM((width // 128, rows, 128), F32),
            pltpu.VMEM((width // 128, rows, 128), F32),
            pltpu.VMEM((n_src, width // 128, rows, 128), F32),
            pltpu.VMEM((n_src, rows, width), F32),
            pltpu.VMEM((n_src, rows, width), BF16),
            pltpu.VMEM((n_src, rows, width), BF16),
            pltpu.VMEM(small, F32),
            pltpu.VMEM(small, F32),
            pltpu.VMEM(small, F32),
            pltpu.VMEM((n_tp, rows, feats), BF16),
            pltpu.VMEM((n_tp, rows, feats), BF16),
            pltpu.VMEM((rows, width), BF16),
            pltpu.VMEM((rows, feats), F32),
            dma((2,)),
            dma((n_src + 1,)),
            *[dma((n_src,)) for _ in range(4)],
            dma((2,)),
            dma((2, 2)),
            dma((2, 2)),
            dma((4, 2)),
            *[dma((n_kv,)) for _ in range(5)],
            dma((n_src + 1,)),
            dma((n_src + 1,)),
            dma((n_tp,)),
            dma((n_tp,)),
            dma((10,)),
        ],
        compiler_params=pltpu.CompilerParams(
            collective_id=1, has_side_effects=True, vmem_limit_bytes=67043328 - rows * feats * 2 - seqs * hd * width * 4),
    )(*args)


def body(
    sizes,
    tokens, in_gain, w_query, w_key, w_value, w_gate, w_beta, w_decay, decay_base, out_gain, w_out,
    state, prev_keys, prev_values, prev_beta, prev_decay, accepted,
):
    n_grp, n_kv, n_tp = sizes
    seqs, props, feats = tokens.shape
    heads = decay_base.shape[0]
    hd = out_gain.shape[0]
    width = heads * hd
    rows = seqs * props
    pad = 2 * props
    paired = (
        n_grp == 2 and n_kv == n_tp and n_kv // 2 == 2
        and w_query.shape[0] == feats and w_query.shape[0] * n_kv == in_gain.shape[0])
    gather_out = n_kv == n_tp
    if not gather_out:
        w_out = lax.all_gather(w_out, "kv", axis=1, tiled=True)
        w_out = jnp.transpose(w_out.reshape(width, n_tp, feats), (1, 0, 2))
    n_mat = 5 if gather_out else 4
    cfg = (n_grp, n_kv, n_tp, seqs, props, heads, hd, gather_out)
    vmem = pl.BlockSpec(memory_space=pltpu.VMEM)
    hbm = pl.BlockSpec(memory_space=pltpu.HBM)
    args = (
        tokens, in_gain.reshape(1, -1), w_query, w_key, w_value, w_gate,
        w_beta.T, w_decay.T, decay_base.reshape(1, -1), out_gain.reshape(1, -1), w_out,
        state.reshape(seqs * hd, width), prev_keys, prev_values,
        jnp.transpose(prev_beta, (1, 2, 0)), jnp.transpose(prev_decay, (1, 2, 0)),
        accepted.reshape(1, seqs),
    )
    if paired:
        mixed, new_state = pair_call(
            sizes, args, seqs, props, feats, heads, hd, width, rows, pad)
        return mixed, new_state.reshape(seqs, hd, width)
    dma = pltpu.SemaphoreType.DMA
    mixed, new_state = pl.pallas_call(
        functools.partial(kernel, cfg),
        out_shape=(
            jax.ShapeDtypeStruct((seqs, props, feats), BF16),
            jax.ShapeDtypeStruct((seqs * hd, width), F32),
        ),
        in_specs=[hbm] * len(args),
        out_specs=(vmem, pl.BlockSpec(memory_space=pl.ANY)),
        scratch_shapes=[
            *[pltpu.VMEM(args[i].shape, args[i].dtype) for i in (1, 6, 7, 8, 9, 12, 13, 14, 15, 16)],
            pltpu.VMEM((n_tp, seqs, props, feats), BF16),
            pltpu.VMEM((4, n_kv * w_key.shape[0], width), BF16),
            pltpu.VMEM((n_tp, width, feats), BF16),
            pltpu.VMEM((seqs * hd, width), F32),
            pltpu.VMEM((rows, n_tp * feats), BF16),
            pltpu.VMEM((width // 128, seqs * pad, 128), F32),
            pltpu.VMEM((width // 128, seqs * pad, 128), F32),
            pltpu.VMEM((width // 128, seqs * pad, 128), F32),
            pltpu.VMEM((width // 128, seqs * pad, 128), F32),
            pltpu.VMEM((seqs, width), F32),
            pltpu.VMEM((width // 128, rows, 128), F32),
            pltpu.VMEM((width // 128, rows, 128), F32),
            pltpu.VMEM((4, width // 128, rows, 128), F32),
            pltpu.VMEM((n_tp, rows, feats), BF16),
            pltpu.VMEM((n_tp, rows, feats), BF16),
            pltpu.VMEM((rows, width), BF16),
            pltpu.VMEM((rows, feats), F32),
            dma((2,)),
            dma((6,)),
            dma((n_mat, n_kv)),
            dma((n_mat, n_kv)),
            dma((n_mat, n_kv)),
            dma((max(n_grp - 1, 1), n_mat, n_kv)),
            dma((max(n_grp - 1, 1), n_mat, n_kv)),
            dma((n_tp - 1,)),
            dma((n_tp - 1,)),
            dma((n_tp,)),
            dma((n_tp,)),
            dma(()),
            dma((10,)),
        ],
        compiler_params=pltpu.CompilerParams(
            collective_id=0, has_side_effects=True, vmem_limit_bytes=67043328),
    )(*args)
    return mixed, new_state.reshape(seqs, hd, width)


def solution(mesh):
    sizes = (mesh.shape["grp"], mesh.shape["kv"], mesh.shape["tp"])
    tokens = P(("grp", "kv"), None, "tp")
    placed = (
        tokens, P(), P("kv", "tp"), P("kv", "tp"), P("kv", "tp"), P("kv", "tp"), P(), P(),
        P("tp"), P(), P("tp", "kv"), tokens, tokens, tokens, tokens, tokens, P(("grp", "kv")),
    )
    return jax.shard_map(
        functools.partial(body, sizes),
        mesh=mesh,
        in_specs=placed,
        out_specs=(tokens, tokens),
        check_vma=False,
    )
```

```python
import functools

import jax
import jax.numpy as jnp
from jax import lax
from jax.experimental import pallas as pl
from jax.experimental.pallas import tpu as pltpu
from jax.sharding import PartitionSpec as P

EPS = 1e-06
F32 = jnp.float32
BF16 = jnp.bfloat16
MESH = pl.DeviceIdType.MESH


def kernel(
    cfg,
    tok_hbm, gain_hbm, wq_hbm, wk_hbm, wv_hbm, wg_hbm, wb_hbm, wd_hbm, base_hbm, og_hbm, wo_hbm,
    state_hbm, pk_hbm, pv_hbm, pb_hbm, pd_hbm, acc_hbm,
    mixed_ref, new_hbm,
    gain_ref, wb_ref, wd_ref, base_ref, og_ref, pk_ref, pv_ref, pb_ref, pd_ref, acc_ref, tok, wp, wo, st, normed, kq, res, tk, up, al, rows_a, rows_b, proj, send_buf, recv_buf, gate_buf, own_share,
    in_sem, own_sem, zr_send, zl_send, z_recv, y_send, y_recv, t_send, t_recv, r_send, r_recv,
    out_sem, small_sem,
):
    n_grp, n_kv, n_tp, seqs, props, heads, hd, gather_out = cfg
    width = heads * hd
    g = lax.axis_index("grp")
    k = lax.axis_index("kv")
    t_me = lax.axis_index("tp")
    rows = seqs * props
    own_rows = wk_hbm.shape[0]
    piece = own_rows // n_grp
    out_piece = wo.shape[1] // n_grp
    sources = [wk_hbm, wq_hbm, wv_hbm, wg_hbm]
    n_mat = len(sources) + (1 if gather_out else 0)

    tok_in = pltpu.make_async_copy(tok_hbm, tok.at[t_me], in_sem.at[0])
    tok_in.start()
    own_copies = []
    for m in range(n_mat):
        if m < len(sources):
            dst = wp.at[m, pl.ds(k * own_rows, own_rows), :]
            copy = pltpu.make_async_copy(sources[m], dst, own_sem.at[m])
        else:
            copy = pltpu.make_async_copy(wo_hbm, wo.at[k], own_sem.at[m])
        copy.start()
        own_copies.append(copy)
    early, late = [], []
    pairs = [
        (pk_hbm, pk_ref, early), (pv_hbm, pv_ref, early), (pb_hbm, pb_ref, early),
        (pd_hbm, pd_ref, early), (acc_hbm, acc_ref, early), (gain_hbm, gain_ref, late),
        (wb_hbm, wb_ref, late), (wd_hbm, wd_ref, late), (base_hbm, base_ref, late),
        (og_hbm, og_ref, late),
    ]
    for i, (src, dst, group) in enumerate(pairs):
        copy = pltpu.make_async_copy(src, dst, small_sem.at[i])
        copy.start()
        group.append(copy)
    state_in = pltpu.make_async_copy(state_hbm, st, in_sem.at[1])
    state_in.start()
    out_in = None
    if not gather_out:
        out_in = pltpu.make_async_copy(wo_hbm, wo, own_sem.at[n_mat])
        out_in.start()

    barrier = pltpu.get_barrier_semaphore()

    def greet(dev):
        pl.semaphore_signal(barrier, inc=1, device_id=dev, device_id_type=MESH)

    @pl.when(k > 0)
    def _():
        greet({"kv": k - 1})

    @pl.when(k < n_kv - 1)
    def _():
        greet({"kv": k + 1})

    for d in range(1, n_grp):
        greet({"grp": lax.rem(g + d, n_grp)})
    for d in range(1, n_tp):
        greet({"tp": lax.rem(t_me + d, n_tp)})

    beside = jnp.minimum(k, 1) + jnp.minimum(n_kv - 1 - k, 1)
    pl.semaphore_wait(barrier, n_grp + n_tp - 2 + beside)

    def slot(m, origin, part):
        if m < len(sources):
            return wp.at[m, pl.ds(origin * own_rows + part * piece, piece), :]
        return wo.at[origin, pl.ds(part * out_piece, out_piece), :]

    def z_right(m, origin):
        ref = slot(m, origin, g)
        return pltpu.make_async_remote_copy(
            ref, ref, zr_send.at[m, origin], z_recv.at[m, origin],
            device_id={"kv": k + 1}, device_id_type=MESH)

    def z_left(m, origin):
        ref = slot(m, origin, g)
        return pltpu.make_async_remote_copy(
            ref, ref, zl_send.at[m, origin], z_recv.at[m, origin],
            device_id={"kv": k - 1}, device_id_type=MESH)

    def y_copy(m, origin, d):
        ref = slot(m, origin, g)
        return pltpu.make_async_remote_copy(
            ref, ref, y_send.at[d - 1, m, origin], y_recv.at[d - 1, m, origin],
            device_id={"grp": lax.rem(g + d, n_grp)}, device_id_type=MESH)

    def y_wait(m, origin, d):
        ref = slot(m, origin, lax.rem(g + n_grp - d, n_grp))
        pltpu.make_async_remote_copy(
            ref, ref, y_send.at[d - 1, m, origin], y_recv.at[d - 1, m, origin],
            device_id={"grp": lax.rem(g + d, n_grp)}, device_id_type=MESH).wait_recv()

    def send_own(m):
        own_copies[m].wait()

        @pl.when(k < n_kv - 1)
        def _():
            z_right(m, k).start()

        @pl.when(k > 0)
        def _():
            z_left(m, k).start()

    def forward_step(m, s):
        left = k - 1 - s
        right = k + 1 + s

        @pl.when(left >= 0)
        def _():
            z_right(m, left).wait_recv()

            @pl.when(k < n_kv - 1)
            def _():
                z_right(m, left).start()

            for d in range(1, n_grp):
                y_copy(m, left, d).start()

        @pl.when(right < n_kv)
        def _():
            z_left(m, right).wait_recv()

            @pl.when(k > 0)
            def _():
                z_left(m, right).start()

            for d in range(1, n_grp):
                y_copy(m, right, d).start()

    def forward(m):
        def step(s, carry):
            forward_step(m, s)
            return carry

        lax.fori_loop(0, n_kv - 1, step, 0)

    def wait_y(m):
        def step(o, carry):
            @pl.when(o != k)
            def _():
                for d in range(1, n_grp):
                    y_wait(m, o, d)

            return carry

        lax.fori_loop(0, n_kv, step, 0)

    def t_copy(d):
        return pltpu.make_async_remote_copy(
            tok.at[t_me], tok.at[t_me], t_send.at[d - 1], t_recv.at[d - 1],
            device_id={"tp": lax.rem(t_me + d, n_tp)}, device_id_type=MESH)

    def t_wait(d):
        origin = lax.rem(t_me + n_tp - d, n_tp)
        pltpu.make_async_remote_copy(
            tok.at[origin], tok.at[origin], t_send.at[d - 1], t_recv.at[d - 1],
            device_id={"tp": lax.rem(t_me + d, n_tp)}, device_id_type=MESH).wait_recv()

    send_own(0)
    tok_in.wait()
    for d in range(1, n_tp):
        t_copy(d).start()
    send_own(1)
    send_own(2)

    blk = (
        lax.broadcasted_iota(jnp.int32, (width, width), 0) // hd
        == lax.broadcasted_iota(jnp.int32, (width, width), 1) // hd
    ).astype(F32).astype(BF16)
    lane_head = lax.broadcasted_iota(jnp.int32, (1, width), 1) // hd
    masks = [(lane_head == h).astype(F32) for h in range(heads)]

    def head_sum(x):
        hi = x.astype(BF16)
        lo = (x - hi.astype(F32)).astype(BF16)
        return jnp.dot(hi, blk, preferred_element_type=F32) + jnp.dot(
            lo, blk, preferred_element_type=F32)

    lanes = 128
    blocks = width // lanes

    def rd(ref, at, *lead):
        return jnp.concatenate([ref[(*lead, c, at)] for c in range(blocks)], axis=-1)

    def wr(ref, at, x, *lead):
        for c in range(blocks):
            ref[(*lead, c, at)] = x[:, c * lanes : (c + 1) * lanes]

    every = pl.ds(0, rows)

    pad = 2 * props

    def by_state(s, carry):
        tile = st[pl.ds(pl.multiple_of(s * hd, hd), hd), :]
        stacked = jnp.concatenate([(tile * mask).astype(BF16) for mask in masks], axis=0)
        at = pl.ds(pl.multiple_of(s * pad, pad), pad)
        lhs = rd(kq, at).astype(BF16)
        wr(res, at, jnp.dot(lhs, stacked, preferred_element_type=F32))
        return carry

    def solve(keys, values, weights, logs, queries):
        cumul = []
        run = None
        for t in range(props):
            run = logs[t] if run is None else run + logs[t]
            cumul.append(run)
        low = [(i, j) for i in range(props) for j in range(i)]
        products = [keys[i] * keys[j] for i, j in low]
        full = []
        if queries is not None:
            full = [(i, j) for i in range(props) for j in range(i + 1)]
            products += [queries[i] * keys[j] for i, j in full]
        sums = head_sum(jnp.concatenate(products, axis=0))
        sums = [sums[i * seqs : (i + 1) * seqs] for i in range(len(products))]
        kk = dict(zip(low, sums))
        qk = dict(zip(full, sums[len(low):]))
        dec = {pair: jnp.exp(cumul[pair[0]] - cumul[pair[1]]) for pair in low}
        growth = [jnp.exp(c) for c in cumul]
        update = []
        for t in range(props):
            seen = rd(res, pl.ds(t, seqs, stride=pad))
            term = values[t] - growth[t] * seen
            for j in range(t):
                term = term - kk[t, j] * dec[t, j] * update[j]
            update.append(weights[t] * term)
        outs = []
        if queries is not None:
            for t in range(props):
                out = growth[t] * rd(res, pl.ds(props + t, seqs, stride=pad))
                for j in range(t + 1):
                    score = qk[t, j] if j == t else qk[t, j] * dec[t, j]
                    out = out + score * update[j]
                outs.append(out)
        return cumul, growth, update, outs

    def split(ref):
        return [rd(ref, pl.ds(t, seqs, stride=props)) for t in range(props)]

    for copy in early:
        copy.wait()
    pk = pk_ref[...].astype(F32).reshape(rows, width)
    wr(rows_a, every, pk * lax.rsqrt(head_sum(pk * pk) + EPS))
    wr(rows_b, every, pv_ref[...].astype(F32).reshape(rows, width))
    keys = split(rows_a)
    values = split(rows_b)
    own_head = (
        lax.broadcasted_iota(jnp.int32, (heads, width), 0)
        == lax.broadcasted_iota(jnp.int32, (heads, width), 1) // hd
    ).astype(F32)

    def over_lanes(x):
        return lax.dot_general(
            x, own_head, (((0,), (0,)), ((), ())),
            precision=lax.Precision.HIGHEST, preferred_element_type=F32)

    weights, logs = [], []
    for t in range(props):
        live = (acc_ref[...] > t).astype(F32)
        weights.append(over_lanes(jax.nn.sigmoid(pb_ref[t]) * live))
        logs.append(over_lanes(pd_ref[t] * live))
        wr(kq, pl.ds(t, seqs, stride=pad), keys[t])
        wr(kq, pl.ds(props + t, seqs, stride=pad), keys[t])
    state_in.wait()
    lax.fori_loop(0, seqs, by_state, 0, unroll=4)
    cumul, growth, update, _ = solve(keys, values, weights, logs, None)
    al[...] = growth[-1]
    for t in range(props):
        wr(tk, pl.ds(t, seqs, stride=pad), jnp.exp(cumul[-1] - cumul[t]) * keys[t])
        wr(up, pl.ds(t, seqs, stride=pad), update[t])
        wr(tk, pl.ds(props + t, seqs, stride=pad), jnp.zeros((seqs, width), F32))
        wr(up, pl.ds(props + t, seqs, stride=pad), jnp.zeros((seqs, width), F32))

    def renew(s, carry):
        at = pl.ds(pl.multiple_of(s * pad, pad), pad)
        outer = lax.dot_general(
            rd(tk, at), rd(up, at), (((0,), (0,)), ((), ())), preferred_element_type=F32)
        where = pl.ds(pl.multiple_of(s * hd, hd), hd)
        tile = al[pl.ds(s, 1), :] * st[where, :]
        for h in range(heads):
            tile = tile + masks[h] * outer[h * hd : (h + 1) * hd, :]
        st[where, :] = tile
        return carry

    forward(0)
    send_own(3)
    lax.fori_loop(0, seqs // 2, renew, 0, unroll=2)
    forward(1)
    if gather_out:
        send_own(n_mat - 1)
    lax.fori_loop(seqs // 2, seqs, renew, 0, unroll=2)
    state_out = pltpu.make_async_copy(st, new_hbm, out_sem)
    state_out.start()

    for d in range(1, n_tp):
        t_wait(d)
    for copy in late:
        copy.wait()
    square = jnp.zeros((rows, 1), F32)
    for i in range(n_tp):
        wide = tok[i].astype(F32).reshape(rows, -1)
        square = square + jnp.sum(wide * wide, -1, keepdims=True)
    feats = tok.shape[3]
    scale = lax.rsqrt(square / (n_tp * feats) + EPS)
    for i in range(n_tp):
        cols = slice(i * feats, (i + 1) * feats)
        normed[:, cols] = (tok[i].astype(F32).reshape(rows, -1) * scale * gain_ref[:, cols]).astype(BF16)
    all_heads = wb_ref.shape[0]
    pick = (
        lax.broadcasted_iota(jnp.int32, (all_heads, width), 0)
        == t_me * heads + lax.broadcasted_iota(jnp.int32, (all_heads, width), 1) // hd
    ).astype(F32)

    def per_head(ref):
        raw = lax.dot_general(
            normed[...], ref[...], (((1,), (1,)), ((), ())), preferred_element_type=F32)
        return jnp.dot(raw, pick, precision=lax.Precision.HIGHEST, preferred_element_type=F32)

    wr(rows_a, every, jax.nn.sigmoid(per_head(wb_ref)))
    weights = split(rows_a)
    base = jnp.zeros((1, width), F32)
    for h in range(heads):
        base = jnp.where(lane_head == h, base_ref[:, h : h + 1], base)
    wr(rows_b, every, -base * jax.nn.softplus(per_head(wd_ref)))
    logs = split(rows_b)

    def project(m):
        return jnp.dot(normed[...], wp[m], preferred_element_type=F32)

    def finish(m):
        wait_y(m)
        if m < len(sources):
            value = project(m)
            if m == 0:
                value = value * lax.rsqrt(head_sum(value * value) + EPS)
            elif m == 1:
                value = value * lax.rsqrt(head_sum(value * value) + EPS) * hd ** (-0.5)
            wr(proj, every, value, m)

    outs = None
    def r_copy(dest):
        return pltpu.make_async_remote_copy(
            send_buf.at[dest], recv_buf.at[t_me], r_send.at[dest], r_recv.at[t_me],
            device_id={"tp": dest}, device_id_type=MESH)

    def r_wait(origin):
        pltpu.make_async_remote_copy(
            send_buf.at[origin], recv_buf.at[origin], r_send.at[origin], r_recv.at[origin],
            device_id={"tp": origin}, device_id_type=MESH).wait_recv()

    def send_share(dest):
        share = jnp.dot(gate_buf[...], wo[dest], preferred_element_type=F32)

        @pl.when(dest == t_me)
        def _():
            own_share[...] = share

        @pl.when(dest != t_me)
        def _():
            send_buf[dest] = share.astype(BF16)
            r_copy(dest).start()

    for m in range(len(sources)):
        if m >= 2:
            forward(m)
        if m >= 1:
            finish(m - 1)
        if m == 3:
            keys = [rd(proj, pl.ds(t, seqs, stride=props), 0) for t in range(props)]
            queries = [rd(proj, pl.ds(t, seqs, stride=props), 1) for t in range(props)]
            values = [rd(proj, pl.ds(t, seqs, stride=props), 2) for t in range(props)]
            for t in range(props):
                wr(kq, pl.ds(t, seqs, stride=pad), keys[t])
                wr(kq, pl.ds(props + t, seqs, stride=pad), queries[t])
            lax.fori_loop(0, seqs, by_state, 0, unroll=4)
            outs = solve(keys, values, weights, logs, queries)[3]
            for t in range(props):
                wr(rows_a, pl.ds(t, seqs, stride=props), outs[t])
            out = rd(rows_a, every)
            out = out * lax.rsqrt(head_sum(out * out) / hd + EPS)
            tile_gain = (
                lax.broadcasted_iota(jnp.int32, (hd, width), 0)
                == lax.broadcasted_iota(jnp.int32, (hd, width), 1) % hd
            ).astype(F32)
            gain = jnp.dot(
                jnp.broadcast_to(og_ref[...], (8, hd)), tile_gain,
                precision=lax.Precision.HIGHEST, preferred_element_type=F32)[:1]
            wr(rows_a, every, out * gain)
    finish(len(sources) - 1)
    gate = rd(proj, every, 3)
    gate_buf[...] = (rd(rows_a, every) * (gate / (1.0 + jnp.exp(-gate)))).astype(BF16)
    if gather_out:
        m = n_mat - 1

        def take(s, carry):
            @pl.when(s < n_kv - 1)
            def _():
                forward_step(m, s)

            @pl.when(k - s >= 0)
            def _():
                @pl.when(s > 0)
                def _():
                    for d in range(1, n_grp):
                        y_wait(m, k - s, d)

                send_share(k - s)

            @pl.when(jnp.logical_and(s > 0, k + s < n_kv))
            def _():
                for d in range(1, n_grp):
                    y_wait(m, k + s, d)
                send_share(k + s)

            return carry

        lax.fori_loop(0, n_kv, take, 0)
    else:
        out_in.wait()
        for d in range(n_tp):
            send_share(lax.rem(t_me + d, n_tp))
    total = own_share[...]
    for d in range(1, n_tp):
        origin = lax.rem(t_me + d, n_tp)
        r_wait(origin)
        total = total + recv_buf[origin].astype(F32)
    mixed_ref[...] = total.reshape(seqs, props, feats).astype(BF16)

    for d in range(1, n_tp):
        t_copy(d).wait_send()
        r_copy(lax.rem(t_me + d, n_tp)).wait_send()

    def drain(m):
        def step(o, carry):
            @pl.when(jnp.logical_and(o <= k, k < n_kv - 1))
            def _():
                z_right(m, o).wait_send()

            @pl.when(jnp.logical_and(o >= k, k > 0))
            def _():
                z_left(m, o).wait_send()

            @pl.when(o != k)
            def _():
                for d in range(1, n_grp):
                    y_copy(m, o, d).wait_send()

            return carry

        lax.fori_loop(0, n_kv, step, 0)

    for m in range(n_mat):
        drain(m)
    state_out.wait()


def pair_kernel(
    cfg,
    tok_hbm, gain_hbm, wq_hbm, wk_hbm, wv_hbm, wg_hbm, wb_hbm, wd_hbm, base_hbm, og_hbm, wo_hbm,
    state_hbm, pk_hbm, pv_hbm, pb_hbm, pd_hbm, acc_hbm,
    mixed_ref, st,
    gain_ref, wbd_ref, base_ref, og_ref, pk_ref, pv_ref, pb_ref, pd_ref, acc_ref, tok, wp, wo, normed, kq, res, tk, up, al, rows_a, rows_b, proj, own_part, part_send, part_recv, small_own, small_send, small_recv, send_buf, recv_buf, gate_buf, own_share,
    in_sem, own_sem, wz_send, wz_recv, wy_send, wy_recv, t_send, f_send, d_send, t_recv, zr_send, zl_send, z_recv, y_send, y_recv, p_send, p_recv, r_send, r_recv,
    small_sem,
):
    n_grp, n_kv, n_tp, seqs, props, heads, hd = cfg
    width = heads * hd
    g = lax.axis_index("grp")
    k = lax.axis_index("kv")
    t_me = lax.axis_index("tp")
    rows = seqs * props
    own_rows = wk_hbm.shape[0]
    piece = own_rows // n_grp
    out_piece = wo.shape[1] // n_grp
    out_bits = 2
    w_bits = 2
    out_bit = out_piece // out_bits
    feats = tok_hbm.shape[2]
    sources = [wk_hbm, wq_hbm, wv_hbm, wg_hbm]
    n_src = len(sources)
    all_heads = wb_hbm.shape[0]
    pair = k // 2
    side = lax.rem(k, 2)
    mate = k + 1 - 2 * side
    partner = lax.rem(k + n_kv // 2, n_kv)
    chip = t_me // 2
    core = lax.rem(t_me, 2)
    beside_core = 2 * chip + 1 - core
    home = lax.rem(pair + chip + 1, 2)
    g_other = lax.rem(g + 1, n_grp)
    half_feats = 2 * feats

    own_slot = home * (2 + core) + (1 - home) * 4
    tok_in = pltpu.make_async_copy(tok_hbm, tok.at[own_slot], in_sem.at[0])
    tok_in.start()
    own_copies = []
    for m in range(n_src + 1):
        if m < n_src:
            dst = wp.at[m, pl.ds(side * own_rows, own_rows), :]
            copy = pltpu.make_async_copy(sources[m], dst, own_sem.at[m])
        else:
            copy = pltpu.make_async_copy(wo_hbm, wo.at[k], own_sem.at[m])
        copy.start()
        own_copies.append(copy)
    early, late = [], []
    ours = pl.ds(pl.multiple_of(pair * half_feats, half_feats), half_feats)
    pairs = [
        (pk_hbm, pk_ref, early), (pv_hbm, pv_ref, early), (pb_hbm, pb_ref, early),
        (pd_hbm, pd_ref, early), (acc_hbm, acc_ref, early),
        (gain_hbm.at[:, ours], gain_ref, late),
        (wb_hbm.at[:, ours], wbd_ref.at[pl.ds(0, all_heads), :], late),
        (wd_hbm.at[:, ours], wbd_ref.at[pl.ds(all_heads, all_heads), :], late),
        (base_hbm, base_ref, late), (og_hbm, og_ref, late),
    ]
    for i, (src, dst, group) in enumerate(pairs):
        copy = pltpu.make_async_copy(src, dst, small_sem.at[i])
        copy.start()
        group.append(copy)
    state_in = pltpu.make_async_copy(state_hbm, st, in_sem.at[1])
    state_in.start()

    barrier = pltpu.get_barrier_semaphore()

    def greet(dev):
        pl.semaphore_signal(barrier, inc=1, device_id=dev, device_id_type=MESH)

    for d in range(1, n_kv):
        greet({"kv": lax.rem(k + d, n_kv)})
    for d in range(1, n_tp):
        greet({"tp": lax.rem(t_me + d, n_tp)})
    greet({"grp": g_other})
    far_tp = 2 * (1 - chip) + core
    pl.semaphore_wait(barrier, n_kv + n_tp - 1)

    def remote(src, dst, send, recv, dev):
        return pltpu.make_async_remote_copy(
            src, dst, send, recv, device_id=dev, device_id_type=MESH)

    part = seqs // 2

    def tok_piece(slot, half):
        return tok.at[slot, pl.ds(half * part, part)]

    def tok_partner():
        return remote(tok_piece(4, 0), tok_piece(core, 0), t_send.at[0],
                      t_recv.at[core, 0], {"kv": partner})

    def tok_shift():
        return remote(tok_piece(4, 1), tok_piece(5, 1), t_send.at[1], t_recv.at[4, 1],
                      {"tp": far_tp})

    def tok_relay():
        return remote(tok_piece(5, 1), tok_piece(core, 1), t_send.at[0],
                      t_recv.at[core, 1], {"kv": partner})

    def tok_far(slot, half):
        ref = tok_piece(slot, half)
        return remote(ref, ref, f_send.at[slot // 2, half], t_recv.at[slot, half],
                      {"tp": far_tp})

    def tok_beside(slot, half):
        ref = tok_piece(slot, half)
        return remote(ref, ref, d_send.at[slot // 2, half], t_recv.at[slot, half],
                      {"tp": beside_core})

    def tok_wait(slot, half):
        ref = tok_piece(slot, half)
        remote(ref, ref, d_send.at[0, half], t_recv.at[slot, half],
               {"tp": beside_core}).wait_recv()

    def tok_land_z():
        tok_wait(core, 1 - home)
        tok_far(core, 1 - home).start()
        tok_beside(core, 1 - home).start()

    def tok_land_x():
        tok_wait(core, home)
        tok_beside(core, home).start()

    def w_slot(m, block, half, bit):
        at = pl.ds(block * own_rows + half * piece + bit * (piece // w_bits), piece // w_bits)
        return wp.at[m, at, :]

    def w_mate(m, bit):
        ref = w_slot(m, side, g, bit)
        return remote(ref, ref, wz_send.at[m, bit], wz_recv.at[m, bit], {"kv": mate})

    def w_share(m, bit):
        ref = w_slot(m, 1 - side, g, bit)
        return remote(ref, ref, wy_send.at[m, bit], wy_recv.at[m, bit], {"grp": g_other})

    def w_pass(m):
        for bit in range(w_bits):
            ref = w_slot(m, 1 - side, g, bit)
            remote(ref, ref, wz_send.at[m, bit], wz_recv.at[m, bit], {"kv": mate}).wait_recv()
            w_share(m, bit).start()

    def w_ready(m):
        for bit in range(w_bits):
            ref = w_slot(m, 1 - side, g_other, bit)
            remote(ref, ref, wy_send.at[m, bit], wy_recv.at[m, bit], {"grp": g_other}).wait_recv()

    def o_slot(origin, part, bit):
        return wo.at[origin, pl.ds(part * out_piece + bit * out_bit, out_bit), :]

    def z_right(origin, bit):
        ref = o_slot(origin, g, bit)
        return remote(ref, ref, zr_send.at[origin, bit], z_recv.at[origin, bit], {"kv": k + 1})

    def z_left(origin, bit):
        ref = o_slot(origin, g, bit)
        return remote(ref, ref, zl_send.at[origin, bit], z_recv.at[origin, bit], {"kv": k - 1})

    def y_copy(origin, bit):
        ref = o_slot(origin, g, bit)
        return remote(ref, ref, y_send.at[origin, bit], y_recv.at[origin, bit], {"grp": g_other})

    def y_wait(origin):
        for bit in range(out_bits):
            ref = o_slot(origin, g_other, bit)
            remote(ref, ref, y_send.at[origin, bit], y_recv.at[origin, bit],
                   {"grp": g_other}).wait_recv()

    def right_start(origin):
        for bit in range(out_bits):
            z_right(origin, bit).start()

    def left_start(origin):
        for bit in range(out_bits):
            z_left(origin, bit).start()

    def from_left(origin):
        for bit in range(out_bits):
            z_right(origin, bit).wait_recv()

            @pl.when(k < n_kv - 1)
            def _():
                z_right(origin, bit).start()

    def from_right(origin):
        for bit in range(out_bits):
            z_left(origin, bit).wait_recv()

            @pl.when(k > 0)
            def _():
                z_left(origin, bit).start()

    def share_out(origin):
        for bit in range(out_bits):
            y_copy(origin, bit).start()

    def middle_pass(s):
        @pl.when(jnp.logical_and(side == 1, pair == 0))
        def _():
            if s == 0:
                from_left(k - 1)
            else:
                from_right(k + s)

        @pl.when(jnp.logical_and(side == 0, pair == 1))
        def _():
            if s == 0:
                from_right(k + 1)
            else:
                from_left(k - s)

    def middle_share(s):
        @pl.when(jnp.logical_and(side == 1, pair == 0))
        def _():
            share_out(k - 1 if s == 0 else k + s)

        @pl.when(jnp.logical_and(side == 0, pair == 1))
        def _():
            share_out(k + 1 if s == 0 else k - s)

    def end_pass(s):
        @pl.when(k == 0)
        def _():
            from_right(k + s)
            share_out(k + s)

        @pl.when(k == n_kv - 1)
        def _():
            from_left(k - s)
            share_out(k - s)

    def p_copy(m, b):
        at = pl.ds(b * half_rows, half_rows)
        return remote(part_send.at[m, at], part_recv.at[m, at], p_send.at[m, b],
                      p_recv.at[m, b], {"kv": partner})

    def small_copy():
        return remote(small_send, small_recv, p_send.at[n_src, 0], p_recv.at[n_src, 0],
                      {"kv": partner})

    at_end = jnp.logical_or(k == 0, k == n_kv - 1)
    tok_in.wait()

    @pl.when(home == 0)
    def _():
        tok_shift().start()
        tok_partner().start()

    @pl.when(home == 1)
    def _():
        for half in range(2):
            tok_far(2 + core, half).start()
            tok_beside(2 + core, half).start()

    def w_first(m):
        own_copies[m].wait()
        for bit in range(w_bits):
            w_mate(m, bit).start()

    w_first(0)
    own_copies[n_src].wait()

    def w_rest():
        @pl.when(k == 0)
        def _():
            right_start(k)

        @pl.when(k == n_kv - 1)
        def _():
            left_start(k)

        w_first(1)
        w_first(2)
        w_first(3)

    relays_first = jnp.logical_and(at_end, home == 1)

    @pl.when(jnp.logical_not(relays_first))
    def _():
        w_rest()

    blk = (
        lax.broadcasted_iota(jnp.int32, (width, width), 0) // hd
        == lax.broadcasted_iota(jnp.int32, (width, width), 1) // hd
    ).astype(F32).astype(BF16)
    lane_head = lax.broadcasted_iota(jnp.int32, (1, width), 1) // hd
    masks = [(lane_head == h).astype(F32) for h in range(heads)]

    def head_sum(x):
        hi = x.astype(BF16)
        lo = (x - hi.astype(F32)).astype(BF16)
        return jnp.dot(hi, blk, preferred_element_type=F32) + jnp.dot(
            lo, blk, preferred_element_type=F32)

    lanes = 128
    blocks = width // lanes

    def rd(ref, at, *lead):
        return jnp.concatenate([ref[(*lead, c, at)] for c in range(blocks)], axis=-1)

    def wr(ref, at, x, *lead):
        for c in range(blocks):
            ref[(*lead, c, at)] = x[:, c * lanes : (c + 1) * lanes]

    every = pl.ds(0, rows)
    count = seqs // 2
    half_rows = count * props

    pad = 2 * props

    def head_first(x, head):
        block, at = divmod(head * hd, lanes)
        x = x[:, block * lanes : (block + 1) * lanes]
        return jnp.concatenate([x[:, at:], x[:, :at]], axis=-1) if at else x

    def put_heads(ref, x, first, each, low=0):
        step = heads * each
        for head in range(heads):
            at = pl.ds(low * step + head * each + first, x.shape[0], stride=step)
            ref[at] = head_first(x, head)

    def by_state(s, carry):
        at = pl.ds(pl.multiple_of(s * heads * pad, heads * pad), heads * pad)
        tile = st[pl.ds(pl.multiple_of(s * hd, hd), hd), :].astype(BF16)
        found = jnp.dot(kq[at, :hd].astype(BF16), tile, preferred_element_type=F32)
        own = masks[0] * found[:pad]
        for head in range(1, heads):
            own = own + masks[head] * found[head * pad : (head + 1) * pad]
        wr(res, pl.ds(pl.multiple_of(s * pad, pad), pad), own)
        return carry

    def solve(keys, values, weights, logs, queries, start=0):
        count = keys[0].shape[0]
        cumul = []
        run = None
        for t in range(props):
            run = logs[t] if run is None else run + logs[t]
            cumul.append(run)
        low = [(i, j) for i in range(props) for j in range(i)]
        products = [keys[i] * keys[j] for i, j in low]
        full = []
        if queries is not None:
            full = [(i, j) for i in range(props) for j in range(i + 1)]
            products += [queries[i] * keys[j] for i, j in full]
        sums = head_sum(jnp.concatenate(products, axis=0))
        sums = [sums[i * count : (i + 1) * count] for i in range(len(products))]
        kk = dict(zip(low, sums))
        qk = dict(zip(full, sums[len(low):]))
        dec = {pair: jnp.exp(cumul[pair[0]] - cumul[pair[1]]) for pair in low}
        growth = [jnp.exp(c) for c in cumul]
        update = []
        for t in range(props):
            seen = rd(res, pl.ds(start * pad + t, count, stride=pad))
            term = values[t] - growth[t] * seen
            for j in range(t):
                term = term - kk[t, j] * dec[t, j] * update[j]
            update.append(weights[t] * term)
        outs = []
        if queries is not None:
            for t in range(props):
                out = growth[t] * rd(
                    res, pl.ds(start * pad + props + t, count, stride=pad))
                for j in range(t + 1):
                    score = qk[t, j] if j == t else qk[t, j] * dec[t, j]
                    out = out + score * update[j]
                outs.append(out)
        return cumul, growth, update, outs

    def split(ref):
        return [rd(ref, pl.ds(t, seqs, stride=props)) for t in range(props)]

    for copy in early:
        copy.wait()
    pk = pk_ref[...].astype(F32).reshape(rows, width)
    wr(rows_a, every, pk * lax.rsqrt(head_sum(pk * pk) + EPS))
    wr(rows_b, every, pv_ref[...].astype(F32).reshape(rows, width))
    keys = split(rows_a)
    values = split(rows_b)
    own_head = (
        lax.broadcasted_iota(jnp.int32, (heads, width), 0)
        == lax.broadcasted_iota(jnp.int32, (heads, width), 1) // hd
    ).astype(F32)

    def over_lanes(x):
        return lax.dot_general(
            x, own_head, (((0,), (0,)), ((), ())),
            precision=lax.Precision.HIGHEST, preferred_element_type=F32)

    weights, logs = [], []
    for t in range(props):
        live = (acc_ref[...] > t).astype(F32)
        weights.append(over_lanes(jax.nn.sigmoid(pb_ref[t]) * live))
        logs.append(over_lanes(pd_ref[t] * live))
        put_heads(kq, keys[t], t, pad)
        put_heads(kq, keys[t], props + t, pad)
    state_in.wait()
    lax.fori_loop(0, seqs, by_state, 0, unroll=4)
    cumul, growth, update, _ = solve(keys, values, weights, logs, None)
    al[...] = growth[-1]
    for t in range(props):
        put_heads(tk, jnp.exp(cumul[-1] - cumul[t]) * keys[t], t, props)
        for head in range(heads):
            wr(up, pl.ds(head * props + t, seqs, stride=heads * props), masks[head] * update[t])

    def renew(s, carry):
        each = heads * props
        at = pl.ds(pl.multiple_of(s * each, each), each)
        outer = lax.dot_general(
            tk[at, :hd], rd(up, at), (((0,), (0,)), ((), ())), preferred_element_type=F32)
        where = pl.ds(pl.multiple_of(s * hd, hd), hd)
        st[where, :] = al[pl.ds(s, 1), :] * st[where, :] + outer
        return carry


    @pl.when(home == 1)
    def _():
        remote(tok_piece(5, 1), tok_piece(5, 1), t_send.at[1], t_recv.at[4, 1],
               {"tp": far_tp}).wait_recv()
        tok_relay().start()

    @pl.when(relays_first)
    def _():
        w_rest()

    @pl.when(home == 0)
    def _():
        for half in range(2):
            tok_wait(2 + core, half)
            tok_beside(2 + core, half).start()

    @pl.when(home == 1)
    def _():
        tok_land_z()

    w_pass(0)

    @pl.when(jnp.logical_not(at_end))
    def _():
        right_start(k)
        left_start(k)

    @pl.when(home == 0)
    def _():
        tok_land_z()
        tok_land_x()

    middle_pass(0)
    middle_share(0)

    @pl.when(home == 1)
    def _():
        tok_land_x()

    w_pass(1)
    middle_pass(1)

    for copy in late:
        copy.wait()
    for half in range(2):
        tok_wait(3 - core, half)
        tok_wait(1 - core, half)
    ones = jnp.ones((8, feats), BF16)
    squares = jnp.zeros((8, 2 * rows), F32)
    last = (((1,), (1,)), ((), ()))
    for c in range(2):
        cols = slice(c * feats, (c + 1) * feats)
        wide = jnp.concatenate(
            [tok[c].astype(F32).reshape(rows, feats), tok[2 + c].astype(F32).reshape(rows, feats)],
            axis=0)
        normed[:, cols] = (wide * gain_ref[:, cols]).astype(BF16)
        sq = wide * wide
        hi = sq.astype(BF16)
        lo = (sq - hi.astype(F32)).astype(BF16)
        squares = squares + lax.dot_general(ones, hi, last, preferred_element_type=F32)
        squares = squares + lax.dot_general(ones, lo, last, preferred_element_type=F32)
    raw = lax.dot_general(wbd_ref[...], normed[...], last, preferred_element_type=F32)
    small = jnp.concatenate([raw, squares], axis=0)
    kind = lax.broadcasted_iota(jnp.int32, (small_own.shape[0], small.shape[0]), 0)
    taken = lax.broadcasted_iota(jnp.int32, (small_own.shape[0], small.shape[0]), 1)
    first_head = t_me * heads
    wanted = jnp.where(
        kind < heads, first_head + kind,
        jnp.where(kind < 2 * heads, all_heads + first_head + kind - heads, 2 * all_heads))
    small = jnp.dot(
        (taken == wanted).astype(F32), small,
        precision=lax.Precision.HIGHEST, preferred_element_type=F32)
    small_send[...] = small[:, :rows]
    small_copy().start()
    small_own[...] = small[:, rows:]

    def project(m):
        both = jnp.dot(normed[...], wp[m], preferred_element_type=F32)
        part_send[m] = both[:rows].astype(BF16)
        own_part[m] = both[rows:]

    def give(*pieces):
        for m, b in pieces:
            p_copy(m, b).start()

    w_ready(0)
    project(0)
    give((0, 0), (0, 1))
    w_pass(2)
    w_ready(1)
    project(1)
    give((1, 0))
    middle_pass(2)
    w_pass(3)
    end_pass(1)
    middle_share(1)
    middle_share(2)
    w_ready(2)
    project(2)
    give((2, 0), (1, 1))
    lax.fori_loop(0, seqs // 2, renew, 0, unroll=4)
    w_ready(3)
    project(3)
    give((3, 0), (2, 1), (3, 1))
    end_pass(2)
    lax.fori_loop(seqs // 2, seqs, renew, 0, unroll=4)

    small_copy().wait_recv()
    small = small_own[...] + small_recv[...]
    scale = lax.rsqrt(small[2 * heads :] / (n_tp * feats) + EPS)
    beta = small[:heads] * scale[:1]
    decay = small[heads : 2 * heads] * scale[:1]

    def spread(x, over):
        return lax.dot_general(
            x, over, (((0,), (0,)), ((), ())),
            precision=lax.Precision.HIGHEST, preferred_element_type=F32)

    wr(rows_a, every, spread(jax.nn.sigmoid(beta), own_head))
    base = jnp.zeros((1, width), F32)
    for h in range(heads):
        base = jnp.where(lane_head == h, base_ref[:, h : h + 1], base)
    wr(rows_b, every, -base * spread(jax.nn.softplus(decay), own_head))
    row_scale = spread(
        scale, (lax.broadcasted_iota(jnp.int32, (scale.shape[0], width), 0) == 0).astype(F32))

    def finish(m, b):
        p_copy(m, b).wait_recv()
        at = slice(b * half_rows, (b + 1) * half_rows)
        value = (own_part[m, at] + part_recv[m, at].astype(F32)) * row_scale[at]
        if m == 0:
            value = value * lax.rsqrt(head_sum(value * value) + EPS)
        elif m == 1:
            value = value * lax.rsqrt(head_sum(value * value) + EPS) * hd ** (-0.5)
        wr(proj, pl.ds(b * half_rows, half_rows), value, m)

    def r_copy(dest, b):
        at = pl.ds(b * half_rows, half_rows)
        return remote(send_buf.at[dest, at], recv_buf.at[t_me, at], r_send.at[dest, b],
                      r_recv.at[t_me, b], {"tp": dest})

    def r_wait(origin, b):
        at = pl.ds(b * half_rows, half_rows)
        remote(send_buf.at[origin, at], recv_buf.at[origin, at], r_send.at[origin, b],
               r_recv.at[origin, b], {"tp": origin}).wait_recv()

    def send_share(dest, b):
        at = slice(b * half_rows, (b + 1) * half_rows)
        share = jnp.dot(gate_buf[at], wo[dest], preferred_element_type=F32)

        @pl.when(dest == t_me)
        def _():
            own_share[at] = share

        @pl.when(dest != t_me)
        def _():
            send_buf[dest, at] = share.astype(BF16)
            r_copy(dest, b).start()

    tile_gain = (
        lax.broadcasted_iota(jnp.int32, (hd, width), 0)
        == lax.broadcasted_iota(jnp.int32, (hd, width), 1) % hd
    ).astype(F32)
    gain = jnp.dot(
        jnp.broadcast_to(og_ref[...], (8, hd)), tile_gain,
        precision=lax.Precision.HIGHEST, preferred_element_type=F32)[:1]

    def delta(b):
        low, first = b * count, b * half_rows
        steps = [pl.ds(first + t, count, stride=props) for t in range(props)]
        for m in range(3):
            finish(m, b)
        keys, queries, values = [[rd(proj, at, m) for at in steps] for m in range(3)]
        weights = [rd(rows_a, at) for at in steps]
        logs = [rd(rows_b, at) for at in steps]
        for t in range(props):
            put_heads(kq, keys[t], t, pad, low)
            put_heads(kq, queries[t], props + t, pad, low)
        lax.fori_loop(low, low + count, by_state, 0, unroll=4)
        outs = solve(keys, values, weights, logs, queries, low)[3]
        for t in range(props):
            wr(rows_a, steps[t], outs[t])
        half = pl.ds(first, half_rows)
        out = rd(rows_a, half)
        out = out * lax.rsqrt(head_sum(out * out) / hd + EPS) * gain
        finish(n_src - 1, b)
        gate = rd(proj, half, 3)
        gate_buf[first : first + half_rows] = (
            out * (gate / (1.0 + jnp.exp(-gate)))).astype(BF16)

    def take(b):
        def step(s, carry):
            @pl.when(k - s >= 0)
            def _():
                if b == 0:
                    @pl.when(s > 0)
                    def _():
                        y_wait(k - s)

                send_share(k - s, b)

            @pl.when(jnp.logical_and(s > 0, k + s < n_kv))
            def _():
                if b == 0:
                    y_wait(k + s)
                send_share(k + s, b)

            return carry

        return step

    def settle(b):
        at = slice(b * half_rows, (b + 1) * half_rows)
        total = own_share[at]
        for d in range(1, n_tp):
            origin = lax.rem(t_me + d, n_tp)
            r_wait(origin, b)
            total = total + recv_buf[origin, at].astype(F32)
        mixed_ref[b * count : (b + 1) * count] = total.reshape(count, props, feats).astype(BF16)

    delta(0)
    end_pass(3)
    lax.fori_loop(0, n_kv // 2, take(0), 0)
    delta(1)
    lax.fori_loop(n_kv // 2, n_kv - 1, take(0), 0)
    lax.fori_loop(0, n_kv - 1, take(1), 0)
    lax.fori_loop(n_kv - 1, n_kv, take(0), 0)
    lax.fori_loop(n_kv - 1, n_kv, take(1), 0)
    settle(0)
    settle(1)

    for half in range(2):
        tok_beside(core, half).wait_send()
        tok_beside(2 + core, half).wait_send()
    tok_far(core, 1 - home).wait_send()

    @pl.when(home == 1)
    def _():
        tok_far(2 + core, 0).wait_send()
        tok_far(2 + core, 1).wait_send()
        tok_relay().wait_send()

    @pl.when(home == 0)
    def _():
        tok_partner().wait_send()
        tok_shift().wait_send()

    for m in range(n_src):
        for bit in range(w_bits):
            w_mate(m, bit).wait_send()
            w_share(m, bit).wait_send()
        p_copy(m, 0).wait_send()
        p_copy(m, 1).wait_send()
    small_copy().wait_send()
    for d in range(1, n_tp):
        r_copy(lax.rem(t_me + d, n_tp), 0).wait_send()
        r_copy(lax.rem(t_me + d, n_tp), 1).wait_send()

    def drain(o, carry):
        for bit in range(out_bits):
            @pl.when(jnp.logical_and(o <= k, k < n_kv - 1))
            def _():
                z_right(o, bit).wait_send()

            @pl.when(jnp.logical_and(o >= k, k > 0))
            def _():
                z_left(o, bit).wait_send()

            @pl.when(o != k)
            def _():
                y_copy(o, bit).wait_send()

        return carry

    lax.fori_loop(0, n_kv, drain, 0)


def pair_call(sizes, args, seqs, props, feats, heads, hd, width, rows, pad):
    n_grp, n_kv, n_tp = sizes
    cfg = (n_grp, n_kv, n_tp, seqs, props, heads, hd)
    vmem = pl.BlockSpec(memory_space=pltpu.VMEM)
    hbm = pl.BlockSpec(memory_space=pltpu.HBM)
    dma = pltpu.SemaphoreType.DMA
    own_rows = args[2].shape[0]
    all_heads = args[6].shape[0]
    n_src = 4
    small = (2 * heads + 8, rows)
    return pl.pallas_call(
        functools.partial(pair_kernel, cfg),
        out_shape=(
            pltpu.VMEM((seqs, props, feats), BF16),
            pltpu.VMEM((seqs * hd, width), F32),
        ),
        in_specs=[hbm] * len(args),
        out_specs=(vmem, vmem),
        scratch_shapes=[
            pltpu.VMEM((1, 2 * feats), F32),
            pltpu.VMEM((2 * all_heads, 2 * feats), BF16),
            *[pltpu.VMEM(args[i].shape, args[i].dtype) for i in (8, 9, 12, 13, 14, 15, 16)],
            pltpu.VMEM((6, seqs, props, feats), BF16),
            pltpu.VMEM((n_src, 2 * own_rows, width), BF16),
            pltpu.VMEM((n_tp, width, feats), BF16),
            pltpu.VMEM((2 * rows, 2 * feats), BF16),
            pltpu.VMEM((seqs * heads * pad, 128), F32),
            pltpu.VMEM((width // 128, seqs * pad, 128), F32),
            pltpu.VMEM((seqs * heads * props, 128), F32),
            pltpu.VMEM((width // 128, seqs * heads * props, 128), F32),
            pltpu.VMEM((seqs, width), F32),
            pltpu.VMEM((width // 128, rows, 128), F32),
            pltpu.VMEM((width // 128, rows, 128), F32),
            pltpu.VMEM((n_src, width // 128, rows, 128), F32),
            pltpu.VMEM((n_src, rows, width), F32),
            pltpu.VMEM((n_src, rows, width), BF16),
            pltpu.VMEM((n_src, rows, width), BF16),
            pltpu.VMEM(small, F32),
            pltpu.VMEM(small, F32),
            pltpu.VMEM(small, F32),
            pltpu.VMEM((n_tp, rows, feats), BF16),
            pltpu.VMEM((n_tp, rows, feats), BF16),
            pltpu.VMEM((rows, width), BF16),
            pltpu.VMEM((rows, feats), F32),
            dma((2,)),
            dma((n_src + 1,)),
            *[dma((n_src, 2)) for _ in range(4)],
            dma((2,)),
            dma((2, 2)),
            dma((2, 2)),
            dma((5, 2)),
            *[dma((n_kv, 2)) for _ in range(5)],
            dma((n_src + 1, 2)),
            dma((n_src + 1, 2)),
            dma((n_tp, 2)),
            dma((n_tp, 2)),
            dma((10,)),
        ],
        compiler_params=pltpu.CompilerParams(
            collective_id=1, has_side_effects=True, vmem_limit_bytes=67043328 - rows * feats * 2 - seqs * hd * width * 4),
    )(*args)


def body(
    sizes,
    tokens, in_gain, w_query, w_key, w_value, w_gate, w_beta, w_decay, decay_base, out_gain, w_out,
    state, prev_keys, prev_values, prev_beta, prev_decay, accepted,
):
    n_grp, n_kv, n_tp = sizes
    seqs, props, feats = tokens.shape
    heads = decay_base.shape[0]
    hd = out_gain.shape[0]
    width = heads * hd
    rows = seqs * props
    pad = 2 * props
    paired = (
        n_grp == 2 and n_kv == n_tp and n_kv // 2 == 2
        and w_query.shape[0] == feats and w_query.shape[0] * n_kv == in_gain.shape[0])
    gather_out = n_kv == n_tp
    if not gather_out:
        w_out = lax.all_gather(w_out, "kv", axis=1, tiled=True)
        w_out = jnp.transpose(w_out.reshape(width, n_tp, feats), (1, 0, 2))
    n_mat = 5 if gather_out else 4
    cfg = (n_grp, n_kv, n_tp, seqs, props, heads, hd, gather_out)
    vmem = pl.BlockSpec(memory_space=pltpu.VMEM)
    hbm = pl.BlockSpec(memory_space=pltpu.HBM)
    args = (
        tokens, in_gain.reshape(1, -1), w_query, w_key, w_value, w_gate,
        w_beta.T, w_decay.T, decay_base.reshape(1, -1), out_gain.reshape(1, -1), w_out,
        state.reshape(seqs * hd, width), prev_keys, prev_values,
        jnp.transpose(prev_beta, (1, 2, 0)), jnp.transpose(prev_decay, (1, 2, 0)),
        accepted.reshape(1, seqs),
    )
    if paired:
        mixed, new_state = pair_call(
            sizes, args, seqs, props, feats, heads, hd, width, rows, pad)
        return mixed, new_state.reshape(seqs, hd, width)
    dma = pltpu.SemaphoreType.DMA
    mixed, new_state = pl.pallas_call(
        functools.partial(kernel, cfg),
        out_shape=(
            jax.ShapeDtypeStruct((seqs, props, feats), BF16),
            jax.ShapeDtypeStruct((seqs * hd, width), F32),
        ),
        in_specs=[hbm] * len(args),
        out_specs=(vmem, pl.BlockSpec(memory_space=pl.ANY)),
        scratch_shapes=[
            *[pltpu.VMEM(args[i].shape, args[i].dtype) for i in (1, 6, 7, 8, 9, 12, 13, 14, 15, 16)],
            pltpu.VMEM((n_tp, seqs, props, feats), BF16),
            pltpu.VMEM((4, n_kv * w_key.shape[0], width), BF16),
            pltpu.VMEM((n_tp, width, feats), BF16),
            pltpu.VMEM((seqs * hd, width), F32),
            pltpu.VMEM((rows, n_tp * feats), BF16),
            pltpu.VMEM((width // 128, seqs * pad, 128), F32),
            pltpu.VMEM((width // 128, seqs * pad, 128), F32),
            pltpu.VMEM((width // 128, seqs * pad, 128), F32),
            pltpu.VMEM((width // 128, seqs * pad, 128), F32),
            pltpu.VMEM((seqs, width), F32),
            pltpu.VMEM((width // 128, rows, 128), F32),
            pltpu.VMEM((width // 128, rows, 128), F32),
            pltpu.VMEM((4, width // 128, rows, 128), F32),
            pltpu.VMEM((n_tp, rows, feats), BF16),
            pltpu.VMEM((n_tp, rows, feats), BF16),
            pltpu.VMEM((rows, width), BF16),
            pltpu.VMEM((rows, feats), F32),
            dma((2,)),
            dma((6,)),
            dma((n_mat, n_kv)),
            dma((n_mat, n_kv)),
            dma((n_mat, n_kv)),
            dma((max(n_grp - 1, 1), n_mat, n_kv)),
            dma((max(n_grp - 1, 1), n_mat, n_kv)),
            dma((n_tp - 1,)),
            dma((n_tp - 1,)),
            dma((n_tp,)),
            dma((n_tp,)),
            dma(()),
            dma((10,)),
        ],
        compiler_params=pltpu.CompilerParams(
            collective_id=0, has_side_effects=True, vmem_limit_bytes=67043328),
    )(*args)
    return mixed, new_state.reshape(seqs, hd, width)


def solution(mesh):
    sizes = (mesh.shape["grp"], mesh.shape["kv"], mesh.shape["tp"])
    tokens = P(("grp", "kv"), None, "tp")
    placed = (
        tokens, P(), P("kv", "tp"), P("kv", "tp"), P("kv", "tp"), P("kv", "tp"), P(), P(),
        P("tp"), P(), P("tp", "kv"), tokens, tokens, tokens, tokens, tokens, P(("grp", "kv")),
    )
    return jax.shard_map(
        functools.partial(body, sizes),
        mesh=mesh,
        in_specs=placed,
        out_specs=(tokens, tokens),
        check_vma=False,
    )
```

```python
import functools

import jax
import jax.numpy as jnp
from jax import lax
from jax.experimental import pallas as pl
from jax.experimental.pallas import tpu as pltpu
from jax.sharding import PartitionSpec as P

EPS = 1e-06
F32 = jnp.float32
BF16 = jnp.bfloat16
MESH = pl.DeviceIdType.MESH


def kernel(
    cfg,
    tok_hbm, gain_hbm, wq_hbm, wk_hbm, wv_hbm, wg_hbm, wb_hbm, wd_hbm, base_hbm, og_hbm, wo_hbm,
    state_hbm, pk_hbm, pv_hbm, pb_hbm, pd_hbm, acc_hbm,
    mixed_ref, new_hbm,
    gain_ref, wb_ref, wd_ref, base_ref, og_ref, pk_ref, pv_ref, pb_ref, pd_ref, acc_ref, tok, wp, wo, st, normed, kq, res, tk, up, al, rows_a, rows_b, proj, send_buf, recv_buf, gate_buf, own_share,
    in_sem, own_sem, zr_send, zl_send, z_recv, y_send, y_recv, t_send, t_recv, r_send, r_recv,
    out_sem, small_sem,
):
    n_grp, n_kv, n_tp, seqs, props, heads, hd, gather_out = cfg
    width = heads * hd
    g = lax.axis_index("grp")
    k = lax.axis_index("kv")
    t_me = lax.axis_index("tp")
    rows = seqs * props
    own_rows = wk_hbm.shape[0]
    piece = own_rows // n_grp
    out_piece = wo.shape[1] // n_grp
    sources = [wk_hbm, wq_hbm, wv_hbm, wg_hbm]
    n_mat = len(sources) + (1 if gather_out else 0)

    tok_in = pltpu.make_async_copy(tok_hbm, tok.at[t_me], in_sem.at[0])
    tok_in.start()
    own_copies = []
    for m in range(n_mat):
        if m < len(sources):
            dst = wp.at[m, pl.ds(k * own_rows, own_rows), :]
            copy = pltpu.make_async_copy(sources[m], dst, own_sem.at[m])
        else:
            copy = pltpu.make_async_copy(wo_hbm, wo.at[k], own_sem.at[m])
        copy.start()
        own_copies.append(copy)
    early, late = [], []
    pairs = [
        (pk_hbm, pk_ref, early), (pv_hbm, pv_ref, early), (pb_hbm, pb_ref, early),
        (pd_hbm, pd_ref, early), (acc_hbm, acc_ref, early), (gain_hbm, gain_ref, late),
        (wb_hbm, wb_ref, late), (wd_hbm, wd_ref, late), (base_hbm, base_ref, late),
        (og_hbm, og_ref, late),
    ]
    for i, (src, dst, group) in enumerate(pairs):
        copy = pltpu.make_async_copy(src, dst, small_sem.at[i])
        copy.start()
        group.append(copy)
    state_in = pltpu.make_async_copy(state_hbm, st, in_sem.at[1])
    state_in.start()
    out_in = None
    if not gather_out:
        out_in = pltpu.make_async_copy(wo_hbm, wo, own_sem.at[n_mat])
        out_in.start()

    barrier = pltpu.get_barrier_semaphore()

    def greet(dev):
        pl.semaphore_signal(barrier, inc=1, device_id=dev, device_id_type=MESH)

    @pl.when(k > 0)
    def _():
        greet({"kv": k - 1})

    @pl.when(k < n_kv - 1)
    def _():
        greet({"kv": k + 1})

    for d in range(1, n_grp):
        greet({"grp": lax.rem(g + d, n_grp)})
    for d in range(1, n_tp):
        greet({"tp": lax.rem(t_me + d, n_tp)})

    beside = jnp.minimum(k, 1) + jnp.minimum(n_kv - 1 - k, 1)
    pl.semaphore_wait(barrier, n_grp + n_tp - 2 + beside)

    def slot(m, origin, part):
        if m < len(sources):
            return wp.at[m, pl.ds(origin * own_rows + part * piece, piece), :]
        return wo.at[origin, pl.ds(part * out_piece, out_piece), :]

    def z_right(m, origin):
        ref = slot(m, origin, g)
        return pltpu.make_async_remote_copy(
            ref, ref, zr_send.at[m, origin], z_recv.at[m, origin],
            device_id={"kv": k + 1}, device_id_type=MESH)

    def z_left(m, origin):
        ref = slot(m, origin, g)
        return pltpu.make_async_remote_copy(
            ref, ref, zl_send.at[m, origin], z_recv.at[m, origin],
            device_id={"kv": k - 1}, device_id_type=MESH)

    def y_copy(m, origin, d):
        ref = slot(m, origin, g)
        return pltpu.make_async_remote_copy(
            ref, ref, y_send.at[d - 1, m, origin], y_recv.at[d - 1, m, origin],
            device_id={"grp": lax.rem(g + d, n_grp)}, device_id_type=MESH)

    def y_wait(m, origin, d):
        ref = slot(m, origin, lax.rem(g + n_grp - d, n_grp))
        pltpu.make_async_remote_copy(
            ref, ref, y_send.at[d - 1, m, origin], y_recv.at[d - 1, m, origin],
            device_id={"grp": lax.rem(g + d, n_grp)}, device_id_type=MESH).wait_recv()

    def send_own(m):
        own_copies[m].wait()

        @pl.when(k < n_kv - 1)
        def _():
            z_right(m, k).start()

        @pl.when(k > 0)
        def _():
            z_left(m, k).start()

    def forward_step(m, s):
        left = k - 1 - s
        right = k + 1 + s

        @pl.when(left >= 0)
        def _():
            z_right(m, left).wait_recv()

            @pl.when(k < n_kv - 1)
            def _():
                z_right(m, left).start()

            for d in range(1, n_grp):
                y_copy(m, left, d).start()

        @pl.when(right < n_kv)
        def _():
            z_left(m, right).wait_recv()

            @pl.when(k > 0)
            def _():
                z_left(m, right).start()

            for d in range(1, n_grp):
                y_copy(m, right, d).start()

    def forward(m):
        def step(s, carry):
            forward_step(m, s)
            return carry

        lax.fori_loop(0, n_kv - 1, step, 0)

    def wait_y(m):
        def step(o, carry):
            @pl.when(o != k)
            def _():
                for d in range(1, n_grp):
                    y_wait(m, o, d)

            return carry

        lax.fori_loop(0, n_kv, step, 0)

    def t_copy(d):
        return pltpu.make_async_remote_copy(
            tok.at[t_me], tok.at[t_me], t_send.at[d - 1], t_recv.at[d - 1],
            device_id={"tp": lax.rem(t_me + d, n_tp)}, device_id_type=MESH)

    def t_wait(d):
        origin = lax.rem(t_me + n_tp - d, n_tp)
        pltpu.make_async_remote_copy(
            tok.at[origin], tok.at[origin], t_send.at[d - 1], t_recv.at[d - 1],
            device_id={"tp": lax.rem(t_me + d, n_tp)}, device_id_type=MESH).wait_recv()

    send_own(0)
    tok_in.wait()
    for d in range(1, n_tp):
        t_copy(d).start()
    send_own(1)
    send_own(2)

    blk = (
        lax.broadcasted_iota(jnp.int32, (width, width), 0) // hd
        == lax.broadcasted_iota(jnp.int32, (width, width), 1) // hd
    ).astype(F32).astype(BF16)
    lane_head = lax.broadcasted_iota(jnp.int32, (1, width), 1) // hd
    masks = [(lane_head == h).astype(F32) for h in range(heads)]

    def head_sum(x):
        hi = x.astype(BF16)
        lo = (x - hi.astype(F32)).astype(BF16)
        return jnp.dot(hi, blk, preferred_element_type=F32) + jnp.dot(
            lo, blk, preferred_element_type=F32)

    lanes = 128
    blocks = width // lanes

    def rd(ref, at, *lead):
        return jnp.concatenate([ref[(*lead, c, at)] for c in range(blocks)], axis=-1)

    def wr(ref, at, x, *lead):
        for c in range(blocks):
            ref[(*lead, c, at)] = x[:, c * lanes : (c + 1) * lanes]

    every = pl.ds(0, rows)

    pad = 2 * props

    def by_state(s, carry):
        tile = st[pl.ds(pl.multiple_of(s * hd, hd), hd), :]
        stacked = jnp.concatenate([(tile * mask).astype(BF16) for mask in masks], axis=0)
        at = pl.ds(pl.multiple_of(s * pad, pad), pad)
        lhs = rd(kq, at).astype(BF16)
        wr(res, at, jnp.dot(lhs, stacked, preferred_element_type=F32))
        return carry

    def solve(keys, values, weights, logs, queries):
        cumul = []
        run = None
        for t in range(props):
            run = logs[t] if run is None else run + logs[t]
            cumul.append(run)
        low = [(i, j) for i in range(props) for j in range(i)]
        products = [keys[i] * keys[j] for i, j in low]
        full = []
        if queries is not None:
            full = [(i, j) for i in range(props) for j in range(i + 1)]
            products += [queries[i] * keys[j] for i, j in full]
        sums = head_sum(jnp.concatenate(products, axis=0))
        sums = [sums[i * seqs : (i + 1) * seqs] for i in range(len(products))]
        kk = dict(zip(low, sums))
        qk = dict(zip(full, sums[len(low):]))
        dec = {pair: jnp.exp(cumul[pair[0]] - cumul[pair[1]]) for pair in low}
        growth = [jnp.exp(c) for c in cumul]
        update = []
        for t in range(props):
            seen = rd(res, pl.ds(t, seqs, stride=pad))
            term = values[t] - growth[t] * seen
            for j in range(t):
                term = term - kk[t, j] * dec[t, j] * update[j]
            update.append(weights[t] * term)
        outs = []
        if queries is not None:
            for t in range(props):
                out = growth[t] * rd(res, pl.ds(props + t, seqs, stride=pad))
                for j in range(t + 1):
                    score = qk[t, j] if j == t else qk[t, j] * dec[t, j]
                    out = out + score * update[j]
                outs.append(out)
        return cumul, growth, update, outs

    def split(ref):
        return [rd(ref, pl.ds(t, seqs, stride=props)) for t in range(props)]

    for copy in early:
        copy.wait()
    pk = pk_ref[...].astype(F32).reshape(rows, width)
    wr(rows_a, every, pk * lax.rsqrt(head_sum(pk * pk) + EPS))
    wr(rows_b, every, pv_ref[...].astype(F32).reshape(rows, width))
    keys = split(rows_a)
    values = split(rows_b)
    own_head = (
        lax.broadcasted_iota(jnp.int32, (heads, width), 0)
        == lax.broadcasted_iota(jnp.int32, (heads, width), 1) // hd
    ).astype(F32)

    def over_lanes(x):
        return lax.dot_general(
            x, own_head, (((0,), (0,)), ((), ())),
            precision=lax.Precision.HIGHEST, preferred_element_type=F32)

    weights, logs = [], []
    for t in range(props):
        live = (acc_ref[...] > t).astype(F32)
        weights.append(over_lanes(jax.nn.sigmoid(pb_ref[t]) * live))
        logs.append(over_lanes(pd_ref[t] * live))
        wr(kq, pl.ds(t, seqs, stride=pad), keys[t])
        wr(kq, pl.ds(props + t, seqs, stride=pad), keys[t])
    state_in.wait()
    lax.fori_loop(0, seqs, by_state, 0, unroll=4)
    cumul, growth, update, _ = solve(keys, values, weights, logs, None)
    al[...] = growth[-1]
    for t in range(props):
        wr(tk, pl.ds(t, seqs, stride=pad), jnp.exp(cumul[-1] - cumul[t]) * keys[t])
        wr(up, pl.ds(t, seqs, stride=pad), update[t])
        wr(tk, pl.ds(props + t, seqs, stride=pad), jnp.zeros((seqs, width), F32))
        wr(up, pl.ds(props + t, seqs, stride=pad), jnp.zeros((seqs, width), F32))

    def renew(s, carry):
        at = pl.ds(pl.multiple_of(s * pad, pad), pad)
        outer = lax.dot_general(
            rd(tk, at), rd(up, at), (((0,), (0,)), ((), ())), preferred_element_type=F32)
        where = pl.ds(pl.multiple_of(s * hd, hd), hd)
        tile = al[pl.ds(s, 1), :] * st[where, :]
        for h in range(heads):
            tile = tile + masks[h] * outer[h * hd : (h + 1) * hd, :]
        st[where, :] = tile
        return carry

    forward(0)
    send_own(3)
    lax.fori_loop(0, seqs // 2, renew, 0, unroll=2)
    forward(1)
    if gather_out:
        send_own(n_mat - 1)
    lax.fori_loop(seqs // 2, seqs, renew, 0, unroll=2)
    state_out = pltpu.make_async_copy(st, new_hbm, out_sem)
    state_out.start()

    for d in range(1, n_tp):
        t_wait(d)
    for copy in late:
        copy.wait()
    square = jnp.zeros((rows, 1), F32)
    for i in range(n_tp):
        wide = tok[i].astype(F32).reshape(rows, -1)
        square = square + jnp.sum(wide * wide, -1, keepdims=True)
    feats = tok.shape[3]
    scale = lax.rsqrt(square / (n_tp * feats) + EPS)
    for i in range(n_tp):
        cols = slice(i * feats, (i + 1) * feats)
        normed[:, cols] = (tok[i].astype(F32).reshape(rows, -1) * scale * gain_ref[:, cols]).astype(BF16)
    all_heads = wb_ref.shape[0]
    pick = (
        lax.broadcasted_iota(jnp.int32, (all_heads, width), 0)
        == t_me * heads + lax.broadcasted_iota(jnp.int32, (all_heads, width), 1) // hd
    ).astype(F32)

    def per_head(ref):
        raw = lax.dot_general(
            normed[...], ref[...], (((1,), (1,)), ((), ())), preferred_element_type=F32)
        return jnp.dot(raw, pick, precision=lax.Precision.HIGHEST, preferred_element_type=F32)

    wr(rows_a, every, jax.nn.sigmoid(per_head(wb_ref)))
    weights = split(rows_a)
    base = jnp.zeros((1, width), F32)
    for h in range(heads):
        base = jnp.where(lane_head == h, base_ref[:, h : h + 1], base)
    wr(rows_b, every, -base * jax.nn.softplus(per_head(wd_ref)))
    logs = split(rows_b)

    def project(m):
        return jnp.dot(normed[...], wp[m], preferred_element_type=F32)

    def finish(m):
        wait_y(m)
        if m < len(sources):
            value = project(m)
            if m == 0:
                value = value * lax.rsqrt(head_sum(value * value) + EPS)
            elif m == 1:
                value = value * lax.rsqrt(head_sum(value * value) + EPS) * hd ** (-0.5)
            wr(proj, every, value, m)

    outs = None
    def r_copy(dest):
        return pltpu.make_async_remote_copy(
            send_buf.at[dest], recv_buf.at[t_me], r_send.at[dest], r_recv.at[t_me],
            device_id={"tp": dest}, device_id_type=MESH)

    def r_wait(origin):
        pltpu.make_async_remote_copy(
            send_buf.at[origin], recv_buf.at[origin], r_send.at[origin], r_recv.at[origin],
            device_id={"tp": origin}, device_id_type=MESH).wait_recv()

    def send_share(dest):
        share = jnp.dot(gate_buf[...], wo[dest], preferred_element_type=F32)

        @pl.when(dest == t_me)
        def _():
            own_share[...] = share

        @pl.when(dest != t_me)
        def _():
            send_buf[dest] = share.astype(BF16)
            r_copy(dest).start()

    for m in range(len(sources)):
        if m >= 2:
            forward(m)
        if m >= 1:
            finish(m - 1)
        if m == 3:
            keys = [rd(proj, pl.ds(t, seqs, stride=props), 0) for t in range(props)]
            queries = [rd(proj, pl.ds(t, seqs, stride=props), 1) for t in range(props)]
            values = [rd(proj, pl.ds(t, seqs, stride=props), 2) for t in range(props)]
            for t in range(props):
                wr(kq, pl.ds(t, seqs, stride=pad), keys[t])
                wr(kq, pl.ds(props + t, seqs, stride=pad), queries[t])
            lax.fori_loop(0, seqs, by_state, 0, unroll=4)
            outs = solve(keys, values, weights, logs, queries)[3]
            for t in range(props):
                wr(rows_a, pl.ds(t, seqs, stride=props), outs[t])
            out = rd(rows_a, every)
            out = out * lax.rsqrt(head_sum(out * out) / hd + EPS)
            tile_gain = (
                lax.broadcasted_iota(jnp.int32, (hd, width), 0)
                == lax.broadcasted_iota(jnp.int32, (hd, width), 1) % hd
            ).astype(F32)
            gain = jnp.dot(
                jnp.broadcast_to(og_ref[...], (8, hd)), tile_gain,
                precision=lax.Precision.HIGHEST, preferred_element_type=F32)[:1]
            wr(rows_a, every, out * gain)
    finish(len(sources) - 1)
    gate = rd(proj, every, 3)
    gate_buf[...] = (rd(rows_a, every) * (gate / (1.0 + jnp.exp(-gate)))).astype(BF16)
    if gather_out:
        m = n_mat - 1

        def take(s, carry):
            @pl.when(s < n_kv - 1)
            def _():
                forward_step(m, s)

            @pl.when(k - s >= 0)
            def _():
                @pl.when(s > 0)
                def _():
                    for d in range(1, n_grp):
                        y_wait(m, k - s, d)

                send_share(k - s)

            @pl.when(jnp.logical_and(s > 0, k + s < n_kv))
            def _():
                for d in range(1, n_grp):
                    y_wait(m, k + s, d)
                send_share(k + s)

            return carry

        lax.fori_loop(0, n_kv, take, 0)
    else:
        out_in.wait()
        for d in range(n_tp):
            send_share(lax.rem(t_me + d, n_tp))
    total = own_share[...]
    for d in range(1, n_tp):
        origin = lax.rem(t_me + d, n_tp)
        r_wait(origin)
        total = total + recv_buf[origin].astype(F32)
    mixed_ref[...] = total.reshape(seqs, props, feats).astype(BF16)

    for d in range(1, n_tp):
        t_copy(d).wait_send()
        r_copy(lax.rem(t_me + d, n_tp)).wait_send()

    def drain(m):
        def step(o, carry):
            @pl.when(jnp.logical_and(o <= k, k < n_kv - 1))
            def _():
                z_right(m, o).wait_send()

            @pl.when(jnp.logical_and(o >= k, k > 0))
            def _():
                z_left(m, o).wait_send()

            @pl.when(o != k)
            def _():
                for d in range(1, n_grp):
                    y_copy(m, o, d).wait_send()

            return carry

        lax.fori_loop(0, n_kv, step, 0)

    for m in range(n_mat):
        drain(m)
    state_out.wait()


def pair_kernel(
    cfg,
    tok_hbm, gain_hbm, wq_hbm, wk_hbm, wv_hbm, wg_hbm, wb_hbm, wd_hbm, base_hbm, og_hbm, wo_hbm,
    state_hbm, pk_hbm, pv_hbm, pb_hbm, pd_hbm, acc_hbm,
    mixed_ref, st,
    gain_ref, wbd_ref, base_ref, og_ref, pkv_ref, pbd_ref, acc_ref, tok, wp, wo, normed, kq, res, tk, up, al, rows_a, rows_b, proj, own_part, part_send, part_recv, small_own, small_send, small_recv, send_buf, recv_buf, gate_buf, own_share,
    in_sem, own_sem, wz_send, wz_recv, wy_send, wy_recv, t_send, f_send, d_send, t_recv, zs_send, z_recv, y_send, y_recv, p_send, p_recv, s_recv, r_send, r_recv,
    small_sem,
):
    n_grp, n_kv, n_tp, seqs, props, heads, hd = cfg
    width = heads * hd
    g = lax.axis_index("grp")
    k = lax.axis_index("kv")
    t_me = lax.axis_index("tp")
    rows = seqs * props
    own_rows = wk_hbm.shape[0]
    piece = own_rows // n_grp
    out_piece = wo.shape[1] // n_grp
    out_bits = 2
    w_bits = 2
    out_bit = out_piece // out_bits
    feats = tok_hbm.shape[2]
    sources = [wk_hbm, wq_hbm, wv_hbm, wg_hbm]
    n_src = len(sources)
    all_heads = wb_hbm.shape[0]
    pair = k // 2
    side = lax.rem(k, 2)
    mate = k + 1 - 2 * side
    partner = lax.rem(k + n_kv // 2, n_kv)
    chip = t_me // 2
    core = lax.rem(t_me, 2)
    beside_core = 2 * chip + 1 - core
    home = lax.rem(pair + chip + 1, 2)
    g_other = lax.rem(g + 1, n_grp)
    half_feats = 2 * feats

    own_slot = home * (2 + core) + (1 - home) * 4
    tok_in = pltpu.make_async_copy(tok_hbm, tok.at[own_slot], in_sem.at[0])
    tok_in.start()
    own_copies = []
    for m in range(n_src + 1):
        if m < n_src:
            dst = wp.at[m, pl.ds(side * own_rows, own_rows), :]
            copy = pltpu.make_async_copy(sources[m], dst, own_sem.at[min(m, 1)])
        else:
            copy = pltpu.make_async_copy(wo_hbm, wo.at[k], own_sem.at[2])
        copy.start()
        own_copies.append(copy)
    ours = pl.ds(pl.multiple_of(pair * half_feats, half_feats), half_feats)
    loads = [
        (pk_hbm, pkv_ref.at[0], 0), (pv_hbm, pkv_ref.at[1], 0),
        (pb_hbm, pbd_ref.at[0], 1), (pd_hbm, pbd_ref.at[1], 1), (acc_hbm, acc_ref, 2),
        (wb_hbm.at[:, ours], wbd_ref.at[pl.ds(0, all_heads), :], 3),
        (wd_hbm.at[:, ours], wbd_ref.at[pl.ds(all_heads, all_heads), :], 3),
        (gain_hbm.at[:, ours], gain_ref, 4), (base_hbm, base_ref, 5), (og_hbm, og_ref, 6),
    ]
    for src, dst, i in loads:
        pltpu.make_async_copy(src, dst, small_sem.at[i]).start()
    early = [(pkv_ref, 0), (pbd_ref, 1), (acc_ref, 2)]
    late = [(wbd_ref, 3), (gain_ref, 4), (base_ref, 5), (og_ref, 6)]

    def loaded(group):
        for ref, i in group:
            pltpu.make_async_copy(ref, ref, small_sem.at[i]).wait()

    state_in = pltpu.make_async_copy(state_hbm, st, in_sem.at[1])
    state_in.start()

    barrier = pltpu.get_barrier_semaphore()

    def greet(dev):
        pl.semaphore_signal(barrier, inc=1, device_id=dev, device_id_type=MESH)

    for d in range(1, n_kv):
        greet({"kv": lax.rem(k + d, n_kv)})
    for d in range(1, n_tp):
        greet({"tp": lax.rem(t_me + d, n_tp)})
    greet({"grp": g_other})
    far_tp = 2 * (1 - chip) + core
    pl.semaphore_wait(barrier, n_kv + n_tp - 1)

    def remote(src, dst, send, recv, dev):
        return pltpu.make_async_remote_copy(
            src, dst, send, recv, device_id=dev, device_id_type=MESH)

    part = seqs // 2

    def tok_piece(slot, half):
        return tok.at[slot, pl.ds(half * part, part)]

    def tok_partner():
        return remote(tok_piece(4, 0), tok_piece(core, 0), t_send.at[0],
                      t_recv.at[2 * core], {"kv": partner})

    def tok_shift():
        return remote(tok_piece(4, 1), tok_piece(5, 1), t_send.at[1], t_recv.at[6],
                      {"tp": far_tp})

    def tok_relay():
        return remote(tok_piece(5, 1), tok_piece(core, 1), t_send.at[0],
                      t_recv.at[2 * core + 1], {"kv": partner})

    def tok_far(half):
        ref = tok_piece(core, half)
        return remote(ref, ref, f_send.at[0], t_recv.at[2 * core + half], {"tp": far_tp})

    def tok_beside(half):
        ref = tok_piece(core, half)
        return remote(ref, ref, d_send.at[0], t_recv.at[2 * core + half], {"tp": beside_core})

    def own_far():
        ref = tok.at[2 + core]
        return remote(ref, ref, f_send.at[1], t_recv.at[4 + core], {"tp": far_tp})

    def own_beside():
        ref = tok.at[2 + core]
        return remote(ref, ref, d_send.at[0], t_recv.at[4 + core], {"tp": beside_core})

    def tok_wait(ref, index):
        remote(ref, ref, d_send.at[0], t_recv.at[index], {"tp": beside_core}).wait_recv()

    def tok_land_z():
        tok_wait(tok_piece(core, 1 - home), 2 * core + 1 - home)
        tok_far(1 - home).start()
        tok_beside(1 - home).start()

    def tok_land_x():
        tok_wait(tok_piece(core, home), 2 * core + home)
        tok_beside(home).start()

    def w_slot(m, block, half, bit):
        at = pl.ds(block * own_rows + half * piece + bit * (piece // w_bits), piece // w_bits)
        return wp.at[m, at, :]

    def w_mate(m, bit):
        ref = w_slot(m, side, g, bit)
        return remote(ref, ref, wz_send.at[0], wz_recv.at[m, bit], {"kv": mate})

    def w_share(m, bit):
        ref = w_slot(m, 1 - side, g, bit)
        return remote(ref, ref, wy_send.at[0], wy_recv.at[m], {"grp": g_other})

    def w_pass(m):
        for bit in range(w_bits):
            ref = w_slot(m, 1 - side, g, bit)
            remote(ref, ref, wz_send.at[0], wz_recv.at[m, bit], {"kv": mate}).wait_recv()
            w_share(m, bit).start()

    def w_ready(m):
        at = pl.ds((1 - side) * own_rows + g_other * piece, piece)
        ref = wp.at[m, at, :]
        remote(ref, ref, wy_send.at[0], wy_recv.at[m], {"grp": g_other}).wait_recv()

    def o_slot(origin, part, bit):
        return wo.at[origin, pl.ds(part * out_piece + bit * out_bit, out_bit), :]

    def z_right(origin, bit):
        ref = o_slot(origin, g, bit)
        return remote(ref, ref, zs_send.at[1 - pair], z_recv.at[origin, bit], {"kv": k + 1})

    def z_left(origin, bit):
        ref = o_slot(origin, g, bit)
        return remote(ref, ref, zs_send.at[pair], z_recv.at[origin, bit], {"kv": k - 1})

    def y_copy(origin, bit):
        ref = o_slot(origin, g, bit)
        return remote(ref, ref, y_send.at[0], y_recv.at[origin], {"grp": g_other})

    def y_wait(origin):
        ref = wo.at[origin, pl.ds(g_other * out_piece, out_piece), :]
        remote(ref, ref, y_send.at[0], y_recv.at[origin], {"grp": g_other}).wait_recv()

    def right_start(origin):
        for bit in range(out_bits):
            z_right(origin, bit).start()

    def left_start(origin):
        for bit in range(out_bits):
            z_left(origin, bit).start()

    def from_left(origin):
        for bit in range(out_bits):
            z_right(origin, bit).wait_recv()

            @pl.when(k < n_kv - 1)
            def _():
                z_right(origin, bit).start()

    def from_right(origin):
        for bit in range(out_bits):
            z_left(origin, bit).wait_recv()

            @pl.when(k > 0)
            def _():
                z_left(origin, bit).start()

    def share_out(origin):
        for bit in range(out_bits):
            y_copy(origin, bit).start()

    def middle_pass(s):
        @pl.when(jnp.logical_and(side == 1, pair == 0))
        def _():
            if s == 0:
                from_left(k - 1)
            else:
                from_right(k + s)

        @pl.when(jnp.logical_and(side == 0, pair == 1))
        def _():
            if s == 0:
                from_right(k + 1)
            else:
                from_left(k - s)

    def middle_share(s):
        @pl.when(jnp.logical_and(side == 1, pair == 0))
        def _():
            share_out(k - 1 if s == 0 else k + s)

        @pl.when(jnp.logical_and(side == 0, pair == 1))
        def _():
            share_out(k + 1 if s == 0 else k - s)

    def end_pass(s, bits=(0, 1)):
        for bit in bits:
            @pl.when(k == 0)
            def _():
                z_left(k + s, bit).wait_recv()
                y_copy(k + s, bit).start()

            @pl.when(k == n_kv - 1)
            def _():
                z_right(k - s, bit).wait_recv()
                y_copy(k - s, bit).start()

    def p_copy(m, b):
        at = pl.ds(b * half_rows, half_rows)
        return remote(part_send.at[m, at], part_recv.at[m, at], p_send.at[0],
                      p_recv.at[m, b], {"kv": partner})

    def small_copy():
        return remote(small_send, small_recv, p_send.at[1], s_recv.at[0],
                      {"kv": partner})

    at_end = jnp.logical_or(k == 0, k == n_kv - 1)
    tok_in.wait()

    @pl.when(home == 0)
    def _():
        tok_shift().start()
        tok_partner().start()

    @pl.when(home == 1)
    def _():
        own_far().start()
        own_beside().start()

    def w_first(m):
        for bit in range(w_bits):
            w_mate(m, bit).start()

    own_copies[0].wait()
    w_first(0)
    own_copies[n_src].wait()

    def w_rest():
        @pl.when(k == 0)
        def _():
            right_start(k)

        @pl.when(k == n_kv - 1)
        def _():
            left_start(k)

        rest = wp.at[pl.ds(1, n_src - 1), pl.ds(side * own_rows, own_rows), :]
        pltpu.make_async_copy(rest, rest, own_sem.at[1]).wait()
        for m in range(1, n_src):
            w_first(m)

    relays_first = jnp.logical_and(at_end, home == 1)

    @pl.when(jnp.logical_not(relays_first))
    def _():
        w_rest()

    blk = (
        lax.broadcasted_iota(jnp.int32, (width, width), 0) // hd
        == lax.broadcasted_iota(jnp.int32, (width, width), 1) // hd
    ).astype(F32).astype(BF16)
    lane_head = lax.broadcasted_iota(jnp.int32, (1, width), 1) // hd
    masks = [(lane_head == h).astype(F32) for h in range(heads)]

    def head_sum(x):
        hi = x.astype(BF16)
        lo = (x - hi.astype(F32)).astype(BF16)
        return jnp.dot(hi, blk, preferred_element_type=F32) + jnp.dot(
            lo, blk, preferred_element_type=F32)

    lanes = 128
    blocks = width // lanes

    def rd(ref, at, *lead):
        return jnp.concatenate([ref[(*lead, c, at)] for c in range(blocks)], axis=-1)

    def wr(ref, at, x, *lead):
        for c in range(blocks):
            ref[(*lead, c, at)] = x[:, c * lanes : (c + 1) * lanes]

    every = pl.ds(0, rows)
    count = seqs // 2
    half_rows = count * props

    pad = 2 * props

    def head_first(x, head):
        block, at = divmod(head * hd, lanes)
        x = x[:, block * lanes : (block + 1) * lanes]
        return jnp.concatenate([x[:, at:], x[:, :at]], axis=-1) if at else x

    def put_heads(ref, x, first, each, low=0):
        step = heads * each
        for head in range(heads):
            at = pl.ds(low * step + head * each + first, x.shape[0], stride=step)
            ref[at] = head_first(x, head)

    def by_state(s, carry):
        at = pl.ds(pl.multiple_of(s * heads * pad, heads * pad), heads * pad)
        tile = st[pl.ds(pl.multiple_of(s * hd, hd), hd), :].astype(BF16)
        found = jnp.dot(kq[at, :hd].astype(BF16), tile, preferred_element_type=F32)
        own = masks[0] * found[:pad]
        for head in range(1, heads):
            own = own + masks[head] * found[head * pad : (head + 1) * pad]
        wr(res, pl.ds(pl.multiple_of(s * pad, pad), pad), own)
        return carry

    def solve(keys, values, weights, logs, queries, start=0):
        count = keys[0].shape[0]
        cumul = []
        run = None
        for t in range(props):
            run = logs[t] if run is None else run + logs[t]
            cumul.append(run)
        low = [(i, j) for i in range(props) for j in range(i)]
        products = [keys[i] * keys[j] for i, j in low]
        full = []
        if queries is not None:
            full = [(i, j) for i in range(props) for j in range(i + 1)]
            products += [queries[i] * keys[j] for i, j in full]
        sums = head_sum(jnp.concatenate(products, axis=0))
        sums = [sums[i * count : (i + 1) * count] for i in range(len(products))]
        kk = dict(zip(low, sums))
        qk = dict(zip(full, sums[len(low):]))
        dec = {pair: jnp.exp(cumul[pair[0]] - cumul[pair[1]]) for pair in low}
        growth = [jnp.exp(c) for c in cumul]
        update = []
        for t in range(props):
            seen = rd(res, pl.ds(start * pad + t, count, stride=pad))
            term = values[t] - growth[t] * seen
            for j in range(t):
                term = term - kk[t, j] * dec[t, j] * update[j]
            update.append(weights[t] * term)
        outs = []
        if queries is not None:
            for t in range(props):
                out = growth[t] * rd(
                    res, pl.ds(start * pad + props + t, count, stride=pad))
                for j in range(t + 1):
                    score = qk[t, j] if j == t else qk[t, j] * dec[t, j]
                    out = out + score * update[j]
                outs.append(out)
        return cumul, growth, update, outs

    def split(ref):
        return [rd(ref, pl.ds(t, seqs, stride=props)) for t in range(props)]

    loaded(early)
    pk = pkv_ref[0].astype(F32).reshape(rows, width)
    wr(rows_a, every, pk * lax.rsqrt(head_sum(pk * pk) + EPS))
    wr(rows_b, every, pkv_ref[1].astype(F32).reshape(rows, width))
    keys = split(rows_a)
    values = split(rows_b)
    own_head = (
        lax.broadcasted_iota(jnp.int32, (heads, width), 0)
        == lax.broadcasted_iota(jnp.int32, (heads, width), 1) // hd
    ).astype(F32)

    def over_lanes(x):
        return lax.dot_general(
            x, own_head, (((0,), (0,)), ((), ())),
            precision=lax.Precision.HIGHEST, preferred_element_type=F32)

    weights, logs = [], []
    for t in range(props):
        live = (acc_ref[...] > t).astype(F32)
        weights.append(over_lanes(jax.nn.sigmoid(pbd_ref[0, t]) * live))
        logs.append(over_lanes(pbd_ref[1, t] * live))
        put_heads(kq, keys[t], t, pad)
        put_heads(kq, keys[t], props + t, pad)
    state_in.wait()
    lax.fori_loop(0, seqs, by_state, 0, unroll=4)
    cumul, growth, update, _ = solve(keys, values, weights, logs, None)
    al[...] = growth[-1]
    for t in range(props):
        put_heads(tk, jnp.exp(cumul[-1] - cumul[t]) * keys[t], t, props)
        for head in range(heads):
            wr(up, pl.ds(head * props + t, seqs, stride=heads * props), masks[head] * update[t])

    def renew(s, carry):
        each = heads * props
        at = pl.ds(pl.multiple_of(s * each, each), each)
        outer = lax.dot_general(
            tk[at, :hd], rd(up, at), (((0,), (0,)), ((), ())), preferred_element_type=F32)
        where = pl.ds(pl.multiple_of(s * hd, hd), hd)
        st[where, :] = al[pl.ds(s, 1), :] * st[where, :] + outer
        return carry


    @pl.when(home == 1)
    def _():
        tok_wait(tok_piece(5, 1), 6)
        tok_relay().start()

    @pl.when(relays_first)
    def _():
        w_rest()

    @pl.when(home == 0)
    def _():
        tok_wait(tok.at[2 + core], 4 + core)
        own_beside().start()

    @pl.when(home == 1)
    def _():
        tok_land_z()

    w_pass(0)

    @pl.when(jnp.logical_not(at_end))
    def _():
        right_start(k)
        left_start(k)

    @pl.when(home == 0)
    def _():
        tok_land_z()
        tok_land_x()

    middle_pass(0)
    middle_share(0)

    @pl.when(home == 1)
    def _():
        tok_land_x()

    w_pass(1)
    middle_pass(1)

    loaded(late)
    tok_wait(tok.at[3 - core], 5 - core)
    for half in range(2):
        tok_wait(tok_piece(1 - core, half), 2 * (1 - core) + half)
    ones = jnp.ones((8, feats), BF16)
    squares = jnp.zeros((8, 2 * rows), F32)
    last = (((1,), (1,)), ((), ()))
    for c in range(2):
        cols = slice(c * feats, (c + 1) * feats)
        wide = jnp.concatenate(
            [tok[c].astype(F32).reshape(rows, feats), tok[2 + c].astype(F32).reshape(rows, feats)],
            axis=0)
        normed[:, cols] = (wide * gain_ref[:, cols]).astype(BF16)
        sq = wide * wide
        hi = sq.astype(BF16)
        lo = (sq - hi.astype(F32)).astype(BF16)
        squares = squares + lax.dot_general(ones, hi, last, preferred_element_type=F32)
        squares = squares + lax.dot_general(ones, lo, last, preferred_element_type=F32)
    raw = lax.dot_general(wbd_ref[...], normed[...], last, preferred_element_type=F32)
    small = jnp.concatenate([raw, squares], axis=0)
    kind = lax.broadcasted_iota(jnp.int32, (small_own.shape[0], small.shape[0]), 0)
    taken = lax.broadcasted_iota(jnp.int32, (small_own.shape[0], small.shape[0]), 1)
    first_head = t_me * heads
    wanted = jnp.where(
        kind < heads, first_head + kind,
        jnp.where(kind < 2 * heads, all_heads + first_head + kind - heads, 2 * all_heads))
    small = jnp.dot(
        (taken == wanted).astype(F32), small,
        precision=lax.Precision.HIGHEST, preferred_element_type=F32)
    small_send[...] = small[:, :rows]
    small_copy().start()
    small_own[...] = small[:, rows:]

    def project(m):
        both = jnp.dot(normed[...], wp[m], preferred_element_type=F32)
        part_send[m] = both[:rows].astype(BF16)
        own_part[m] = both[rows:]

    def give(*pieces):
        for m, b in pieces:
            p_copy(m, b).start()

    w_ready(0)
    project(0)
    give((0, 0), (0, 1))
    w_pass(2)
    w_ready(1)
    project(1)
    give((1, 0))
    middle_pass(2)
    w_pass(3)
    end_pass(1)
    middle_share(1)
    middle_share(2)
    lax.fori_loop(0, seqs // 2, renew, 0, unroll=4)
    w_ready(2)
    project(2)
    give((2, 0), (1, 1))
    lax.fori_loop(seqs // 2, seqs, renew, 0, unroll=4)
    w_ready(3)
    project(3)
    give((3, 0), (2, 1), (3, 1))
    end_pass(2)

    small_copy().wait_recv()
    small = small_own[...] + small_recv[...]
    scale = lax.rsqrt(small[2 * heads :] / (n_tp * feats) + EPS)
    beta = small[:heads] * scale[:1]
    decay = small[heads : 2 * heads] * scale[:1]

    def spread(x, over):
        return lax.dot_general(
            x, over, (((0,), (0,)), ((), ())),
            precision=lax.Precision.HIGHEST, preferred_element_type=F32)

    wr(rows_a, every, spread(jax.nn.sigmoid(beta), own_head))
    base = jnp.zeros((1, width), F32)
    for h in range(heads):
        base = jnp.where(lane_head == h, base_ref[:, h : h + 1], base)
    wr(rows_b, every, -base * spread(jax.nn.softplus(decay), own_head))
    row_scale = spread(
        scale, (lax.broadcasted_iota(jnp.int32, (scale.shape[0], width), 0) == 0).astype(F32))

    def finish(m, b):
        p_copy(m, b).wait_recv()
        at = slice(b * half_rows, (b + 1) * half_rows)
        value = (own_part[m, at] + part_recv[m, at].astype(F32)) * row_scale[at]
        if m == 0:
            value = value * lax.rsqrt(head_sum(value * value) + EPS)
        elif m == 1:
            value = value * lax.rsqrt(head_sum(value * value) + EPS) * hd ** (-0.5)
        wr(proj, pl.ds(b * half_rows, half_rows), value, m)

    def r_copy(dest, b):
        at = pl.ds(b * half_rows, half_rows)
        far = lax.rem(dest - t_me + n_tp, n_tp)
        return remote(send_buf.at[dest, at], recv_buf.at[t_me, at], r_send.at[0],
                      r_recv.at[far - 1, b], {"tp": dest})

    def r_wait(d, b):
        origin = lax.rem(t_me + n_tp - d, n_tp)
        ref = recv_buf.at[origin, pl.ds(b * half_rows, half_rows)]
        remote(ref, ref, r_send.at[0], r_recv.at[d - 1, b], {"tp": origin}).wait_recv()

    def send_share(dest, b):
        at = slice(b * half_rows, (b + 1) * half_rows)
        share = jnp.dot(gate_buf[at], wo[dest], preferred_element_type=F32)

        @pl.when(dest == t_me)
        def _():
            own_share[at] = share

        @pl.when(dest != t_me)
        def _():
            send_buf[dest, at] = share.astype(BF16)
            r_copy(dest, b).start()

    tile_gain = (
        lax.broadcasted_iota(jnp.int32, (hd, width), 0)
        == lax.broadcasted_iota(jnp.int32, (hd, width), 1) % hd
    ).astype(F32)
    gain = jnp.dot(
        jnp.broadcast_to(og_ref[...], (8, hd)), tile_gain,
        precision=lax.Precision.HIGHEST, preferred_element_type=F32)[:1]

    def delta(b):
        low, first = b * count, b * half_rows
        steps = [pl.ds(first + t, count, stride=props) for t in range(props)]
        for m in range(3):
            finish(m, b)
            if b == 0 and m == 1:
                end_pass(3, (0,))
        keys, queries, values = [[rd(proj, at, m) for at in steps] for m in range(3)]
        weights = [rd(rows_a, at) for at in steps]
        logs = [rd(rows_b, at) for at in steps]
        for t in range(props):
            put_heads(kq, keys[t], t, pad, low)
            put_heads(kq, queries[t], props + t, pad, low)
        lax.fori_loop(low, low + count, by_state, 0, unroll=4)
        if b == 0:
            end_pass(3, (1,))
        outs = solve(keys, values, weights, logs, queries, low)[3]
        for t in range(props):
            wr(rows_a, steps[t], outs[t])
        half = pl.ds(first, half_rows)
        out = rd(rows_a, half)
        out = out * lax.rsqrt(head_sum(out * out) / hd + EPS) * gain
        finish(n_src - 1, b)
        gate = rd(proj, half, 3)
        gate_buf[first : first + half_rows] = (
            out * (gate / (1.0 + jnp.exp(-gate)))).astype(BF16)

    def take(b):
        def step(s, carry):
            @pl.when(k - s >= 0)
            def _():
                if b == 0:
                    @pl.when(s > 0)
                    def _():
                        y_wait(k - s)

                send_share(k - s, b)

            @pl.when(jnp.logical_and(s > 0, k + s < n_kv))
            def _():
                if b == 0:
                    y_wait(k + s)
                send_share(k + s, b)

            return carry

        return step

    def settle(b):
        at = slice(b * half_rows, (b + 1) * half_rows)
        total = own_share[at]
        for d in range(1, n_tp):
            r_wait(d, b)
            total = total + recv_buf[lax.rem(t_me + n_tp - d, n_tp), at].astype(F32)
        mixed_ref[b * count : (b + 1) * count] = total.reshape(count, props, feats).astype(BF16)

    delta(0)
    lax.fori_loop(0, n_kv - 1, take(0), 0)
    delta(1)
    lax.fori_loop(0, n_kv - 1, take(1), 0)
    lax.fori_loop(n_kv - 1, n_kv, take(0), 0)
    lax.fori_loop(n_kv - 1, n_kv, take(1), 0)
    def sent(ref, sem):
        remote(ref, ref, sem, s_recv.at[0], {"kv": mate}).wait_send()

    sent(tok.at[pl.ds(0, 2)], d_send.at[0])
    tok_far(1 - home).wait_send()

    @pl.when(home == 1)
    def _():
        own_far().wait_send()
        tok_relay().wait_send()

    @pl.when(home == 0)
    def _():
        tok_partner().wait_send()
        tok_shift().wait_send()

    sent(wp.at[0], wz_send.at[0])
    sent(wp.at[0], wy_send.at[0])
    sent(part_send, p_send.at[0])
    sent(small_send, p_send.at[1])
    some = pl.ds(0, out_piece)
    sent(wo.at[pl.ds(0, n_kv - 1), some], y_send.at[0])

    @pl.when(at_end)
    def _():
        sent(wo.at[0, some], zs_send.at[1])

    @pl.when(jnp.logical_not(at_end))
    def _():
        sent(wo.at[pl.ds(0, 3), some], zs_send.at[0])
        sent(wo.at[pl.ds(0, 2), some], zs_send.at[1])

    settle(0)
    settle(1)
    sent(send_buf.at[pl.ds(0, n_tp - 1)], r_send.at[0])

def pair_call(sizes, args, seqs, props, feats, heads, hd, width, rows, pad):
    n_grp, n_kv, n_tp = sizes
    cfg = (n_grp, n_kv, n_tp, seqs, props, heads, hd)
    vmem = pl.BlockSpec(memory_space=pltpu.VMEM)
    hbm = pl.BlockSpec(memory_space=pltpu.HBM)
    dma = pltpu.SemaphoreType.DMA
    own_rows = args[2].shape[0]
    all_heads = args[6].shape[0]
    n_src = 4
    small = (2 * heads + 8, rows)
    return pl.pallas_call(
        functools.partial(pair_kernel, cfg),
        out_shape=(
            pltpu.VMEM((seqs, props, feats), BF16),
            pltpu.VMEM((seqs * hd, width), F32),
        ),
        in_specs=[hbm] * len(args),
        out_specs=(vmem, vmem),
        scratch_shapes=[
            pltpu.VMEM((1, 2 * feats), F32),
            pltpu.VMEM((2 * all_heads, 2 * feats), BF16),
            *[pltpu.VMEM(args[i].shape, args[i].dtype) for i in (8, 9)],
            *[pltpu.VMEM((2, *args[i].shape), args[i].dtype) for i in (12, 14)],
            pltpu.VMEM(args[16].shape, args[16].dtype),
            pltpu.VMEM((6, seqs, props, feats), BF16),
            pltpu.VMEM((n_src, 2 * own_rows, width), BF16),
            pltpu.VMEM((n_tp, width, feats), BF16),
            pltpu.VMEM((2 * rows, 2 * feats), BF16),
            pltpu.VMEM((seqs * heads * pad, 128), F32),
            pltpu.VMEM((width // 128, seqs * pad, 128), F32),
            pltpu.VMEM((seqs * heads * props, 128), F32),
            pltpu.VMEM((width // 128, seqs * heads * props, 128), F32),
            pltpu.VMEM((seqs, width), F32),
            pltpu.VMEM((width // 128, rows, 128), F32),
            pltpu.VMEM((width // 128, rows, 128), F32),
            pltpu.VMEM((n_src, width // 128, rows, 128), F32),
            pltpu.VMEM((n_src, rows, width), F32),
            pltpu.VMEM((n_src, rows, width), BF16),
            pltpu.VMEM((n_src, rows, width), BF16),
            pltpu.VMEM(small, F32),
            pltpu.VMEM(small, F32),
            pltpu.VMEM(small, F32),
            pltpu.VMEM((n_tp, rows, feats), BF16),
            pltpu.VMEM((n_tp, rows, feats), BF16),
            pltpu.VMEM((rows, width), BF16),
            pltpu.VMEM((rows, feats), F32),
            dma((2,)),
            dma((3,)),
            dma((1,)),
            dma((n_src, 2)),
            dma((1,)),
            dma((n_src,)),
            dma((2,)),
            dma((2,)),
            dma((1,)),
            dma((7,)),
            dma((2,)),
            dma((n_kv, 2)),
            dma((1,)),
            dma((n_kv,)),
            dma((2,)),
            dma((n_src, 2)),
            dma((1,)),
            dma((1,)),
            dma((n_tp - 1, 2)),
            dma((7,)),
        ],
        compiler_params=pltpu.CompilerParams(
            collective_id=1, has_side_effects=True, vmem_limit_bytes=67043328 - rows * feats * 2 - seqs * hd * width * 4),
    )(*args)


def body(
    sizes,
    tokens, in_gain, w_query, w_key, w_value, w_gate, w_beta, w_decay, decay_base, out_gain, w_out,
    state, prev_keys, prev_values, prev_beta, prev_decay, accepted,
):
    n_grp, n_kv, n_tp = sizes
    seqs, props, feats = tokens.shape
    heads = decay_base.shape[0]
    hd = out_gain.shape[0]
    width = heads * hd
    rows = seqs * props
    pad = 2 * props
    paired = (
        n_grp == 2 and n_kv == n_tp and n_kv // 2 == 2
        and w_query.shape[0] == feats and w_query.shape[0] * n_kv == in_gain.shape[0])
    gather_out = n_kv == n_tp
    if not gather_out:
        w_out = lax.all_gather(w_out, "kv", axis=1, tiled=True)
        w_out = jnp.transpose(w_out.reshape(width, n_tp, feats), (1, 0, 2))
    n_mat = 5 if gather_out else 4
    cfg = (n_grp, n_kv, n_tp, seqs, props, heads, hd, gather_out)
    vmem = pl.BlockSpec(memory_space=pltpu.VMEM)
    hbm = pl.BlockSpec(memory_space=pltpu.HBM)
    args = (
        tokens, in_gain.reshape(1, -1), w_query, w_key, w_value, w_gate,
        w_beta.T, w_decay.T, decay_base.reshape(1, -1), out_gain.reshape(1, -1), w_out,
        state.reshape(seqs * hd, width), prev_keys, prev_values,
        jnp.transpose(prev_beta, (1, 2, 0)), jnp.transpose(prev_decay, (1, 2, 0)),
        accepted.reshape(1, seqs),
    )
    if paired:
        mixed, new_state = pair_call(
            sizes, args, seqs, props, feats, heads, hd, width, rows, pad)
        return mixed, new_state.reshape(seqs, hd, width)
    dma = pltpu.SemaphoreType.DMA
    mixed, new_state = pl.pallas_call(
        functools.partial(kernel, cfg),
        out_shape=(
            jax.ShapeDtypeStruct((seqs, props, feats), BF16),
            jax.ShapeDtypeStruct((seqs * hd, width), F32),
        ),
        in_specs=[hbm] * len(args),
        out_specs=(vmem, pl.BlockSpec(memory_space=pl.ANY)),
        scratch_shapes=[
            *[pltpu.VMEM(args[i].shape, args[i].dtype) for i in (1, 6, 7, 8, 9, 12, 13, 14, 15, 16)],
            pltpu.VMEM((n_tp, seqs, props, feats), BF16),
            pltpu.VMEM((4, n_kv * w_key.shape[0], width), BF16),
            pltpu.VMEM((n_tp, width, feats), BF16),
            pltpu.VMEM((seqs * hd, width), F32),
            pltpu.VMEM((rows, n_tp * feats), BF16),
            pltpu.VMEM((width // 128, seqs * pad, 128), F32),
            pltpu.VMEM((width // 128, seqs * pad, 128), F32),
            pltpu.VMEM((width // 128, seqs * pad, 128), F32),
            pltpu.VMEM((width // 128, seqs * pad, 128), F32),
            pltpu.VMEM((seqs, width), F32),
            pltpu.VMEM((width // 128, rows, 128), F32),
            pltpu.VMEM((width // 128, rows, 128), F32),
            pltpu.VMEM((4, width // 128, rows, 128), F32),
            pltpu.VMEM((n_tp, rows, feats), BF16),
            pltpu.VMEM((n_tp, rows, feats), BF16),
            pltpu.VMEM((rows, width), BF16),
            pltpu.VMEM((rows, feats), F32),
            dma((2,)),
            dma((6,)),
            dma((n_mat, n_kv)),
            dma((n_mat, n_kv)),
            dma((n_mat, n_kv)),
            dma((max(n_grp - 1, 1), n_mat, n_kv)),
            dma((max(n_grp - 1, 1), n_mat, n_kv)),
            dma((n_tp - 1,)),
            dma((n_tp - 1,)),
            dma((n_tp,)),
            dma((n_tp,)),
            dma(()),
            dma((10,)),
        ],
        compiler_params=pltpu.CompilerParams(
            collective_id=0, has_side_effects=True, vmem_limit_bytes=67043328),
    )(*args)
    return mixed, new_state.reshape(seqs, hd, width)


def solution(mesh):
    sizes = (mesh.shape["grp"], mesh.shape["kv"], mesh.shape["tp"])
    tokens = P(("grp", "kv"), None, "tp")
    placed = (
        tokens, P(), P("kv", "tp"), P("kv", "tp"), P("kv", "tp"), P("kv", "tp"), P(), P(),
        P("tp"), P(), P("tp", "kv"), tokens, tokens, tokens, tokens, tokens, P(("grp", "kv")),
    )
    return jax.shard_map(
        functools.partial(body, sizes),
        mesh=mesh,
        in_specs=placed,
        out_specs=(tokens, tokens),
        check_vma=False,
    )
```

```python
import functools

import jax
import jax.numpy as jnp
from jax import lax
from jax.experimental import pallas as pl
from jax.experimental.pallas import tpu as pltpu
from jax.sharding import PartitionSpec as P

EPS = 1e-06
F32 = jnp.float32
BF16 = jnp.bfloat16
MESH = pl.DeviceIdType.MESH


def kernel(
    cfg,
    tok_hbm, gain_hbm, wq_hbm, wk_hbm, wv_hbm, wg_hbm, wb_hbm, wd_hbm, base_hbm, og_hbm, wo_hbm,
    state_hbm, pk_hbm, pv_hbm, pb_hbm, pd_hbm, acc_hbm,
    mixed_ref, new_hbm,
    gain_ref, wb_ref, wd_ref, base_ref, og_ref, pk_ref, pv_ref, pb_ref, pd_ref, acc_ref, tok, wp, wo, st, normed, kq, res, tk, up, al, rows_a, rows_b, proj, send_buf, recv_buf, gate_buf, own_share,
    in_sem, own_sem, zr_send, zl_send, z_recv, y_send, y_recv, t_send, t_recv, r_send, r_recv,
    out_sem, small_sem,
):
    n_grp, n_kv, n_tp, seqs, props, heads, hd, gather_out = cfg
    width = heads * hd
    g = lax.axis_index("grp")
    k = lax.axis_index("kv")
    t_me = lax.axis_index("tp")
    rows = seqs * props
    own_rows = wk_hbm.shape[0]
    piece = own_rows // n_grp
    out_piece = wo.shape[1] // n_grp
    sources = [wk_hbm, wq_hbm, wv_hbm, wg_hbm]
    n_mat = len(sources) + (1 if gather_out else 0)

    tok_in = pltpu.make_async_copy(tok_hbm, tok.at[t_me], in_sem.at[0])
    tok_in.start()
    own_copies = []
    for m in range(n_mat):
        if m < len(sources):
            dst = wp.at[m, pl.ds(k * own_rows, own_rows), :]
            copy = pltpu.make_async_copy(sources[m], dst, own_sem.at[m])
        else:
            copy = pltpu.make_async_copy(wo_hbm, wo.at[k], own_sem.at[m])
        copy.start()
        own_copies.append(copy)
    early, late = [], []
    pairs = [
        (pk_hbm, pk_ref, early), (pv_hbm, pv_ref, early), (pb_hbm, pb_ref, early),
        (pd_hbm, pd_ref, early), (acc_hbm, acc_ref, early), (gain_hbm, gain_ref, late),
        (wb_hbm, wb_ref, late), (wd_hbm, wd_ref, late), (base_hbm, base_ref, late),
        (og_hbm, og_ref, late),
    ]
    for i, (src, dst, group) in enumerate(pairs):
        copy = pltpu.make_async_copy(src, dst, small_sem.at[i])
        copy.start()
        group.append(copy)
    state_in = pltpu.make_async_copy(state_hbm, st, in_sem.at[1])
    state_in.start()
    out_in = None
    if not gather_out:
        out_in = pltpu.make_async_copy(wo_hbm, wo, own_sem.at[n_mat])
        out_in.start()

    barrier = pltpu.get_barrier_semaphore()

    def greet(dev):
        pl.semaphore_signal(barrier, inc=1, device_id=dev, device_id_type=MESH)

    @pl.when(k > 0)
    def _():
        greet({"kv": k - 1})

    @pl.when(k < n_kv - 1)
    def _():
        greet({"kv": k + 1})

    for d in range(1, n_grp):
        greet({"grp": lax.rem(g + d, n_grp)})
    for d in range(1, n_tp):
        greet({"tp": lax.rem(t_me + d, n_tp)})

    beside = jnp.minimum(k, 1) + jnp.minimum(n_kv - 1 - k, 1)
    pl.semaphore_wait(barrier, n_grp + n_tp - 2 + beside)

    def slot(m, origin, part):
        if m < len(sources):
            return wp.at[m, pl.ds(origin * own_rows + part * piece, piece), :]
        return wo.at[origin, pl.ds(part * out_piece, out_piece), :]

    def z_right(m, origin):
        ref = slot(m, origin, g)
        return pltpu.make_async_remote_copy(
            ref, ref, zr_send.at[m, origin], z_recv.at[m, origin],
            device_id={"kv": k + 1}, device_id_type=MESH)

    def z_left(m, origin):
        ref = slot(m, origin, g)
        return pltpu.make_async_remote_copy(
            ref, ref, zl_send.at[m, origin], z_recv.at[m, origin],
            device_id={"kv": k - 1}, device_id_type=MESH)

    def y_copy(m, origin, d):
        ref = slot(m, origin, g)
        return pltpu.make_async_remote_copy(
            ref, ref, y_send.at[d - 1, m, origin], y_recv.at[d - 1, m, origin],
            device_id={"grp": lax.rem(g + d, n_grp)}, device_id_type=MESH)

    def y_wait(m, origin, d):
        ref = slot(m, origin, lax.rem(g + n_grp - d, n_grp))
        pltpu.make_async_remote_copy(
            ref, ref, y_send.at[d - 1, m, origin], y_recv.at[d - 1, m, origin],
            device_id={"grp": lax.rem(g + d, n_grp)}, device_id_type=MESH).wait_recv()

    def send_own(m):
        own_copies[m].wait()

        @pl.when(k < n_kv - 1)
        def _():
            z_right(m, k).start()

        @pl.when(k > 0)
        def _():
            z_left(m, k).start()

    def forward_step(m, s):
        left = k - 1 - s
        right = k + 1 + s

        @pl.when(left >= 0)
        def _():
            z_right(m, left).wait_recv()

            @pl.when(k < n_kv - 1)
            def _():
                z_right(m, left).start()

            for d in range(1, n_grp):
                y_copy(m, left, d).start()

        @pl.when(right < n_kv)
        def _():
            z_left(m, right).wait_recv()

            @pl.when(k > 0)
            def _():
                z_left(m, right).start()

            for d in range(1, n_grp):
                y_copy(m, right, d).start()

    def forward(m):
        def step(s, carry):
            forward_step(m, s)
            return carry

        lax.fori_loop(0, n_kv - 1, step, 0)

    def wait_y(m):
        def step(o, carry):
            @pl.when(o != k)
            def _():
                for d in range(1, n_grp):
                    y_wait(m, o, d)

            return carry

        lax.fori_loop(0, n_kv, step, 0)

    def t_copy(d):
        return pltpu.make_async_remote_copy(
            tok.at[t_me], tok.at[t_me], t_send.at[d - 1], t_recv.at[d - 1],
            device_id={"tp": lax.rem(t_me + d, n_tp)}, device_id_type=MESH)

    def t_wait(d):
        origin = lax.rem(t_me + n_tp - d, n_tp)
        pltpu.make_async_remote_copy(
            tok.at[origin], tok.at[origin], t_send.at[d - 1], t_recv.at[d - 1],
            device_id={"tp": lax.rem(t_me + d, n_tp)}, device_id_type=MESH).wait_recv()

    send_own(0)
    tok_in.wait()
    for d in range(1, n_tp):
        t_copy(d).start()
    send_own(1)
    send_own(2)

    blk = (
        lax.broadcasted_iota(jnp.int32, (width, width), 0) // hd
        == lax.broadcasted_iota(jnp.int32, (width, width), 1) // hd
    ).astype(F32).astype(BF16)
    lane_head = lax.broadcasted_iota(jnp.int32, (1, width), 1) // hd
    masks = [(lane_head == h).astype(F32) for h in range(heads)]

    def head_sum(x):
        hi = x.astype(BF16)
        lo = (x - hi.astype(F32)).astype(BF16)
        return jnp.dot(hi, blk, preferred_element_type=F32) + jnp.dot(
            lo, blk, preferred_element_type=F32)

    lanes = 128
    blocks = width // lanes

    def rd(ref, at, *lead):
        return jnp.concatenate([ref[(*lead, c, at)] for c in range(blocks)], axis=-1)

    def wr(ref, at, x, *lead):
        for c in range(blocks):
            ref[(*lead, c, at)] = x[:, c * lanes : (c + 1) * lanes]

    every = pl.ds(0, rows)

    pad = 2 * props

    def by_state(s, carry):
        tile = st[pl.ds(pl.multiple_of(s * hd, hd), hd), :]
        stacked = jnp.concatenate([(tile * mask).astype(BF16) for mask in masks], axis=0)
        at = pl.ds(pl.multiple_of(s * pad, pad), pad)
        lhs = rd(kq, at).astype(BF16)
        wr(res, at, jnp.dot(lhs, stacked, preferred_element_type=F32))
        return carry

    def solve(keys, values, weights, logs, queries):
        cumul = []
        run = None
        for t in range(props):
            run = logs[t] if run is None else run + logs[t]
            cumul.append(run)
        low = [(i, j) for i in range(props) for j in range(i)]
        products = [keys[i] * keys[j] for i, j in low]
        full = []
        if queries is not None:
            full = [(i, j) for i in range(props) for j in range(i + 1)]
            products += [queries[i] * keys[j] for i, j in full]
        sums = head_sum(jnp.concatenate(products, axis=0))
        sums = [sums[i * seqs : (i + 1) * seqs] for i in range(len(products))]
        kk = dict(zip(low, sums))
        qk = dict(zip(full, sums[len(low):]))
        dec = {pair: jnp.exp(cumul[pair[0]] - cumul[pair[1]]) for pair in low}
        growth = [jnp.exp(c) for c in cumul]
        update = []
        for t in range(props):
            seen = rd(res, pl.ds(t, seqs, stride=pad))
            term = values[t] - growth[t] * seen
            for j in range(t):
                term = term - kk[t, j] * dec[t, j] * update[j]
            update.append(weights[t] * term)
        outs = []
        if queries is not None:
            for t in range(props):
                out = growth[t] * rd(res, pl.ds(props + t, seqs, stride=pad))
                for j in range(t + 1):
                    score = qk[t, j] if j == t else qk[t, j] * dec[t, j]
                    out = out + score * update[j]
                outs.append(out)
        return cumul, growth, update, outs

    def split(ref):
        return [rd(ref, pl.ds(t, seqs, stride=props)) for t in range(props)]

    for copy in early:
        copy.wait()
    pk = pk_ref[...].astype(F32).reshape(rows, width)
    wr(rows_a, every, pk * lax.rsqrt(head_sum(pk * pk) + EPS))
    wr(rows_b, every, pv_ref[...].astype(F32).reshape(rows, width))
    keys = split(rows_a)
    values = split(rows_b)
    own_head = (
        lax.broadcasted_iota(jnp.int32, (heads, width), 0)
        == lax.broadcasted_iota(jnp.int32, (heads, width), 1) // hd
    ).astype(F32)

    def over_lanes(x):
        return lax.dot_general(
            x, own_head, (((0,), (0,)), ((), ())),
            precision=lax.Precision.HIGHEST, preferred_element_type=F32)

    weights, logs = [], []
    for t in range(props):
        live = (acc_ref[...] > t).astype(F32)
        weights.append(over_lanes(jax.nn.sigmoid(pb_ref[t]) * live))
        logs.append(over_lanes(pd_ref[t] * live))
        wr(kq, pl.ds(t, seqs, stride=pad), keys[t])
        wr(kq, pl.ds(props + t, seqs, stride=pad), keys[t])
    state_in.wait()
    lax.fori_loop(0, seqs, by_state, 0, unroll=4)
    cumul, growth, update, _ = solve(keys, values, weights, logs, None)
    al[...] = growth[-1]
    for t in range(props):
        wr(tk, pl.ds(t, seqs, stride=pad), jnp.exp(cumul[-1] - cumul[t]) * keys[t])
        wr(up, pl.ds(t, seqs, stride=pad), update[t])
        wr(tk, pl.ds(props + t, seqs, stride=pad), jnp.zeros((seqs, width), F32))
        wr(up, pl.ds(props + t, seqs, stride=pad), jnp.zeros((seqs, width), F32))

    def renew(s, carry):
        at = pl.ds(pl.multiple_of(s * pad, pad), pad)
        outer = lax.dot_general(
            rd(tk, at), rd(up, at), (((0,), (0,)), ((), ())), preferred_element_type=F32)
        where = pl.ds(pl.multiple_of(s * hd, hd), hd)
        tile = al[pl.ds(s, 1), :] * st[where, :]
        for h in range(heads):
            tile = tile + masks[h] * outer[h * hd : (h + 1) * hd, :]
        st[where, :] = tile
        return carry

    forward(0)
    send_own(3)
    lax.fori_loop(0, seqs // 2, renew, 0, unroll=2)
    forward(1)
    if gather_out:
        send_own(n_mat - 1)
    lax.fori_loop(seqs // 2, seqs, renew, 0, unroll=2)
    state_out = pltpu.make_async_copy(st, new_hbm, out_sem)
    state_out.start()

    for d in range(1, n_tp):
        t_wait(d)
    for copy in late:
        copy.wait()
    square = jnp.zeros((rows, 1), F32)
    for i in range(n_tp):
        wide = tok[i].astype(F32).reshape(rows, -1)
        square = square + jnp.sum(wide * wide, -1, keepdims=True)
    feats = tok.shape[3]
    scale = lax.rsqrt(square / (n_tp * feats) + EPS)
    for i in range(n_tp):
        cols = slice(i * feats, (i + 1) * feats)
        normed[:, cols] = (tok[i].astype(F32).reshape(rows, -1) * scale * gain_ref[:, cols]).astype(BF16)
    all_heads = wb_ref.shape[0]
    pick = (
        lax.broadcasted_iota(jnp.int32, (all_heads, width), 0)
        == t_me * heads + lax.broadcasted_iota(jnp.int32, (all_heads, width), 1) // hd
    ).astype(F32)

    def per_head(ref):
        raw = lax.dot_general(
            normed[...], ref[...], (((1,), (1,)), ((), ())), preferred_element_type=F32)
        return jnp.dot(raw, pick, precision=lax.Precision.HIGHEST, preferred_element_type=F32)

    wr(rows_a, every, jax.nn.sigmoid(per_head(wb_ref)))
    weights = split(rows_a)
    base = jnp.zeros((1, width), F32)
    for h in range(heads):
        base = jnp.where(lane_head == h, base_ref[:, h : h + 1], base)
    wr(rows_b, every, -base * jax.nn.softplus(per_head(wd_ref)))
    logs = split(rows_b)

    def project(m):
        return jnp.dot(normed[...], wp[m], preferred_element_type=F32)

    def finish(m):
        wait_y(m)
        if m < len(sources):
            value = project(m)
            if m == 0:
                value = value * lax.rsqrt(head_sum(value * value) + EPS)
            elif m == 1:
                value = value * lax.rsqrt(head_sum(value * value) + EPS) * hd ** (-0.5)
            wr(proj, every, value, m)

    outs = None
    def r_copy(dest):
        return pltpu.make_async_remote_copy(
            send_buf.at[dest], recv_buf.at[t_me], r_send.at[dest], r_recv.at[t_me],
            device_id={"tp": dest}, device_id_type=MESH)

    def r_wait(origin):
        pltpu.make_async_remote_copy(
            send_buf.at[origin], recv_buf.at[origin], r_send.at[origin], r_recv.at[origin],
            device_id={"tp": origin}, device_id_type=MESH).wait_recv()

    def send_share(dest):
        share = jnp.dot(gate_buf[...], wo[dest], preferred_element_type=F32)

        @pl.when(dest == t_me)
        def _():
            own_share[...] = share

        @pl.when(dest != t_me)
        def _():
            send_buf[dest] = share.astype(BF16)
            r_copy(dest).start()

    for m in range(len(sources)):
        if m >= 2:
            forward(m)
        if m >= 1:
            finish(m - 1)
        if m == 3:
            keys = [rd(proj, pl.ds(t, seqs, stride=props), 0) for t in range(props)]
            queries = [rd(proj, pl.ds(t, seqs, stride=props), 1) for t in range(props)]
            values = [rd(proj, pl.ds(t, seqs, stride=props), 2) for t in range(props)]
            for t in range(props):
                wr(kq, pl.ds(t, seqs, stride=pad), keys[t])
                wr(kq, pl.ds(props + t, seqs, stride=pad), queries[t])
            lax.fori_loop(0, seqs, by_state, 0, unroll=4)
            outs = solve(keys, values, weights, logs, queries)[3]
            for t in range(props):
                wr(rows_a, pl.ds(t, seqs, stride=props), outs[t])
            out = rd(rows_a, every)
            out = out * lax.rsqrt(head_sum(out * out) / hd + EPS)
            tile_gain = (
                lax.broadcasted_iota(jnp.int32, (hd, width), 0)
                == lax.broadcasted_iota(jnp.int32, (hd, width), 1) % hd
            ).astype(F32)
            gain = jnp.dot(
                jnp.broadcast_to(og_ref[...], (8, hd)), tile_gain,
                precision=lax.Precision.HIGHEST, preferred_element_type=F32)[:1]
            wr(rows_a, every, out * gain)
    finish(len(sources) - 1)
    gate = rd(proj, every, 3)
    gate_buf[...] = (rd(rows_a, every) * (gate / (1.0 + jnp.exp(-gate)))).astype(BF16)
    if gather_out:
        m = n_mat - 1

        def take(s, carry):
            @pl.when(s < n_kv - 1)
            def _():
                forward_step(m, s)

            @pl.when(k - s >= 0)
            def _():
                @pl.when(s > 0)
                def _():
                    for d in range(1, n_grp):
                        y_wait(m, k - s, d)

                send_share(k - s)

            @pl.when(jnp.logical_and(s > 0, k + s < n_kv))
            def _():
                for d in range(1, n_grp):
                    y_wait(m, k + s, d)
                send_share(k + s)

            return carry

        lax.fori_loop(0, n_kv, take, 0)
    else:
        out_in.wait()
        for d in range(n_tp):
            send_share(lax.rem(t_me + d, n_tp))
    total = own_share[...]
    for d in range(1, n_tp):
        origin = lax.rem(t_me + d, n_tp)
        r_wait(origin)
        total = total + recv_buf[origin].astype(F32)
    mixed_ref[...] = total.reshape(seqs, props, feats).astype(BF16)

    for d in range(1, n_tp):
        t_copy(d).wait_send()
        r_copy(lax.rem(t_me + d, n_tp)).wait_send()

    def drain(m):
        def step(o, carry):
            @pl.when(jnp.logical_and(o <= k, k < n_kv - 1))
            def _():
                z_right(m, o).wait_send()

            @pl.when(jnp.logical_and(o >= k, k > 0))
            def _():
                z_left(m, o).wait_send()

            @pl.when(o != k)
            def _():
                for d in range(1, n_grp):
                    y_copy(m, o, d).wait_send()

            return carry

        lax.fori_loop(0, n_kv, step, 0)

    for m in range(n_mat):
        drain(m)
    state_out.wait()


def pair_kernel(
    cfg,
    tok_hbm, gain_hbm, wq_hbm, wk_hbm, wv_hbm, wg_hbm, wb_hbm, wd_hbm, base_hbm, og_hbm, wo_hbm,
    state_hbm, pk_hbm, pv_hbm, pb_hbm, pd_hbm, acc_hbm,
    mixed_ref, st,
    gain_ref, wbd_ref, base_ref, og_ref, pkv_ref, pbd_ref, acc_ref, tok, wp, wo, normed, kq, res, tk, up, al, rows_a, rows_b, proj, own_part, part_send, part_recv, small_own, small_send, small_recv, send_buf, recv_buf, gate_buf, own_share,
    in_sem, own_sem, wz_send, wz_recv, wy_recv, t_send, f_send, d_send, t_recv, zs_send, z_recv, y_send, y_recv, p_send, p_recv, s_recv, r_recv,
    small_sem,
):
    n_grp, n_kv, n_tp, seqs, props, heads, hd = cfg
    width = heads * hd
    g = lax.axis_index("grp")
    k = lax.axis_index("kv")
    t_me = lax.axis_index("tp")
    rows = seqs * props
    own_rows = wk_hbm.shape[0]
    piece = own_rows // n_grp
    out_piece = wo.shape[1] // n_grp
    out_bits = 2
    w_bits = 2
    out_bit = out_piece // out_bits
    feats = tok_hbm.shape[2]
    sources = [wk_hbm, wq_hbm, wv_hbm, wg_hbm]
    n_src = len(sources)
    all_heads = wb_hbm.shape[0]
    pair = k // 2
    side = lax.rem(k, 2)
    mate = k + 1 - 2 * side
    partner = lax.rem(k + n_kv // 2, n_kv)
    chip = t_me // 2
    core = lax.rem(t_me, 2)
    beside_core = 2 * chip + 1 - core
    home = lax.rem(pair + chip + 1, 2)
    g_other = lax.rem(g + 1, n_grp)
    half_feats = 2 * feats

    own_slot = home * (2 + core) + (1 - home) * 4
    tok_in = pltpu.make_async_copy(tok_hbm, tok.at[own_slot], in_sem.at[0])
    tok_in.start()
    own_copies = []
    for m in range(n_src + 1):
        if m < n_src:
            dst = wp.at[m, pl.ds(side * own_rows, own_rows), :]
            copy = pltpu.make_async_copy(sources[m], dst, own_sem.at[min(m, 1)])
        else:
            copy = pltpu.make_async_copy(wo_hbm, wo.at[k], own_sem.at[2])
        copy.start()
        own_copies.append(copy)
    ours = pl.ds(pl.multiple_of(pair * half_feats, half_feats), half_feats)
    loads = [
        (pk_hbm, pkv_ref.at[0], 0), (pv_hbm, pkv_ref.at[1], 0),
        (pb_hbm, pbd_ref.at[0], 1), (pd_hbm, pbd_ref.at[1], 1), (acc_hbm, acc_ref, 2),
        (wb_hbm.at[:, ours], wbd_ref.at[pl.ds(0, all_heads), :], 3),
        (wd_hbm.at[:, ours], wbd_ref.at[pl.ds(all_heads, all_heads), :], 3),
        (gain_hbm.at[:, ours], gain_ref, 4), (base_hbm, base_ref, 5), (og_hbm, og_ref, 6),
    ]
    for src, dst, i in loads:
        pltpu.make_async_copy(src, dst, small_sem.at[i]).start()
    early = [(pkv_ref, 0), (pbd_ref, 1), (acc_ref, 2)]
    late = [(wbd_ref, 3), (gain_ref, 4), (base_ref, 5), (og_ref, 6)]

    def loaded(group):
        for ref, i in group:
            pltpu.make_async_copy(ref, ref, small_sem.at[i]).wait()

    state_in = pltpu.make_async_copy(state_hbm, st, in_sem.at[1])
    state_in.start()

    barrier = pltpu.get_barrier_semaphore()

    def greet(dev):
        pl.semaphore_signal(barrier, inc=1, device_id=dev, device_id_type=MESH)

    for d in range(1, n_kv):
        greet({"kv": lax.rem(k + d, n_kv)})
    for d in range(1, n_tp):
        greet({"tp": lax.rem(t_me + d, n_tp)})
    greet({"grp": g_other})
    far_tp = 2 * (1 - chip) + core
    pl.semaphore_wait(barrier, n_kv + n_tp - 1)

    def remote(src, dst, send, recv, dev):
        return pltpu.make_async_remote_copy(
            src, dst, send, recv, device_id=dev, device_id_type=MESH)

    part = seqs // 2

    def tok_piece(slot, half):
        return tok.at[slot, pl.ds(half * part, part)]

    def tok_partner():
        return remote(tok_piece(4, 0), tok_piece(core, 0), t_send.at[0],
                      t_recv.at[2 * core], {"kv": partner})

    def tok_shift():
        return remote(tok_piece(4, 1), tok_piece(5, 1), t_send.at[1], t_recv.at[6],
                      {"tp": far_tp})

    def tok_relay():
        return remote(tok_piece(5, 1), tok_piece(core, 1), t_send.at[0],
                      t_recv.at[2 * core + 1], {"kv": partner})

    def tok_far(half):
        ref = tok_piece(core, half)
        return remote(ref, ref, f_send.at[0], t_recv.at[2 * core + half], {"tp": far_tp})

    def tok_beside(half):
        ref = tok_piece(core, half)
        return remote(ref, ref, d_send.at[0], t_recv.at[2 * core + half], {"tp": beside_core})

    def own_far():
        ref = tok.at[2 + core]
        return remote(ref, ref, f_send.at[1], t_recv.at[4 + core], {"tp": far_tp})

    def own_beside():
        ref = tok.at[2 + core]
        return remote(ref, ref, d_send.at[0], t_recv.at[4 + core], {"tp": beside_core})

    def tok_wait(ref, index):
        remote(ref, ref, d_send.at[0], t_recv.at[index], {"tp": beside_core}).wait_recv()

    def tok_land_z():
        tok_wait(tok_piece(core, 1 - home), 2 * core + 1 - home)
        tok_far(1 - home).start()
        tok_beside(1 - home).start()

    def tok_land_x():
        tok_wait(tok_piece(core, home), 2 * core + home)
        tok_beside(home).start()

    def w_slot(m, block, half, bit):
        at = pl.ds(block * own_rows + half * piece + bit * (piece // w_bits), piece // w_bits)
        return wp.at[m, at, :]

    def w_mate(m, bit):
        ref = w_slot(m, side, g, bit)
        return remote(ref, ref, wz_send.at[0], wz_recv.at[m, bit], {"kv": mate})

    def w_share(m, bit):
        ref = w_slot(m, 1 - side, g, bit)
        return remote(ref, ref, wz_send.at[0], wy_recv.at[m], {"grp": g_other})

    def w_pass(m):
        for bit in range(w_bits):
            ref = w_slot(m, 1 - side, g, bit)
            remote(ref, ref, wz_send.at[0], wz_recv.at[m, bit], {"kv": mate}).wait_recv()
            w_share(m, bit).start()

    def w_ready(m):
        at = pl.ds((1 - side) * own_rows + g_other * piece, piece)
        ref = wp.at[m, at, :]
        remote(ref, ref, wz_send.at[0], wy_recv.at[m], {"grp": g_other}).wait_recv()

    def o_slot(origin, part, bit):
        return wo.at[origin, pl.ds(part * out_piece + bit * out_bit, out_bit), :]

    def z_right(origin, bit):
        ref = o_slot(origin, g, bit)
        return remote(ref, ref, zs_send.at[1 - pair], z_recv.at[origin, bit], {"kv": k + 1})

    def z_left(origin, bit):
        ref = o_slot(origin, g, bit)
        return remote(ref, ref, zs_send.at[pair], z_recv.at[origin, bit], {"kv": k - 1})

    def y_copy(origin, bit):
        ref = o_slot(origin, g, bit)
        return remote(ref, ref, y_send.at[0], y_recv.at[origin], {"grp": g_other})

    def y_wait(origin):
        ref = wo.at[origin, pl.ds(g_other * out_piece, out_piece), :]
        remote(ref, ref, y_send.at[0], y_recv.at[origin], {"grp": g_other}).wait_recv()

    def right_start(origin):
        for bit in range(out_bits):
            z_right(origin, bit).start()

    def left_start(origin):
        for bit in range(out_bits):
            z_left(origin, bit).start()

    def from_left(origin):
        for bit in range(out_bits):
            z_right(origin, bit).wait_recv()

            @pl.when(k < n_kv - 1)
            def _():
                z_right(origin, bit).start()

    def from_right(origin):
        for bit in range(out_bits):
            z_left(origin, bit).wait_recv()

            @pl.when(k > 0)
            def _():
                z_left(origin, bit).start()

    def share_out(origin):
        for bit in range(out_bits):
            y_copy(origin, bit).start()

    def middle_pass(s):
        @pl.when(jnp.logical_and(side == 1, pair == 0))
        def _():
            if s == 0:
                from_left(k - 1)
            else:
                from_right(k + s)

        @pl.when(jnp.logical_and(side == 0, pair == 1))
        def _():
            if s == 0:
                from_right(k + 1)
            else:
                from_left(k - s)

    def middle_share(s):
        @pl.when(jnp.logical_and(side == 1, pair == 0))
        def _():
            share_out(k - 1 if s == 0 else k + s)

        @pl.when(jnp.logical_and(side == 0, pair == 1))
        def _():
            share_out(k + 1 if s == 0 else k - s)

    def end_pass(s, bits=(0, 1)):
        for bit in bits:
            @pl.when(k == 0)
            def _():
                z_left(k + s, bit).wait_recv()
                y_copy(k + s, bit).start()

            @pl.when(k == n_kv - 1)
            def _():
                z_right(k - s, bit).wait_recv()
                y_copy(k - s, bit).start()

    def p_copy(m, b):
        at = pl.ds(b * half_rows, half_rows)
        return remote(part_send.at[m, at], part_recv.at[m, at], p_send.at[0],
                      p_recv.at[max(m, 1) - 1, b], {"kv": partner})

    def small_copy():
        return remote(small_send, small_recv, p_send.at[1], s_recv.at[0],
                      {"kv": partner})

    at_end = jnp.logical_or(k == 0, k == n_kv - 1)
    tok_in.wait()

    @pl.when(home == 0)
    def _():
        tok_shift().start()
        tok_partner().start()

    @pl.when(home == 1)
    def _():
        own_far().start()
        own_beside().start()

    def w_first(m):
        for bit in range(w_bits):
            w_mate(m, bit).start()

    own_copies[0].wait()
    w_first(0)
    own_copies[n_src].wait()

    def w_rest():
        @pl.when(k == 0)
        def _():
            right_start(k)

        @pl.when(k == n_kv - 1)
        def _():
            left_start(k)

        rest = wp.at[pl.ds(1, n_src - 1), pl.ds(side * own_rows, own_rows), :]
        pltpu.make_async_copy(rest, rest, own_sem.at[1]).wait()
        for m in range(1, n_src):
            w_first(m)

    relays_first = jnp.logical_and(at_end, home == 1)

    @pl.when(jnp.logical_not(relays_first))
    def _():
        w_rest()

    blk = (
        lax.broadcasted_iota(jnp.int32, (width, width), 0) // hd
        == lax.broadcasted_iota(jnp.int32, (width, width), 1) // hd
    ).astype(F32).astype(BF16)
    lane_head = lax.broadcasted_iota(jnp.int32, (1, width), 1) // hd
    masks = [(lane_head == h).astype(F32) for h in range(heads)]

    def head_sum(x):
        hi = x.astype(BF16)
        lo = (x - hi.astype(F32)).astype(BF16)
        return jnp.dot(hi, blk, preferred_element_type=F32) + jnp.dot(
            lo, blk, preferred_element_type=F32)

    lanes = 128
    blocks = width // lanes

    def rd(ref, at, *lead):
        return jnp.concatenate([ref[(*lead, c, at)] for c in range(blocks)], axis=-1)

    def wr(ref, at, x, *lead):
        for c in range(blocks):
            ref[(*lead, c, at)] = x[:, c * lanes : (c + 1) * lanes]

    every = pl.ds(0, rows)
    count = seqs // 2
    half_rows = count * props

    pad = 2 * props

    def head_first(x, head):
        block, at = divmod(head * hd, lanes)
        x = x[:, block * lanes : (block + 1) * lanes]
        return jnp.concatenate([x[:, at:], x[:, :at]], axis=-1) if at else x

    def put_heads(ref, x, first, each, low=0):
        step = heads * each
        for head in range(heads):
            at = pl.ds(low * step + head * each + first, x.shape[0], stride=step)
            ref[at] = head_first(x, head)

    def by_state(s, carry):
        at = pl.ds(pl.multiple_of(s * heads * pad, heads * pad), heads * pad)
        tile = st[pl.ds(pl.multiple_of(s * hd, hd), hd), :].astype(BF16)
        found = jnp.dot(kq[at, :hd].astype(BF16), tile, preferred_element_type=F32)
        own = masks[0] * found[:pad]
        for head in range(1, heads):
            own = own + masks[head] * found[head * pad : (head + 1) * pad]
        wr(res, pl.ds(pl.multiple_of(s * pad, pad), pad), own)
        return carry

    def solve(keys, values, weights, logs, queries, start=0):
        count = keys[0].shape[0]
        cumul = []
        run = None
        for t in range(props):
            run = logs[t] if run is None else run + logs[t]
            cumul.append(run)
        low = [(i, j) for i in range(props) for j in range(i)]
        products = [keys[i] * keys[j] for i, j in low]
        full = []
        if queries is not None:
            full = [(i, j) for i in range(props) for j in range(i + 1)]
            products += [queries[i] * keys[j] for i, j in full]
        sums = head_sum(jnp.concatenate(products, axis=0))
        sums = [sums[i * count : (i + 1) * count] for i in range(len(products))]
        kk = dict(zip(low, sums))
        qk = dict(zip(full, sums[len(low):]))
        dec = {pair: jnp.exp(cumul[pair[0]] - cumul[pair[1]]) for pair in low}
        growth = [jnp.exp(c) for c in cumul]
        update = []
        for t in range(props):
            seen = rd(res, pl.ds(start * pad + t, count, stride=pad))
            term = values[t] - growth[t] * seen
            for j in range(t):
                term = term - kk[t, j] * dec[t, j] * update[j]
            update.append(weights[t] * term)
        outs = []
        if queries is not None:
            for t in range(props):
                out = growth[t] * rd(
                    res, pl.ds(start * pad + props + t, count, stride=pad))
                for j in range(t + 1):
                    score = qk[t, j] if j == t else qk[t, j] * dec[t, j]
                    out = out + score * update[j]
                outs.append(out)
        return cumul, growth, update, outs

    def split(ref):
        return [rd(ref, pl.ds(t, seqs, stride=props)) for t in range(props)]

    loaded(early)
    pk = pkv_ref[0].astype(F32).reshape(rows, width)
    wr(rows_a, every, pk * lax.rsqrt(head_sum(pk * pk) + EPS))
    wr(rows_b, every, pkv_ref[1].astype(F32).reshape(rows, width))
    keys = split(rows_a)
    values = split(rows_b)
    own_head = (
        lax.broadcasted_iota(jnp.int32, (heads, width), 0)
        == lax.broadcasted_iota(jnp.int32, (heads, width), 1) // hd
    ).astype(F32)

    def over_lanes(x):
        return lax.dot_general(
            x, own_head, (((0,), (0,)), ((), ())),
            precision=lax.Precision.HIGHEST, preferred_element_type=F32)

    weights, logs = [], []
    for t in range(props):
        live = (acc_ref[...] > t).astype(F32)
        weights.append(over_lanes(jax.nn.sigmoid(pbd_ref[0, t]) * live))
        logs.append(over_lanes(pbd_ref[1, t] * live))
        put_heads(kq, keys[t], t, pad)
        put_heads(kq, keys[t], props + t, pad)
    state_in.wait()
    lax.fori_loop(0, seqs, by_state, 0, unroll=4)
    cumul, growth, update, _ = solve(keys, values, weights, logs, None)
    al[...] = growth[-1]
    for t in range(props):
        put_heads(tk, jnp.exp(cumul[-1] - cumul[t]) * keys[t], t, props)
        for head in range(heads):
            wr(up, pl.ds(head * props + t, seqs, stride=heads * props), masks[head] * update[t])

    def renew(s, carry):
        each = heads * props
        at = pl.ds(pl.multiple_of(s * each, each), each)
        outer = lax.dot_general(
            tk[at, :hd], rd(up, at), (((0,), (0,)), ((), ())), preferred_element_type=F32)
        where = pl.ds(pl.multiple_of(s * hd, hd), hd)
        st[where, :] = al[pl.ds(s, 1), :] * st[where, :] + outer
        return carry


    @pl.when(home == 1)
    def _():
        tok_wait(tok_piece(5, 1), 6)
        tok_relay().start()

    @pl.when(relays_first)
    def _():
        w_rest()

    @pl.when(home == 0)
    def _():
        tok_wait(tok.at[2 + core], 4 + core)
        own_beside().start()

    @pl.when(home == 1)
    def _():
        tok_land_z()

    w_pass(0)

    @pl.when(jnp.logical_not(at_end))
    def _():
        right_start(k)
        left_start(k)

    @pl.when(home == 0)
    def _():
        tok_land_z()
        tok_land_x()

    middle_pass(0)
    middle_share(0)

    @pl.when(home == 1)
    def _():
        tok_land_x()

    w_pass(1)
    middle_pass(1)

    loaded(late)
    tok_wait(tok.at[3 - core], 5 - core)
    for half in range(2):
        tok_wait(tok_piece(1 - core, half), 2 * (1 - core) + half)
    ones = jnp.ones((8, feats), BF16)
    squares = jnp.zeros((8, 2 * rows), F32)
    last = (((1,), (1,)), ((), ()))
    for c in range(2):
        cols = slice(c * feats, (c + 1) * feats)
        wide = jnp.concatenate(
            [tok[c].astype(F32).reshape(rows, feats), tok[2 + c].astype(F32).reshape(rows, feats)],
            axis=0)
        normed[:, cols] = (wide * gain_ref[:, cols]).astype(BF16)
        sq = wide * wide
        hi = sq.astype(BF16)
        lo = (sq - hi.astype(F32)).astype(BF16)
        squares = squares + lax.dot_general(ones, hi, last, preferred_element_type=F32)
        squares = squares + lax.dot_general(ones, lo, last, preferred_element_type=F32)
    raw = lax.dot_general(wbd_ref[...], normed[...], last, preferred_element_type=F32)
    small = jnp.concatenate([raw, squares], axis=0)
    kind = lax.broadcasted_iota(jnp.int32, (small_own.shape[0], small.shape[0]), 0)
    taken = lax.broadcasted_iota(jnp.int32, (small_own.shape[0], small.shape[0]), 1)
    first_head = t_me * heads
    wanted = jnp.where(
        kind < heads, first_head + kind,
        jnp.where(kind < 2 * heads, all_heads + first_head + kind - heads, 2 * all_heads))
    small = jnp.dot(
        (taken == wanted).astype(F32), small,
        precision=lax.Precision.HIGHEST, preferred_element_type=F32)
    small_send[...] = small[:, :rows]
    small_copy().start()
    small_own[...] = small[:, rows:]

    def project(m):
        both = jnp.dot(normed[...], wp[m], preferred_element_type=F32)
        part_send[m] = both[:rows].astype(BF16)
        own_part[m] = both[rows:]

    def give(*pieces):
        for m, b in pieces:
            p_copy(m, b).start()

    w_ready(0)
    project(0)
    give((0, 0), (0, 1))
    w_pass(2)
    w_ready(1)
    project(1)
    give((1, 0))
    w_pass(3)
    middle_pass(2)
    end_pass(1)
    middle_share(1)
    middle_share(2)
    lax.fori_loop(0, seqs // 2, renew, 0, unroll=4)
    w_ready(2)
    project(2)
    give((2, 0), (1, 1))
    lax.fori_loop(seqs // 2, seqs, renew, 0, unroll=4)
    w_ready(3)
    project(3)
    give((3, 0), (2, 1), (3, 1))
    end_pass(2)

    small_copy().wait_recv()
    small = small_own[...] + small_recv[...]
    scale = lax.rsqrt(small[2 * heads :] / (n_tp * feats) + EPS)
    beta = small[:heads] * scale[:1]
    decay = small[heads : 2 * heads] * scale[:1]

    def spread(x, over):
        return lax.dot_general(
            x, over, (((0,), (0,)), ((), ())),
            precision=lax.Precision.HIGHEST, preferred_element_type=F32)

    wr(rows_a, every, spread(jax.nn.sigmoid(beta), own_head))
    base = jnp.zeros((1, width), F32)
    for h in range(heads):
        base = jnp.where(lane_head == h, base_ref[:, h : h + 1], base)
    wr(rows_b, every, -base * spread(jax.nn.softplus(decay), own_head))
    row_scale = spread(
        scale, (lax.broadcasted_iota(jnp.int32, (scale.shape[0], width), 0) == 0).astype(F32))

    def finish(m, b):
        if m == 0:
            ref = part_recv.at[pl.ds(0, 2), pl.ds(b * half_rows, half_rows)]
            remote(ref, ref, p_send.at[0], p_recv.at[0, b], {"kv": partner}).wait_recv()
        elif m > 1:
            p_copy(m, b).wait_recv()
        at = slice(b * half_rows, (b + 1) * half_rows)
        value = (own_part[m, at] + part_recv[m, at].astype(F32)) * row_scale[at]
        if m == 0:
            value = value * lax.rsqrt(head_sum(value * value) + EPS)
        elif m == 1:
            value = value * lax.rsqrt(head_sum(value * value) + EPS) * hd ** (-0.5)
        wr(proj, pl.ds(b * half_rows, half_rows), value, m)

    def r_copy(dest, b):
        at = pl.ds(b * half_rows, half_rows)
        far = lax.rem(t_me - dest + n_tp, n_tp)
        return remote(send_buf.at[dest, at], recv_buf.at[far - 1, at], y_send.at[0],
                      r_recv.at[b], {"tp": dest})

    def r_wait(b):
        ref = recv_buf.at[pl.ds(0, n_tp - 1), pl.ds(b * half_rows, half_rows)]
        remote(ref, ref, y_send.at[0], r_recv.at[b], {"tp": beside_core}).wait_recv()

    def send_share(dest, b):
        at = slice(b * half_rows, (b + 1) * half_rows)
        share = jnp.dot(gate_buf[at], wo[dest], preferred_element_type=F32)

        @pl.when(dest == t_me)
        def _():
            own_share[at] = share

        @pl.when(dest != t_me)
        def _():
            send_buf[dest, at] = share.astype(BF16)
            r_copy(dest, b).start()

    tile_gain = (
        lax.broadcasted_iota(jnp.int32, (hd, width), 0)
        == lax.broadcasted_iota(jnp.int32, (hd, width), 1) % hd
    ).astype(F32)
    gain = jnp.dot(
        jnp.broadcast_to(og_ref[...], (8, hd)), tile_gain,
        precision=lax.Precision.HIGHEST, preferred_element_type=F32)[:1]

    def delta(b):
        low, first = b * count, b * half_rows
        steps = [pl.ds(first + t, count, stride=props) for t in range(props)]
        for m in range(3):
            finish(m, b)
            if b == 0 and m == 1:
                end_pass(3, (0,))
        keys, queries, values = [[rd(proj, at, m) for at in steps] for m in range(3)]
        weights = [rd(rows_a, at) for at in steps]
        logs = [rd(rows_b, at) for at in steps]
        for t in range(props):
            put_heads(kq, keys[t], t, pad, low)
            put_heads(kq, queries[t], props + t, pad, low)
        lax.fori_loop(low, low + count, by_state, 0, unroll=4)
        if b == 0:
            end_pass(3, (1,))
        outs = solve(keys, values, weights, logs, queries, low)[3]
        for t in range(props):
            wr(rows_a, steps[t], outs[t])
        half = pl.ds(first, half_rows)
        out = rd(rows_a, half)
        out = out * lax.rsqrt(head_sum(out * out) / hd + EPS) * gain
        finish(n_src - 1, b)
        gate = rd(proj, half, 3)
        gate_buf[first : first + half_rows] = (
            out * (gate / (1.0 + jnp.exp(-gate)))).astype(BF16)

    def take(b):
        def step(s, carry):
            @pl.when(k - s >= 0)
            def _():
                if b == 0:
                    @pl.when(s > 0)
                    def _():
                        y_wait(k - s)

                send_share(k - s, b)

            @pl.when(jnp.logical_and(s > 0, k + s < n_kv))
            def _():
                if b == 0:
                    y_wait(k + s)
                send_share(k + s, b)

            return carry

        return step

    def settle(b):
        at = slice(b * half_rows, (b + 1) * half_rows)
        r_wait(b)
        total = own_share[at]
        for d in range(1, n_tp):
            total = total + recv_buf[d - 1, at].astype(F32)
        mixed_ref[b * count : (b + 1) * count] = total.reshape(count, props, feats).astype(BF16)

    delta(0)
    lax.fori_loop(0, n_kv - 1, take(0), 0)
    delta(1)
    lax.fori_loop(0, n_kv - 1, take(1), 0)
    lax.fori_loop(n_kv - 1, n_kv, take(0), 0)
    lax.fori_loop(n_kv - 1, n_kv, take(1), 0)
    def sent(ref, sem):
        remote(ref, ref, sem, s_recv.at[0], {"kv": mate}).wait_send()

    sent(tok.at[pl.ds(0, 2)], d_send.at[0])
    tok_far(1 - home).wait_send()

    @pl.when(home == 1)
    def _():
        own_far().wait_send()
        tok_relay().wait_send()

    @pl.when(home == 0)
    def _():
        tok_partner().wait_send()
        tok_shift().wait_send()

    sent(wp.at[pl.ds(0, 2)], wz_send.at[0])
    sent(part_send, p_send.at[0])
    sent(small_send, p_send.at[1])
    some = pl.ds(0, out_piece)

    @pl.when(at_end)
    def _():
        sent(wo.at[0, some], zs_send.at[1])

    @pl.when(jnp.logical_not(at_end))
    def _():
        sent(wo.at[pl.ds(0, 3), some], zs_send.at[0])
        sent(wo.at[pl.ds(0, 2), some], zs_send.at[1])

    settle(0)
    settle(1)
    sent(wo.at[pl.ds(0, n_kv - 1)], y_send.at[0])

def pair_call(sizes, args, seqs, props, feats, heads, hd, width, rows, pad):
    n_grp, n_kv, n_tp = sizes
    cfg = (n_grp, n_kv, n_tp, seqs, props, heads, hd)
    vmem = pl.BlockSpec(memory_space=pltpu.VMEM)
    hbm = pl.BlockSpec(memory_space=pltpu.HBM)
    dma = pltpu.SemaphoreType.DMA
    own_rows = args[2].shape[0]
    all_heads = args[6].shape[0]
    n_src = 4
    small = (2 * heads + 8, rows)
    return pl.pallas_call(
        functools.partial(pair_kernel, cfg),
        out_shape=(
            pltpu.VMEM((seqs, props, feats), BF16),
            pltpu.VMEM((seqs * hd, width), F32),
        ),
        in_specs=[hbm] * len(args),
        out_specs=(vmem, vmem),
        scratch_shapes=[
            pltpu.VMEM((1, 2 * feats), F32),
            pltpu.VMEM((2 * all_heads, 2 * feats), BF16),
            *[pltpu.VMEM(args[i].shape, args[i].dtype) for i in (8, 9)],
            *[pltpu.VMEM((2, *args[i].shape), args[i].dtype) for i in (12, 14)],
            pltpu.VMEM(args[16].shape, args[16].dtype),
            pltpu.VMEM((6, seqs, props, feats), BF16),
            pltpu.VMEM((n_src, 2 * own_rows, width), BF16),
            pltpu.VMEM((n_tp, width, feats), BF16),
            pltpu.VMEM((2 * rows, 2 * feats), BF16),
            pltpu.VMEM((seqs * heads * pad, 128), F32),
            pltpu.VMEM((width // 128, seqs * pad, 128), F32),
            pltpu.VMEM((seqs * heads * props, 128), F32),
            pltpu.VMEM((width // 128, seqs * heads * props, 128), F32),
            pltpu.VMEM((seqs, width), F32),
            pltpu.VMEM((width // 128, rows, 128), F32),
            pltpu.VMEM((width // 128, rows, 128), F32),
            pltpu.VMEM((n_src, width // 128, rows, 128), F32),
            pltpu.VMEM((n_src, rows, width), F32),
            pltpu.VMEM((n_src, rows, width), BF16),
            pltpu.VMEM((n_src, rows, width), BF16),
            pltpu.VMEM(small, F32),
            pltpu.VMEM(small, F32),
            pltpu.VMEM(small, F32),
            pltpu.VMEM((n_tp, rows, feats), BF16),
            pltpu.VMEM((n_tp, rows, feats), BF16),
            pltpu.VMEM((rows, width), BF16),
            pltpu.VMEM((rows, feats), F32),
            dma((2,)),
            dma((3,)),
            dma((1,)),
            dma((n_src, 2)),
            dma((n_src,)),
            dma((2,)),
            dma((2,)),
            dma((1,)),
            dma((7,)),
            dma((2,)),
            dma((n_kv, 2)),
            dma((1,)),
            dma((n_kv,)),
            dma((2,)),
            dma((n_src - 1, 2)),
            dma((1,)),
            dma((2,)),
            dma((7,)),
        ],
        compiler_params=pltpu.CompilerParams(
            collective_id=1, has_side_effects=True, vmem_limit_bytes=67043328 - rows * feats * 2 - seqs * hd * width * 4),
    )(*args)


def body(
    sizes,
    tokens, in_gain, w_query, w_key, w_value, w_gate, w_beta, w_decay, decay_base, out_gain, w_out,
    state, prev_keys, prev_values, prev_beta, prev_decay, accepted,
):
    n_grp, n_kv, n_tp = sizes
    seqs, props, feats = tokens.shape
    heads = decay_base.shape[0]
    hd = out_gain.shape[0]
    width = heads * hd
    rows = seqs * props
    pad = 2 * props
    paired = (
        n_grp == 2 and n_kv == n_tp and n_kv // 2 == 2
        and w_query.shape[0] == feats and w_query.shape[0] * n_kv == in_gain.shape[0])
    gather_out = n_kv == n_tp
    if not gather_out:
        w_out = lax.all_gather(w_out, "kv", axis=1, tiled=True)
        w_out = jnp.transpose(w_out.reshape(width, n_tp, feats), (1, 0, 2))
    n_mat = 5 if gather_out else 4
    cfg = (n_grp, n_kv, n_tp, seqs, props, heads, hd, gather_out)
    vmem = pl.BlockSpec(memory_space=pltpu.VMEM)
    hbm = pl.BlockSpec(memory_space=pltpu.HBM)
    args = (
        tokens, in_gain.reshape(1, -1), w_query, w_key, w_value, w_gate,
        w_beta.T, w_decay.T, decay_base.reshape(1, -1), out_gain.reshape(1, -1), w_out,
        state.reshape(seqs * hd, width), prev_keys, prev_values,
        jnp.transpose(prev_beta, (1, 2, 0)), jnp.transpose(prev_decay, (1, 2, 0)),
        accepted.reshape(1, seqs),
    )
    if paired:
        mixed, new_state = pair_call(
            sizes, args, seqs, props, feats, heads, hd, width, rows, pad)
        return mixed, new_state.reshape(seqs, hd, width)
    dma = pltpu.SemaphoreType.DMA
    mixed, new_state = pl.pallas_call(
        functools.partial(kernel, cfg),
        out_shape=(
            jax.ShapeDtypeStruct((seqs, props, feats), BF16),
            jax.ShapeDtypeStruct((seqs * hd, width), F32),
        ),
        in_specs=[hbm] * len(args),
        out_specs=(vmem, pl.BlockSpec(memory_space=pl.ANY)),
        scratch_shapes=[
            *[pltpu.VMEM(args[i].shape, args[i].dtype) for i in (1, 6, 7, 8, 9, 12, 13, 14, 15, 16)],
            pltpu.VMEM((n_tp, seqs, props, feats), BF16),
            pltpu.VMEM((4, n_kv * w_key.shape[0], width), BF16),
            pltpu.VMEM((n_tp, width, feats), BF16),
            pltpu.VMEM((seqs * hd, width), F32),
            pltpu.VMEM((rows, n_tp * feats), BF16),
            pltpu.VMEM((width // 128, seqs * pad, 128), F32),
            pltpu.VMEM((width // 128, seqs * pad, 128), F32),
            pltpu.VMEM((width // 128, seqs * pad, 128), F32),
            pltpu.VMEM((width // 128, seqs * pad, 128), F32),
            pltpu.VMEM((seqs, width), F32),
            pltpu.VMEM((width // 128, rows, 128), F32),
            pltpu.VMEM((width // 128, rows, 128), F32),
            pltpu.VMEM((4, width // 128, rows, 128), F32),
            pltpu.VMEM((n_tp, rows, feats), BF16),
            pltpu.VMEM((n_tp, rows, feats), BF16),
            pltpu.VMEM((rows, width), BF16),
            pltpu.VMEM((rows, feats), F32),
            dma((2,)),
            dma((6,)),
            dma((n_mat, n_kv)),
            dma((n_mat, n_kv)),
            dma((n_mat, n_kv)),
            dma((max(n_grp - 1, 1), n_mat, n_kv)),
            dma((max(n_grp - 1, 1), n_mat, n_kv)),
            dma((n_tp - 1,)),
            dma((n_tp - 1,)),
            dma((n_tp,)),
            dma((n_tp,)),
            dma(()),
            dma((10,)),
        ],
        compiler_params=pltpu.CompilerParams(
            collective_id=0, has_side_effects=True, vmem_limit_bytes=67043328),
    )(*args)
    return mixed, new_state.reshape(seqs, hd, width)


def solution(mesh):
    sizes = (mesh.shape["grp"], mesh.shape["kv"], mesh.shape["tp"])
    tokens = P(("grp", "kv"), None, "tp")
    placed = (
        tokens, P(), P("kv", "tp"), P("kv", "tp"), P("kv", "tp"), P("kv", "tp"), P(), P(),
        P("tp"), P(), P("tp", "kv"), tokens, tokens, tokens, tokens, tokens, P(("grp", "kv")),
    )
    return jax.shard_map(
        functools.partial(body, sizes),
        mesh=mesh,
        in_specs=placed,
        out_specs=(tokens, tokens),
        check_vma=False,
    )
```
